256 devices in a mesh: fs: 32 (over z, y), rep: 4 (over x), tp: 2 (over core).
Axes of the slice: x: 4, y: 4, z: 8, core: 2. Of those that a mesh axis runs over, the one named last changes fastest.
Arguments:
- saved_input: bfloat16 [131072, 2048], P(('fs', 'rep')), may hold values from -6 to 6
- cot_input: bfloat16 [131072, 1024], P(('fs', 'rep'), 'tp'), may hold values from -0.015625 to 0.015625
- cot_gate: bfloat16 [131072, 1024], P(('fs', 'rep'), 'tp'), may hold values from -0.015625 to 0.015625
- in_master: float32 [2048, 1024], P('fs', 'tp'), may hold values from -3 to 3
- gate_master: float32 [2048, 1024], P('fs', 'tp'), may hold values from -3 to 3
- in_factor: bfloat16 [2048, 256], P('fs'), may hold values from -0.125 to 0.125
- gate_factor: bfloat16 [2048, 256], P('fs'), may hold values from -0.125 to 0.125
- in_first: float32 [256, 1024], P('fs', 'tp'), may hold values from -6 to 6
- in_second: float32 [256, 1024], P('fs', 'tp'), may hold values from 0.5 to 2
- gate_first: float32 [256, 1024], P('fs', 'tp'), may hold values from -6 to 6
- gate_second: float32 [256, 1024], P('fs', 'tp'), may hold values from 0.5 to 2
Outputs:
- in_master_new: float32 [2048, 1024], P('fs', 'tp')
- gate_master_new: float32 [2048, 1024], P('fs', 'tp')
- in_update: float32 [2048, 1024], P('fs', 'tp')
- gate_update: float32 [2048, 1024], P('fs', 'tp')
- in_first_new: float32 [256, 1024], P('fs', 'tp')
- in_second_new: float32 [256, 1024], P('fs', 'tp')
- gate_first_new: float32 [256, 1024], P('fs', 'tp')
- gate_second_new: float32 [256, 1024], P('fs', 'tp')
- in_copy: bfloat16 [2048, 1024], P(None, 'tp')
- gate_copy: bfloat16 [2048, 1024], P(None, 'tp')
The draws below stay inside these ranges and needn't reach their ends.
All inputs are finite; a program needn't handle non-finite values.
Results may differ from the reference program's by a relative error of at most 0.0065.
Values may be sent and summed in bfloat16 or wider, within the bound.
A program may use at most 64 MiB of HBM per device.

```python
import math
import jax
import jax.numpy as jnp
from jax import lax

D = 2048
W = 1024
RANK = 256
TOKENS = 131072


def steps_of(own_key, shape, pieces, low, top_value):
    level, own = 1.0, jax.random.fold_in(own_key, 6)
    for position, parts in pieces:
        steps = jnp.exp(jax.random.uniform(jax.random.fold_in(own, position), (parts,), jnp.float32, low / len(pieces), top_value / len(pieces)))
        level = level * jnp.repeat(steps, shape[position] // parts).reshape([-1 if axis == position else 1 for axis in range(len(shape))])
    return level


def gaussian(rng, shape, scale, reach, shards=(), kind=jnp.bfloat16):
    gain = steps_of(rng, shape, shards, -0.22, 0.18) if shards else 1.0
    entries = jax.random.normal(rng, shape, jnp.float32) * scale * gain
    return jnp.minimum(jnp.maximum(entries, -reach), reach).astype(kind)


def setup_inputs(seed: int = 0) -> dict:
    keys = jax.random.split(jax.random.key(seed), 12)
    saved_input = gaussian(keys[0], (TOKENS, D), 1.0, 6.0, ((0, 128),))
    cot_input = gaussian(keys[1], (TOKENS, W), TOKENS ** -0.5, 0.015625, ((0, 128), (1, 2)))
    cot_gate = gaussian(keys[2], (TOKENS, W), TOKENS ** -0.5, 0.015625, ((0, 128), (1, 2)))
    in_master = gaussian(keys[3], (D, W), 0.5, 3.0, ((0, 32), (1, 2)), jnp.float32)
    gate_master = gaussian(keys[4], (D, W), 0.5, 3.0, ((0, 32), (1, 2)), jnp.float32)
    in_factor = gaussian(keys[5], (D, RANK), D ** -0.5, 0.125, ((0, 32),))
    gate_factor = gaussian(keys[6], (D, RANK), D ** -0.5, 0.125, ((0, 32),))
    in_first = gaussian(keys[7], (RANK, W), 1.0, 6.0, ((0, 32), (1, 2)), jnp.float32)
    in_second = jnp.clip(jnp.exp(math.log(2.0) - 1.3862944 * jax.random.uniform(keys[8], (RANK, W), jnp.float32) ** steps_of(keys[8], (RANK, W), ((0, 32), (1, 2)), -0.2, 0.2)), 0.5, 2.0)
    gate_first = gaussian(keys[9], (RANK, W), 1.0, 6.0, ((0, 32), (1, 2)), jnp.float32)
    gate_second = jnp.clip(jnp.exp(math.log(2.0) - 1.3862944 * jax.random.uniform(keys[10], (RANK, W), jnp.float32) ** steps_of(keys[10], (RANK, W), ((0, 32), (1, 2)), -0.2, 0.2)), 0.5, 2.0)
    return {"saved_input": saved_input, "cot_input": cot_input, "cot_gate": cot_gate, "in_master": in_master, "gate_master": gate_master, "in_factor": in_factor, "gate_factor": gate_factor, "in_first": in_first, "in_second": in_second, "gate_first": gate_first, "gate_second": gate_second}


def adapt(grad, master, factor, first, second):
    basis = factor.astype(jnp.float32)
    low = jnp.dot(basis.T, grad, precision=lax.Precision.HIGHEST)
    first_new = 0.8 * first + 0.2 * low
    second_new = 0.95 * second + 0.05 * low * low
    normed = first_new / jnp.sqrt(second_new)
    full = jnp.dot(basis, normed, precision=lax.Precision.HIGHEST)
    square = jnp.sum(full * full)
    update = full / jnp.sqrt(square / (D * W) + 0.1)
    master_new = master - 0.05 * update
    return (master_new, update, first_new, second_new, master_new.astype(jnp.bfloat16))

def reference(saved_input, cot_input, cot_gate, in_master, gate_master, in_factor, gate_factor, in_first, in_second, gate_first, gate_second):
    cotangents = jnp.concatenate([cot_input, cot_gate], axis=1)
    span = math.gcd(TOKENS, 8192)
    inputs = saved_input.reshape(TOKENS // span, span, D)
    grads_in = cotangents.reshape(TOKENS // span, span, 2 * W)

    def accumulate(total, pair):
        rows, cots = pair
        part = jnp.dot(rows.astype(jnp.float32).T, cots.astype(jnp.float32), precision=lax.Precision.HIGHEST)
        return (total + part, None)
    grads, _ = lax.scan(accumulate, jnp.zeros((D, 2 * W), jnp.float32), (inputs, grads_in))
    in_out = adapt(grads[:, :W], in_master, in_factor, in_first, in_second)
    gate_out = adapt(grads[:, W:], gate_master, gate_factor, gate_first, gate_second)
    return (in_out[0], gate_out[0], in_out[1], gate_out[1], in_out[2], in_out[3], gate_out[2], gate_out[3], in_out[4], gate_out[4])
```

```python
import jax
import jax.numpy as jnp
from jax import lax
from jax.experimental import pallas as pl
from jax.experimental.pallas import tpu as pltpu
from jax.sharding import PartitionSpec as P

D = 2048
W = 1024
RANK = 256
NX, NY, NZ = 4, 4, 8
ALPHA = 640
BF = jnp.bfloat16
F32 = jnp.float32
ANY = pl.ANY

XY = sorted(
    [(a, b) for a in range(4) for b in range(4) if (a, b) != (0, 0)],
    key=lambda o: -(min(o[0], 4 - o[0]) + min(o[1], 4 - o[1])),
)
ZD = sorted(range(1, 8), key=lambda d: -min(d, 8 - d))


def where_am_i():
    fs, x, c = lax.axis_index("fs"), lax.axis_index("rep"), lax.axis_index("tp")
    return x, lax.rem(fs, 4), lax.div(fs, 4), c


def remote(src, dst, ss, rs, dev):
    return pltpu.make_async_remote_copy(
        src_ref=src,
        dst_ref=dst,
        send_sem=ss,
        recv_sem=rs,
        device_id=dev,
        device_id_type=pl.DeviceIdType.MESH,
    )


def move_kernel(
    x_hbm, ci_hbm, cg_hbm, im_hbm, gm_hbm, if_hbm, gf_hbm, i1_hbm, i2_hbm, g1_hbm, g2_hbm,
    m_out, f_out, n_out, low_out, sq_out,
    xv, cot, cot_t, grad_t, fac, fsh, fall, mast, msh, mom_in, mom_own, mom,
    part, rsb, zb, nb, lowb, sqb,
    s_loc, fz_s, fz_r, mo_s, mo_r, mz_s, mz_r, fx_s, fx_r, ft_s, ft_r, my_s, my_r, mx_s, mx_r,
    rs_s, rs_r, zb_s, zb_r, lo_s, lo_r, ag_s, ag_r, sq_s, sq_r,
):
    x, y, z, c = where_am_i()

    def at(dx, dy, dz, dc=0):
        return {
            "fs": lax.rem(z + dz, 8) * 4 + lax.rem(y + dy, 4),
            "rep": lax.rem(x + dx, 4),
            "tp": lax.rem(c + dc, 2),
        }

    @pl.when(c == 0)
    def _():
        pltpu.make_async_copy(if_hbm, fac, s_loc.at[0]).start()

    @pl.when(c == 1)
    def _():
        pltpu.make_async_copy(gf_hbm, fac, s_loc.at[0]).start()

    moms = [
        pltpu.make_async_copy(r, mom_in.at[k], s_loc.at[1 + k])
        for k, r in enumerate((i1_hbm, g1_hbm, i2_hbm, g2_hbm))
    ]
    masters = [
        pltpu.make_async_copy(r, mast.at[k], s_loc.at[5 + k]) for k, r in enumerate((im_hbm, gm_hbm))
    ]
    cots = [
        pltpu.make_async_copy(r, cot.at[k], s_loc.at[7 + k]) for k, r in enumerate((ci_hbm, cg_hbm))
    ]
    load_x = pltpu.make_async_copy(x_hbm, xv, s_loc.at[9])
    for cp in (*moms, *masters, *cots, load_x):
        cp.start()

    barrier = pltpu.get_barrier_semaphore()
    peers = [at(a, b, 0) for a, b in XY] + [at(0, 0, d) for d in ZD] + [at(0, 0, 0, 1)]
    for p in peers:
        pl.semaphore_signal(barrier, inc=1, device_id=p, device_id_type=pl.DeviceIdType.MESH)

    pltpu.make_async_copy(if_hbm, fac, s_loc.at[0]).wait()
    new = lax.broadcasted_iota(jnp.int32, (RANK, RANK), 1)
    old = lax.broadcasted_iota(jnp.int32, (RANK, RANK), 0)
    ny, nz, ni = lax.shift_right_logical(new, 6), (lax.shift_right_logical(new, 3) & 7), new & 7
    perm = jnp.where(old == (nz * 4 + ny) * 8 + ni, 1.0, 0.0).astype(BF)
    shard = jnp.dot(fac[...], perm, preferred_element_type=F32).astype(BF)
    fsh[...] = shard.reshape(4, 16, RANK)
    fall[c, z, y, x] = fsh[x]

    for cp in moms:
        cp.wait()
    for q in range(4):
        kind, col = q // 2, (q % 2) * 256
        mom_own[q, 0] = mom_in[kind, :, col : col + 256]
        mom_own[q, 1] = mom_in[2 + kind, :, col : col + 256]
    mom[z] = mom_own[x]

    for cp in masters:
        cp.wait()
    msh[:, :512] = mast[0].astype(BF)
    msh[:, 512:] = mast[1].astype(BF)
    keep_m = pltpu.make_async_copy(msh, m_out.at[z, y], s_loc.at[10])
    keep_m.start()

    pl.semaphore_wait(barrier, len(peers))

    fz = [
        remote(fsh.at[x], fall.at[c, z, y, x], fz_s.at[k], fz_r.at[k], at(0, 0, d))
        for k, d in enumerate(ZD)
    ]
    mo = [remote(mom_own.at[x], mom.at[z], mo_s.at[k], mo_r.at[k], at(0, 0, d)) for k, d in enumerate(ZD)]
    mz = [remote(msh, m_out.at[z, y], mz_s.at[k], mz_r.at[k], at(0, 0, d)) for k, d in enumerate(ZD)]
    for cp in (*fz, *mo, *mz):
        cp.start()

    for cp in cots:
        cp.wait()
    for k in range(2):
        cot_t[k * 512 : (k + 1) * 512, :] = cot[k].T
    load_x.wait()

    def grad_step(i, _):
        cols = pl.ds(pl.multiple_of(i * 256, 256), 256)
        grad_t[:, cols] = jnp.dot(cot_t[...], xv[:, cols], preferred_element_type=F32).astype(BF)
        return 0

    lax.fori_loop(0, 2, grad_step, 0)

    for cp in fz:
        cp.wait_recv()
    fx = [
        remote(fall.at[c, :, y, x], fall.at[c, :, y, x], fx_s.at[k], fx_r.at[k], at(a, b, 0))
        for k, (a, b) in enumerate(XY)
    ]
    for cp in fx:
        cp.start()

    def to_partner(k, xs, ys):
        return remote(fall.at[c, :, ys, xs], fall.at[c, :, ys, xs], ft_s.at[k], ft_r.at[k], at(0, 0, 0, 1))

    ft = [to_partner(15, x, y)]
    ft[0].start()

    lax.fori_loop(2, 8, grad_step, 0)

    for k, (a, b) in reversed(list(enumerate(XY))):
        fx[k].wait_recv()
        cp = to_partner(k, lax.rem(x + 4 - a, 4), lax.rem(y + 4 - b, 4))
        cp.start()
        ft.append(cp)
    for cp in ft:
        cp.wait_recv()

    rs = []
    for dx in (2, 1, 3, 0):
        q = lax.rem(x + dx, 4)
        kind = lax.div(q, 2)
        basis = fall[kind].reshape(D, RANK)
        rows = pl.ds(pl.multiple_of(q * 256, 256), 256)
        low_t = jnp.dot(grad_t[rows, :], basis, preferred_element_type=F32)
        part[q] = low_t.T.astype(BF).reshape(4, 64, 256)
        for k, (a, b) in enumerate(XY):
            if a == dx:
                cp = remote(part.at[q, lax.rem(y + b, 4)], rsb.at[k], rs_s.at[k], rs_r.at[k], at(a, b, 0))
                cp.start()
                rs.append(cp)

    for cp in mz:
        cp.wait_recv()
    keep_m.wait()
    rows16 = pl.ds(pl.multiple_of(x * 16, 16), 16)
    my = []
    for k, b in enumerate((2, 1, 3)):
        whole = m_out.at[:, y, :, pl.ds(ALPHA, W - ALPHA)]
        quarter = m_out.at[:, y, rows16, pl.ds(0, ALPHA)]
        my.append(remote(quarter, quarter, my_s.at[2 * k], my_r.at[2 * k], at(0, b, 0)))
        my.append(remote(whole, whole, my_s.at[2 * k + 1], my_r.at[2 * k + 1], at(0, b, 0)))
    for cp in my:
        cp.start()

    keep_f = pltpu.make_async_copy(fall, f_out, s_loc.at[11])
    keep_f.start()

    grams = []
    for kind in range(2):
        basis = fall[kind].reshape(D, RANK)
        g = lax.dot_general(basis, basis, (((0,), (0,)), ((), ())), preferred_element_type=F32)
        hi = g.astype(BF)
        grams.append((hi, (g - hi.astype(F32)).astype(BF)))

    total = part[x, y].astype(F32)
    for cp in rs:
        cp.wait_recv()
    for k in range(15):
        total = total + rsb[k].astype(F32)
    zb[z] = total.astype(BF)
    zs = [remote(zb.at[z], zb.at[z], zb_s.at[k], zb_r.at[k], at(0, 0, d)) for k, d in enumerate(ZD)]
    for cp in zs:
        cp.start()
    for cp in mo:
        cp.wait_recv()
    first = mom[:, 0].reshape(64, 256)
    second = mom[:, 1].reshape(64, 256)
    for cp in zs:
        cp.wait_recv()
    low = zb[0].astype(F32)
    for k in range(1, 8):
        low = low + zb[k].astype(F32)
    first_new = 0.8 * first + 0.2 * low
    second_new = 0.95 * second + 0.05 * low * low
    nb[x, y] = (first_new / jnp.sqrt(second_new)).astype(BF)
    ag = [
        remote(nb.at[x, y], nb.at[x, y], ag_s.at[k], ag_r.at[k], at(a, b, 0))
        for k, (a, b) in enumerate(XY)
    ]
    for cp in ag:
        cp.start()

    part_low = low.reshape(8, 8, 256)
    mine = jnp.zeros((8, 256), F32)
    for k in range(8):
        mine = jnp.where(z == k, part_low[k], mine)
    lowb[x] = mine
    lo = [remote(lowb.at[x], lowb.at[x], lo_s.at[k], lo_r.at[k], at(a, 0, 0)) for k, a in enumerate((2, 1, 3))]
    for cp in lo:
        cp.start()

    for cp in my:
        cp.wait_recv()
    mx = []
    for k, a in enumerate((2, 1, 3)):
        for j in range(3):
            piece = m_out.at[:, lax.rem(y + 1 + j, 4), rows16, pl.ds(0, ALPHA)]
            mx.append(remote(piece, piece, mx_s.at[3 * k + j], mx_r.at[3 * k + j], at(a, 0, 0)))
    for cp in mx:
        cp.start()

    for cp in ag:
        cp.wait_recv()
    keep_n = pltpu.make_async_copy(nb, n_out, s_loc.at[12])
    keep_n.start()
    for kind in range(2):
        acc = jnp.zeros((8, 128), F32)
        for q in (2 * kind, 2 * kind + 1):
            normed = nb[q].reshape(RANK, 256)
            t = jnp.dot(grams[kind][0], normed, preferred_element_type=F32)
            t = t + jnp.dot(grams[kind][1], normed, preferred_element_type=F32)
            s = jnp.sum((t * normed.astype(F32)).reshape(32, 8, 256), axis=0)
            acc = acc + s[:, :128] + s[:, 128:]
        sqb[c, kind] = acc
    sq = remote(sqb.at[c], sqb.at[c], sq_s, sq_r, at(0, 0, 0, 1))
    sq.start()
    for cp in lo:
        cp.wait_recv()
    keep_low = pltpu.make_async_copy(lowb, low_out, s_loc.at[13])
    keep_low.start()
    sq.wait_recv()
    keep_sq = pltpu.make_async_copy(sqb, sq_out, s_loc.at[14])
    keep_sq.start()
    for cp in mx:
        cp.wait_recv()
    for cp in (*fz, *mo, *mz, *fx, *ft, *rs, *my, *zs, *ag, *lo, *mx, sq):
        cp.wait_send()
    for cp in (keep_f, keep_n, keep_low, keep_sq):
        cp.wait()


def gathered(x, ci, cg, im, gm, inf, gf, i1, i2, g1, g2):
    sem = pltpu.SemaphoreType.DMA
    return pl.pallas_call(
        move_kernel,
        name="move",
        out_shape=(
            jax.ShapeDtypeStruct((NZ, NY, 64, W), BF),
            jax.ShapeDtypeStruct((2, NZ, NY, NX, 16, RANK), BF),
            jax.ShapeDtypeStruct((NX, NY, 64, 256), BF),
            jax.ShapeDtypeStruct((NX, 8, 256), F32),
            jax.ShapeDtypeStruct((2, 2, 8, 128), F32),
        ),
        in_specs=[pl.BlockSpec(memory_space=ANY)] * 11,
        out_specs=[pl.BlockSpec(memory_space=ANY)] * 5,
        scratch_shapes=[
            pltpu.VMEM((1024, D), BF),
            pltpu.VMEM((2, 1024, 512), BF),
            pltpu.VMEM((1024, 1024), BF),
            pltpu.VMEM((1024, D), BF),
            pltpu.VMEM((64, RANK), BF),
            pltpu.VMEM((4, 16, RANK), BF),
            pltpu.VMEM((2, NZ, NY, NX, 16, RANK), BF),
            pltpu.VMEM((2, 64, 512), F32),
            pltpu.VMEM((64, W), BF),
            pltpu.VMEM((4, 8, 512), F32),
            pltpu.VMEM((4, 2, 8, 256), F32),
            pltpu.VMEM((NZ, 2, 8, 256), F32),
            pltpu.VMEM((NX, NY, 64, 256), BF),
            pltpu.VMEM((15, 64, 256), BF),
            pltpu.VMEM((NZ, 64, 256), BF),
            pltpu.VMEM((NX, NY, 64, 256), BF),
            pltpu.VMEM((NX, 8, 256), F32),
            pltpu.VMEM((2, 2, 8, 128), F32),
            sem((15,)),
            *[sem((n,)) for n in (7, 7, 7, 7, 7, 7, 15, 15, 16, 16, 6, 6, 9, 9, 15, 15, 7, 7, 3, 3, 15, 15)],
            sem,
            sem,
        ],
        compiler_params=pltpu.CompilerParams(
            collective_id=0, has_side_effects=True, vmem_limit_bytes=48 * 2**20
        ),
        cost_estimate=pl.CostEstimate(flops=6 * 10**9, bytes_accessed=16 * 2**20, transcendentals=0),
    )(x, ci, cg, im, gm, inf, gf, i1, i2, g1, g2)


def scales(sq):
    total = sq[0] + sq[1]
    return [lax.rsqrt(jnp.sum(total[k]) / (D * W) + 0.1) for k in range(2)]


def write_kernel(
    f_ref, n_ref, m_ref, sq_ref, low_ref, im_ref, gm_ref, i1_ref, i2_ref, g1_ref, g2_ref,
    im_out, gm_out, iu_out, gu_out, i1_out, i2_out, g1_out, g2_out, ic_out, gc_out,
):
    _, y, z, _ = where_am_i()
    step = pl.program_id(0)
    scale = scales(sq_ref[...])
    m = m_ref[...].reshape(256, W)
    for kind, out in enumerate((ic_out, gc_out)):
        basis = f_ref[kind].reshape(256, RANK)
        for h in range(2):
            normed = n_ref[2 * kind + h].reshape(RANK, 256)
            full = jnp.dot(basis, normed, preferred_element_type=F32)
            col = 256 * h
            old = m[:, kind * 512 + col : kind * 512 + col + 256].astype(F32)
            out[:, col : col + 256] = (old - 0.05 * (full * scale[kind])).astype(BF)

    @pl.when(step == z)
    def _():
        for kind, (old, new, upd) in enumerate(((im_ref, im_out, iu_out), (gm_ref, gm_out, gu_out))):
            basis = f_ref[kind, 0, y].reshape(64, RANK)
            for h in range(2):
                normed = n_ref[2 * kind + h].reshape(RANK, 256)
                cols = slice(256 * h, 256 * h + 256)
                u = jnp.dot(basis, normed, preferred_element_type=F32) * scale[kind]
                upd[:, cols] = u
                new[:, cols] = old[:, cols] - 0.05 * u

    @pl.when(step == 0)
    def _():
        for kind, (f_old, s_old, f_new, s_new) in enumerate(
            ((i1_ref, i2_ref, i1_out, i2_out), (g1_ref, g2_ref, g1_out, g2_out))
        ):
            for h in range(2):
                low = low_ref[2 * kind + h]
                cols = slice(256 * h, 256 * h + 256)
                f_new[:, cols] = 0.8 * f_old[:, cols] + 0.2 * low
                s_new[:, cols] = 0.95 * s_old[:, cols] + 0.05 * low * low


def written(f, n, m, sq, low, im, gm, i1, i2, g1, g2):
    def fixed(shape):
        return pl.BlockSpec(shape, lambda i: (0,) * len(shape))

    own, mo = fixed((64, 512)), fixed((8, 512))
    return pl.pallas_call(
        write_kernel,
        name="write",
        grid=(NZ,),
        out_shape=(
            *[jax.ShapeDtypeStruct((64, 512), F32)] * 4,
            *[jax.ShapeDtypeStruct((8, 512), F32)] * 4,
            *[jax.ShapeDtypeStruct((D, 512), BF)] * 2,
        ),
        in_specs=[
            pl.BlockSpec((2, 1, NY, NX, 16, RANK), lambda i: (0, i, 0, 0, 0, 0)),
            fixed((NX, NY, 64, 256)),
            pl.BlockSpec((1, NY, 64, W), lambda i: (i, 0, 0, 0)),
            fixed((2, 2, 8, 128)),
            fixed((NX, 8, 256)),
            own, own, mo, mo, mo, mo,
        ],
        out_specs=[own] * 4 + [mo] * 4 + [pl.BlockSpec((256, 512), lambda i: (i, 0))] * 2,
        compiler_params=pltpu.CompilerParams(dimension_semantics=("arbitrary",)),
    )(f, n, m, sq, low, im, gm, i1, i2, g1, g2)


def on_device(x, ci, cg, im, gm, inf, gf, i1, i2, g1, g2):
    m, f, n, low, sq = gathered(x, ci, cg, im, gm, inf, gf, i1, i2, g1, g2)
    out = written(f, n, m, sq, low, im, gm, i1, i2, g1, g2)
    return tuple(out)


def solution(mesh):
    tokens, rows, moments = P(("fs", "rep"), "tp"), P("fs", "tp"), P("fs", "tp")
    return jax.shard_map(
        on_device,
        mesh=mesh,
        in_specs=(
            P(("fs", "rep"), None), tokens, tokens, rows, rows, P("fs", None), P("fs", None),
            moments, moments, moments, moments,
        ),
        out_specs=(rows,) * 4 + (moments,) * 4 + (P(None, "tp"),) * 2,
        check_vma=False,
    )
```

```python
import jax
import jax.numpy as jnp
from jax import lax
from jax.experimental import pallas as pl
from jax.experimental.pallas import tpu as pltpu
from jax.sharding import PartitionSpec as P

D = 2048
W = 1024
RANK = 256
NX, NY, NZ = 4, 4, 8
YZ_COLS, ZY_COLS, ZYX_COLS, Z_COLS = pl.ds(0, 384), pl.ds(384, 256), pl.ds(640, 384), pl.ds(384, 640)
BF = jnp.bfloat16
F32 = jnp.float32
VMEM = 67_043_328
ANY = pl.ANY

XY = sorted(
    [(a, b) for a in range(4) for b in range(4) if (a, b) != (0, 0)],
    key=lambda o: -(min(o[0], 4 - o[0]) + min(o[1], 4 - o[1])),
)
ZD = sorted(range(1, 8), key=lambda d: -min(d, 8 - d))


def where_am_i():
    fs, x, c = lax.axis_index("fs"), lax.axis_index("rep"), lax.axis_index("tp")
    return x, lax.rem(fs, 4), lax.div(fs, 4), c


def remote(src, dst, ss, rs, dev):
    return pltpu.make_async_remote_copy(
        src_ref=src,
        dst_ref=dst,
        send_sem=ss,
        recv_sem=rs,
        device_id=dev,
        device_id_type=pl.DeviceIdType.MESH,
    )


def move_kernel(
    x_hbm, ci_hbm, cg_hbm, im_hbm, gm_hbm, if_hbm, gf_hbm, i1_hbm, i2_hbm, g1_hbm, g2_hbm,
    m_out, f_out, n_out, low_out, sq_out,
    xv, cot, cot_t, grad_t, fac, fsh, fall, mast, msh, mom_in, mom_own, mom,
    part, rsb, zb, nb, lowb, sqb,
    s_loc, fz_s, fz_r, mo_s, mo_r, ra_s, ra_r, rb_s, rb_r, by_s, by_r, fx_s, fx_r, ft_s, ft_r,
    my_s, my_r, mx_s, mx_r,
    rs_s, rs_r, zb_s, zb_r, lo_s, lo_r, ag_s, ag_r, sq_s, sq_r,
):
    x, y, z, c = where_am_i()

    def at(dx, dy, dz, dc=0):
        return {
            "fs": lax.rem(z + dz, 8) * 4 + lax.rem(y + dy, 4),
            "rep": lax.rem(x + dx, 4),
            "tp": lax.rem(c + dc, 2),
        }

    @pl.when(c == 0)
    def _():
        pltpu.make_async_copy(if_hbm, fac, s_loc.at[0]).start()

    @pl.when(c == 1)
    def _():
        pltpu.make_async_copy(gf_hbm, fac, s_loc.at[0]).start()

    moms = [
        pltpu.make_async_copy(r, mom_in.at[k], s_loc.at[1 + k])
        for k, r in enumerate((i1_hbm, g1_hbm, i2_hbm, g2_hbm))
    ]
    masters = [
        pltpu.make_async_copy(r, mast.at[k], s_loc.at[5 + k]) for k, r in enumerate((im_hbm, gm_hbm))
    ]
    cots = [
        pltpu.make_async_copy(r, cot.at[k], s_loc.at[7 + k]) for k, r in enumerate((ci_hbm, cg_hbm))
    ]
    load_x = pltpu.make_async_copy(x_hbm, xv, s_loc.at[9])
    for cp in (*moms, *masters, *cots, load_x):
        cp.start()

    barrier = pltpu.get_barrier_semaphore()
    peers = [at(a, b, 0) for a, b in XY] + [at(0, 0, d) for d in ZD] + [at(0, 0, 0, 1)]
    for p in peers:
        pl.semaphore_signal(barrier, inc=1, device_id=p, device_id_type=pl.DeviceIdType.MESH)

    pltpu.make_async_copy(if_hbm, fac, s_loc.at[0]).wait()
    new = lax.broadcasted_iota(jnp.int32, (RANK, RANK), 1)
    old = lax.broadcasted_iota(jnp.int32, (RANK, RANK), 0)
    ny, nz, ni = lax.shift_right_logical(new, 6), (lax.shift_right_logical(new, 3) & 7), new & 7
    perm = jnp.where(old == (nz * 4 + ny) * 8 + ni, 1.0, 0.0).astype(BF)
    shard = jnp.dot(fac[...], perm, preferred_element_type=F32).astype(BF)
    fsh[...] = shard.reshape(4, 16, RANK)
    fall[c, z, y, x] = fsh[x]

    for cp in moms:
        cp.wait()
    for q in range(4):
        kind, col = q // 2, (q % 2) * 256
        mom_own[q, 0] = mom_in[kind, :, col : col + 256]
        mom_own[q, 1] = mom_in[2 + kind, :, col : col + 256]
    mom[z] = mom_own[x]

    for cp in masters:
        cp.wait()
    msh[:, :512] = mast[0].astype(BF)
    msh[:, 512:] = mast[1].astype(BF)
    keep_m = pltpu.make_async_copy(msh, m_out.at[z, y], s_loc.at[10])
    keep_m.start()

    pl.semaphore_wait(barrier, len(peers))

    fz = [
        remote(fsh.at[x], fall.at[c, z, y, x], fz_s.at[k], fz_r.at[k], at(0, 0, d))
        for k, d in enumerate(ZD)
    ]
    mo = [remote(mom_own.at[x], mom.at[z], mo_s.at[k], mo_r.at[k], at(0, 0, d)) for k, d in enumerate(ZD)]
    by = [
        remote(msh.at[:, YZ_COLS], m_out.at[z, y, :, YZ_COLS], by_s.at[k], by_r.at[k], at(0, b, 0))
        for k, b in enumerate((2, 1, 3))
    ]

    def ring(block, ss, rs):
        hops = []
        for h in range(4):
            rows = (pl.ds(0, 32), pl.ds(32, 32)) if h == 3 else (pl.ds(0, 64),) * 2
            up = block(lax.rem(z + 8 - h, 8), rows[0])
            down = block(lax.rem(z + h, 8), rows[1])
            hops.append(
                (
                    remote(up, up, ss.at[h, 0], rs.at[h, 0], at(0, 0, 1)),
                    remote(down, down, ss.at[h, 1], rs.at[h, 1], at(0, 0, 7)),
                )
            )
        return hops

    def hop(hops, h):
        if h:
            for cp in hops[h - 1]:
                cp.wait_recv()
        for cp in hops[h]:
            cp.start()

    ra = ring(lambda k, rows: m_out.at[k, y, rows, Z_COLS], ra_s, ra_r)
    rb = ring(lambda k, rows: m_out.at[k, :, rows, YZ_COLS], rb_s, rb_r)
    for cp in (*fz, *by):
        cp.start()
    keep_m.wait()
    hop(ra, 0)
    for cp in mo:
        cp.start()

    for cp in cots:
        cp.wait()
    for k in range(2):
        cot_t[k * 512 : (k + 1) * 512, :] = cot[k].T
    load_x.wait()

    def grad_step(i, _):
        cols = pl.ds(pl.multiple_of(i * 256, 256), 256)
        grad_t[:, cols] = jnp.dot(cot_t[...], xv[:, cols], preferred_element_type=F32).astype(BF)
        return 0

    lax.fori_loop(0, 2, grad_step, 0)

    for cp in fz:
        cp.wait_recv()
    fx = [
        remote(fall.at[c, :, y, x], fall.at[c, :, y, x], fx_s.at[k], fx_r.at[k], at(a, b, 0))
        for k, (a, b) in enumerate(XY)
    ]
    for cp in fx:
        cp.start()

    def to_partner(k, xs, ys):
        return remote(fall.at[c, :, ys, xs], fall.at[c, :, ys, xs], ft_s.at[k], ft_r.at[k], at(0, 0, 0, 1))

    ft = [to_partner(15, x, y)]
    ft[0].start()

    lax.fori_loop(2, 4, grad_step, 0)
    hop(ra, 1)
    for cp in by:
        cp.wait_recv()
    hop(rb, 0)
    lax.fori_loop(4, 8, grad_step, 0)
    hop(ra, 2)

    for k, (a, b) in reversed(list(enumerate(XY))):
        if k == 4:
            hop(ra, 3)
            hop(rb, 1)
        fx[k].wait_recv()
        cp = to_partner(k, lax.rem(x + 4 - a, 4), lax.rem(y + 4 - b, 4))
        cp.start()
        ft.append(cp)
    for cp in ft:
        cp.wait_recv()

    for cp in ra[3]:
        cp.wait_recv()
    rows16 = pl.ds(pl.multiple_of(x * 16, 16), 16)
    my = []
    for k, b in enumerate((2, 1, 3)):
        quarter = m_out.at[:, y, rows16, ZYX_COLS]
        my.append(remote(quarter, quarter, my_s.at[k], my_r.at[k], at(0, b, 0)))
    for cp in my:
        cp.start()

    rs = []
    for dx in (2, 1, 3, 0):
        q = lax.rem(x + dx, 4)
        kind = lax.div(q, 2)
        basis = fall[kind].reshape(D, RANK)
        rows = pl.ds(pl.multiple_of(q * 256, 256), 256)
        low_t = jnp.dot(grad_t[rows, :], basis, preferred_element_type=F32)
        part[q] = low_t.T.astype(BF).reshape(4, 64, 256)
        for k, (a, b) in enumerate(XY):
            if a == dx:
                cp = remote(part.at[q, lax.rem(y + b, 4)], rsb.at[k], rs_s.at[k], rs_r.at[k], at(a, b, 0))
                cp.start()
                rs.append(cp)

    mw = []
    for k, b in enumerate((2, 1, 3)):
        whole = m_out.at[:, y, :, ZY_COLS]
        mw.append(remote(whole, whole, my_s.at[3 + k], my_r.at[3 + k], at(0, b, 0)))
    for cp in mw:
        cp.start()

    keep_f = pltpu.make_async_copy(fall, f_out, s_loc.at[11])
    keep_f.start()

    grams = []
    for kind in range(2):
        basis = fall[kind].reshape(D, RANK)
        g = lax.dot_general(basis, basis, (((0,), (0,)), ((), ())), preferred_element_type=F32)
        hi = g.astype(BF)
        grams.append((hi, (g - hi.astype(F32)).astype(BF)))

    hop(rb, 2)
    total = part[x, y].astype(F32)
    for cp in rs:
        cp.wait_recv()
    for k in range(15):
        total = total + rsb[k].astype(F32)
    zb[z] = total.astype(BF)
    zs = [remote(zb.at[z], zb.at[z], zb_s.at[k], zb_r.at[k], at(0, 0, d)) for k, d in enumerate(ZD)]
    for cp in zs:
        cp.start()
    for cp in my:
        cp.wait_recv()
    mx = []
    for k, a in enumerate((2, 1, 3)):
        for j in range(3):
            piece = m_out.at[:, lax.rem(y + 1 + j, 4), rows16, ZYX_COLS]
            mx.append(remote(piece, piece, mx_s.at[3 * k + j], mx_r.at[3 * k + j], at(a, 0, 0)))
    for cp in mx:
        cp.start()

    hop(rb, 3)
    for cp in mo:
        cp.wait_recv()
    first = mom[:, 0].reshape(64, 256)
    second = mom[:, 1].reshape(64, 256)
    for cp in zs:
        cp.wait_recv()
    low = zb[0].astype(F32)
    for k in range(1, 8):
        low = low + zb[k].astype(F32)
    first_new = 0.8 * first + 0.2 * low
    second_new = 0.95 * second + 0.05 * low * low
    nb[x, y] = (first_new / jnp.sqrt(second_new)).astype(BF)
    ag = [
        remote(nb.at[x, y], nb.at[x, y], ag_s.at[k], ag_r.at[k], at(a, b, 0))
        for k, (a, b) in enumerate(XY)
    ]
    for cp in ag:
        cp.start()

    part_low = low.reshape(8, 8, 256)
    mine = jnp.zeros((8, 256), F32)
    for k in range(8):
        mine = jnp.where(z == k, part_low[k], mine)
    lowb[x] = mine
    lo = [remote(lowb.at[x], lowb.at[x], lo_s.at[k], lo_r.at[k], at(a, 0, 0)) for k, a in enumerate((2, 1, 3))]
    for cp in lo:
        cp.start()

    for cp in ag:
        cp.wait_recv()
    keep_n = pltpu.make_async_copy(nb, n_out, s_loc.at[12])
    keep_n.start()
    for kind in range(2):
        acc = jnp.zeros((8, 128), F32)
        for q in (2 * kind, 2 * kind + 1):
            normed = nb[q].reshape(RANK, 256)
            t = jnp.dot(grams[kind][0], normed, preferred_element_type=F32)
            t = t + jnp.dot(grams[kind][1], normed, preferred_element_type=F32)
            s = jnp.sum((t * normed.astype(F32)).reshape(32, 8, 256), axis=0)
            acc = acc + s[:, :128] + s[:, 128:]
        sqb[c, kind] = acc
    sq = remote(sqb.at[c], sqb.at[c], sq_s, sq_r, at(0, 0, 0, 1))
    sq.start()
    for cp in lo:
        cp.wait_recv()
    keep_low = pltpu.make_async_copy(lowb, low_out, s_loc.at[13])
    keep_low.start()
    sq.wait_recv()
    keep_sq = pltpu.make_async_copy(sqb, sq_out, s_loc.at[14])
    keep_sq.start()
    for cp in (*mw, *rb[3], *mx):
        cp.wait_recv()
    rings = [cp for h in (*ra, *rb) for cp in h]
    for cp in (*fz, *mo, *by, *rings, *fx, *ft, *rs, *my, *mw, *zs, *ag, *lo, *mx, sq):
        cp.wait_send()
    for cp in (keep_f, keep_n, keep_low, keep_sq):
        cp.wait()


def gathered(x, ci, cg, im, gm, inf, gf, i1, i2, g1, g2):
    sem = pltpu.SemaphoreType.DMA
    return pl.pallas_call(
        move_kernel,
        name="move",
        out_shape=(
            jax.ShapeDtypeStruct((NZ, NY, 64, W), BF),
            jax.ShapeDtypeStruct((2, NZ, NY, NX, 16, RANK), BF),
            jax.ShapeDtypeStruct((NX, NY, 64, 256), BF),
            jax.ShapeDtypeStruct((NX, 8, 256), F32),
            jax.ShapeDtypeStruct((2, 2, 8, 128), F32),
        ),
        in_specs=[pl.BlockSpec(memory_space=ANY)] * 11,
        out_specs=[pl.BlockSpec(memory_space=ANY)] * 5,
        scratch_shapes=[
            pltpu.VMEM((1024, D), BF),
            pltpu.VMEM((2, 1024, 512), BF),
            pltpu.VMEM((1024, 1024), BF),
            pltpu.VMEM((1024, D), BF),
            pltpu.VMEM((64, RANK), BF),
            pltpu.VMEM((4, 16, RANK), BF),
            pltpu.VMEM((2, NZ, NY, NX, 16, RANK), BF),
            pltpu.VMEM((2, 64, 512), F32),
            pltpu.VMEM((64, W), BF),
            pltpu.VMEM((4, 8, 512), F32),
            pltpu.VMEM((4, 2, 8, 256), F32),
            pltpu.VMEM((NZ, 2, 8, 256), F32),
            pltpu.VMEM((NX, NY, 64, 256), BF),
            pltpu.VMEM((15, 64, 256), BF),
            pltpu.VMEM((NZ, 64, 256), BF),
            pltpu.VMEM((NX, NY, 64, 256), BF),
            pltpu.VMEM((NX, 8, 256), F32),
            pltpu.VMEM((2, 2, 8, 128), F32),
            sem((15,)),
            *[sem((n,)) for n in (7, 7, 7, 7)],
            *[sem((4, 2))] * 4,
            *[sem((n,)) for n in (3, 3, 15, 15, 16, 16, 6, 6, 9, 9, 15, 15, 7, 7, 3, 3, 15, 15)],
            sem,
            sem,
        ],
        compiler_params=pltpu.CompilerParams(
            collective_id=0, has_side_effects=True, vmem_limit_bytes=VMEM
        ),
        cost_estimate=pl.CostEstimate(flops=6 * 10**9, bytes_accessed=16 * 2**20, transcendentals=0),
    )(x, ci, cg, im, gm, inf, gf, i1, i2, g1, g2)


def scales(sq):
    total = sq[0] + sq[1]
    return [lax.rsqrt(jnp.sum(total[k]) / (D * W) + 0.1) for k in range(2)]


def write_kernel(
    f_ref, n_ref, m_ref, sq_ref, low_ref, im_ref, gm_ref, i1_ref, i2_ref, g1_ref, g2_ref,
    im_out, gm_out, iu_out, gu_out, i1_out, i2_out, g1_out, g2_out, ic_out, gc_out,
    scale_ref,
):
    _, y, z, _ = where_am_i()
    step = pl.program_id(0)

    @pl.when(step == 0)
    def _():
        for kind, value in enumerate(scales(sq_ref[...])):
            scale_ref[kind] = jnp.full((8, 128), value, F32)

    scale = [scale_ref[kind, 0:1, 0:1] for kind in range(2)]
    m = m_ref[...].reshape(256, W)
    for kind, out in enumerate((ic_out, gc_out)):
        basis = f_ref[kind].reshape(256, RANK)
        for h in range(2):
            normed = n_ref[2 * kind + h].reshape(RANK, 256)
            full = jnp.dot(basis, normed, preferred_element_type=F32)
            col = 256 * h
            old = m[:, kind * 512 + col : kind * 512 + col + 256].astype(F32)
            out[:, col : col + 256] = (old - 0.05 * (full * scale[kind])).astype(BF)

    @pl.when(step == z)
    def _():
        for kind, (old, new, upd) in enumerate(((im_ref, im_out, iu_out), (gm_ref, gm_out, gu_out))):
            basis = f_ref[kind, 0, y].reshape(64, RANK)
            for h in range(2):
                normed = n_ref[2 * kind + h].reshape(RANK, 256)
                cols = slice(256 * h, 256 * h + 256)
                u = jnp.dot(basis, normed, preferred_element_type=F32) * scale[kind]
                upd[:, cols] = u
                new[:, cols] = old[:, cols] - 0.05 * u

    @pl.when(step == 0)
    def _():
        for kind, (f_old, s_old, f_new, s_new) in enumerate(
            ((i1_ref, i2_ref, i1_out, i2_out), (g1_ref, g2_ref, g1_out, g2_out))
        ):
            for h in range(2):
                low = low_ref[2 * kind + h]
                cols = slice(256 * h, 256 * h + 256)
                f_new[:, cols] = 0.8 * f_old[:, cols] + 0.2 * low
                s_new[:, cols] = 0.95 * s_old[:, cols] + 0.05 * low * low


def written(f, n, m, sq, low, im, gm, i1, i2, g1, g2):
    def fixed(shape):
        return pl.BlockSpec(shape, lambda i: (0,) * len(shape))

    own, mo = fixed((64, 512)), fixed((8, 512))
    return pl.pallas_call(
        write_kernel,
        name="write",
        grid=(NZ,),
        out_shape=(
            *[jax.ShapeDtypeStruct((64, 512), F32)] * 4,
            *[jax.ShapeDtypeStruct((8, 512), F32)] * 4,
            *[jax.ShapeDtypeStruct((D, 512), BF)] * 2,
        ),
        in_specs=[
            pl.BlockSpec((2, 1, NY, NX, 16, RANK), lambda i: (0, i, 0, 0, 0, 0)),
            fixed((NX, NY, 64, 256)),
            pl.BlockSpec((1, NY, 64, W), lambda i: (i, 0, 0, 0)),
            fixed((2, 2, 8, 128)),
            fixed((NX, 8, 256)),
            own, own, mo, mo, mo, mo,
        ],
        out_specs=[own] * 4 + [mo] * 4 + [pl.BlockSpec((256, 512), lambda i: (i, 0))] * 2,
        scratch_shapes=[pltpu.VMEM((2, 8, 128), F32)],
        compiler_params=pltpu.CompilerParams(
            dimension_semantics=("arbitrary",), vmem_limit_bytes=VMEM
        ),
    )(f, n, m, sq, low, im, gm, i1, i2, g1, g2)


def on_device(x, ci, cg, im, gm, inf, gf, i1, i2, g1, g2):
    m, f, n, low, sq = gathered(x, ci, cg, im, gm, inf, gf, i1, i2, g1, g2)
    out = written(f, n, m, sq, low, im, gm, i1, i2, g1, g2)
    return tuple(out)


def solution(mesh):
    tokens, rows, moments = P(("fs", "rep"), "tp"), P("fs", "tp"), P("fs", "tp")
    return jax.shard_map(
        on_device,
        mesh=mesh,
        in_specs=(
            P(("fs", "rep"), None), tokens, tokens, rows, rows, P("fs", None), P("fs", None),
            moments, moments, moments, moments,
        ),
        out_specs=(rows,) * 4 + (moments,) * 4 + (P(None, "tp"),) * 2,
        check_vma=False,
    )
```

```python
import jax
import jax.numpy as jnp
from jax import lax
from jax.experimental import pallas as pl
from jax.experimental.pallas import tpu as pltpu
from jax.sharding import PartitionSpec as P

D = 2048
W = 1024
RANK = 256
NX, NY, NZ = 4, 4, 8
YZ_COLS, YZ0, YZ1 = pl.ds(0, 512), pl.ds(0, 256), pl.ds(256, 256)
ZY_COLS, ZYX_COLS, Z_COLS = pl.ds(512, 128), pl.ds(640, 384), pl.ds(512, 512)
HERE = 3
NEAR, BELOW, ABOVE = pl.ds(2, 3), pl.ds(0, 2), pl.ds(5, 3)
BF = jnp.bfloat16
F32 = jnp.float32
VMEM = 67_043_328
ANY = pl.ANY

XY = sorted(
    [(a, b) for a in range(4) for b in range(4) if (a, b) != (0, 0)],
    key=lambda o: -(min(o[0], 4 - o[0]) + min(o[1], 4 - o[1])),
)
ZD = sorted(range(1, 8), key=lambda d: -min(d, 8 - d))


def where_am_i():
    fs, x, c = lax.axis_index("fs"), lax.axis_index("rep"), lax.axis_index("tp")
    return x, lax.rem(fs, 4), lax.div(fs, 4), c


def remote(src, dst, ss, rs, dev):
    return pltpu.make_async_remote_copy(
        src_ref=src,
        dst_ref=dst,
        send_sem=ss,
        recv_sem=rs,
        device_id=dev,
        device_id_type=pl.DeviceIdType.MESH,
    )


def move_kernel(
    x_hbm, ci_hbm, cg_hbm, im_hbm, gm_hbm, if_hbm, gf_hbm, i1_hbm, i2_hbm, g1_hbm, g2_hbm,
    m_out, f_out, n_out, low_out, sq_out,
    xv, cot, cot_t, grad_t, fac, fsh, fall, mast, msh, mom_in, mom_own, mom,
    part, rsb, zb, nb, lowb, sqb,
    s_loc, fz_s, fz_r, mo_s, mo_r, ra_s, ra_r, rb_s, rb_r, rc_s, rc_r, by_s, by_r, fa_s, fa_r, fb_s, fb_r,
    fc_s, fc_r, fd_s, fd_r, ft_s, ft_r,
    my_s, my_r, mx_s, mx_r,
    rs_s, rs_r, zb_s, zb_r, lo_s, lo_r, ag_s, ag_r, sq_s, sq_r,
):
    x, y, z, c = where_am_i()

    def at(dx, dy, dz, dc=0):
        return {
            "fs": lax.rem(z + dz, 8) * 4 + lax.rem(y + dy, 4),
            "rep": lax.rem(x + dx, 4),
            "tp": lax.rem(c + dc, 2),
        }

    @pl.when(c == 0)
    def _():
        pltpu.make_async_copy(if_hbm, fac, s_loc.at[0]).start()

    @pl.when(c == 1)
    def _():
        pltpu.make_async_copy(gf_hbm, fac, s_loc.at[0]).start()

    moms = [
        pltpu.make_async_copy(r, mom_in.at[k], s_loc.at[1 + k])
        for k, r in enumerate((i1_hbm, g1_hbm, i2_hbm, g2_hbm))
    ]
    masters = [
        pltpu.make_async_copy(r, mast.at[k], s_loc.at[5 + k]) for k, r in enumerate((im_hbm, gm_hbm))
    ]
    cots = [
        pltpu.make_async_copy(r, cot.at[k], s_loc.at[7 + k]) for k, r in enumerate((ci_hbm, cg_hbm))
    ]
    load_x = pltpu.make_async_copy(x_hbm, xv, s_loc.at[9])
    for cp in (*moms, *masters, *cots, load_x):
        cp.start()

    barrier = pltpu.get_barrier_semaphore()
    peers = [at(a, b, 0) for a, b in XY] + [at(0, 0, d) for d in ZD] + [at(0, 0, 0, 1)]
    for p in peers:
        pl.semaphore_signal(barrier, inc=1, device_id=p, device_id_type=pl.DeviceIdType.MESH)

    pltpu.make_async_copy(if_hbm, fac, s_loc.at[0]).wait()
    new = lax.broadcasted_iota(jnp.int32, (RANK, RANK), 1)
    old = lax.broadcasted_iota(jnp.int32, (RANK, RANK), 0)
    ny, nz, ni = lax.shift_right_logical(new, 6), (lax.shift_right_logical(new, 3) & 7), new & 7
    perm = jnp.where(old == (nz * 4 + ny) * 8 + ni, 1.0, 0.0).astype(BF)
    shard = jnp.dot(fac[...], perm, preferred_element_type=F32).astype(BF)
    fsh[...] = shard.reshape(4, 16, RANK)
    fall[c, z, y, x] = fsh[x]

    for cp in moms:
        cp.wait()
    for q in range(4):
        kind, col = q // 2, (q % 2) * 256
        mom_own[q, 0] = mom_in[kind, :, col : col + 256]
        mom_own[q, 1] = mom_in[2 + kind, :, col : col + 256]
    mom[z] = mom_own[x]

    for cp in masters:
        cp.wait()
    msh[:, :512] = mast[0].astype(BF)
    msh[:, 512:] = mast[1].astype(BF)
    keep_m = pltpu.make_async_copy(msh, m_out.at[HERE, y], s_loc.at[10])
    keep_m.start()

    pl.semaphore_wait(barrier, len(peers))

    fz = [
        remote(fsh.at[x], fall.at[c, z, y, x], fz_s.at[k], fz_r.at[k], at(0, 0, d))
        for k, d in enumerate(ZD)
    ]
    mo = [remote(mom_own.at[x], mom.at[z], mo_s.at[k], mo_r.at[k], at(0, 0, d)) for k, d in enumerate(ZD)]
    by = [
        remote(msh.at[:, YZ_COLS], m_out.at[HERE, y, :, YZ_COLS], by_s.at[k], by_r.at[k], at(0, b, 0))
        for k, b in enumerate((2, 1, 3))
    ]

    def ring(block, ss, rs):
        hops = []
        for h in range(4):
            lower, upper = (pl.ds(0, 32), pl.ds(32, 32)) if h == 3 else (pl.ds(0, 64),) * 2
            up = (block(HERE - h, lower), block(HERE - h - 1 if h < 3 else HERE + 4, lower))
            down = (block(HERE + h, upper), block(HERE + h + 1, upper))
            hops.append(
                (
                    remote(*up, ss.at[h, 0], rs.at[h, 0], at(0, 0, 1)),
                    remote(*down, ss.at[h, 1], rs.at[h, 1], at(0, 0, 7)),
                )
            )
        return hops

    def hop(hops, h):
        if h:
            for cp in hops[h - 1]:
                cp.wait_recv()
        for cp in hops[h]:
            cp.start()

    ra = ring(lambda k, rows: m_out.at[k, y, rows, Z_COLS], ra_s, ra_r)
    rb = ring(lambda k, rows: m_out.at[k, :, rows, YZ0], rb_s, rb_r)
    rc = ring(lambda k, rows: m_out.at[k, :, rows, YZ1], rc_s, rc_r)
    for cp in (*fz, *by):
        cp.start()
    keep_m.wait()
    hop(ra, 0)

    rows16 = pl.ds(pl.multiple_of(x * 16, 16), 16)
    part_of = {"near": NEAR, "below": BELOW, "above": ABOVE}

    def along_y(group, rows, cols, first):
        block = m_out.at[part_of[group], y, rows, cols]
        return [
            remote(block, block, my_s.at[first + k], my_r.at[first + k], at(0, b, 0))
            for k, b in enumerate((2, 1, 3))
        ]

    def along_x(group, first):
        out = []
        for k, a in enumerate((2, 1, 3)):
            for j in range(3):
                block = m_out.at[part_of[group], lax.rem(y + 1 + j, 4), rows16, ZYX_COLS]
                n = first + 3 * k + j
                out.append(remote(block, block, mx_s.at[n], mx_r.at[n], at(a, 0, 0)))
        return out

    every = pl.ds(0, 64)
    groups = ("near", "below", "above")
    quarters = {g: along_y(g, rows16, ZYX_COLS, 3 * k) for k, g in enumerate(groups)}
    wholes = {g: along_y(g, every, ZY_COLS, 9 + 3 * k) for k, g in enumerate(groups)}
    acrosses = {g: along_x(g, 9 * k) for k, g in enumerate(groups)}

    def start(*lists):
        for cps in lists:
            for cp in cps:
                cp.start()

    def arrive(*lists):
        for cps in lists:
            for cp in cps:
                cp.wait_recv()

    for cp in cots:
        cp.wait()
    for k in range(2):
        cot_t[k * 512 : (k + 1) * 512, :] = cot[k].T
    load_x.wait()

    def grad_step(i, _):
        cols = pl.ds(pl.multiple_of(i * 256, 256), 256)
        grad_t[:, cols] = jnp.dot(cot_t[...], xv[:, cols], preferred_element_type=F32).astype(BF)
        return 0

    lax.fori_loop(0, 2, grad_step, 0)

    for cp in fz:
        cp.wait_recv()
    def piece(half, xs, ys):
        return fall.at[c, pl.ds(4 * half, 4), ys, xs]

    def send_piece(half, xs, ys, ss, rs, dev):
        block = piece(half, xs, ys)
        return remote(block, block, ss, rs, dev)

    def back(p, d):
        return lax.rem(p + 4 - d, 4)

    near = (1, 3, 2)
    fa = [send_piece(0, x, y, fa_s.at[k], fa_r.at[k], at(0, b, 0)) for k, b in enumerate(near)]
    fb = [send_piece(1, x, y, fb_s.at[k], fb_r.at[k], at(a, 0, 0)) for k, a in enumerate(near)]
    ysrc = [y] + [back(y, b) for b in near]
    xsrc = [x] + [back(x, a) for a in near]
    fc = [
        [send_piece(0, x, ys, fc_s.at[i, k], fc_r.at[i, k], at(a, 0, 0)) for k, a in enumerate(near)]
        for i, ys in enumerate(ysrc)
    ]
    fd = [
        [send_piece(1, xs, y, fd_s.at[i, k], fd_r.at[i, k], at(0, b, 0)) for k, b in enumerate(near)]
        for i, xs in enumerate(xsrc)
    ]
    ft = []

    def to_partner(half, xs, ys):
        k = len(ft)
        cp = send_piece(half, xs, ys, ft_s.at[k], ft_r.at[k], at(0, 0, 0, 1))
        cp.start()
        ft.append(cp)

    start(fa, fb, fc[0], fd[0])
    to_partner(0, x, y)
    to_partner(1, x, y)

    lax.fori_loop(2, 4, grad_step, 0)
    hop(ra, 1)
    start(quarters["near"])
    arrive(by)
    hop(rb, 0)

    def relay(k):
        fa[k].wait_recv()
        start(fc[1 + k])
        fb[k].wait_recv()
        start(fd[1 + k])
        to_partner(0, x, ysrc[1 + k])
        to_partner(1, xsrc[1 + k], y)

    relay(0)
    relay(1)
    lax.fori_loop(4, 5, grad_step, 0)
    relay(2)
    hop(ra, 2)
    hop(rc, 0)
    lax.fori_loop(5, 7, grad_step, 0)

    def land(i):
        for k in range(3):
            fc[i][k].wait_recv()
            to_partner(0, xsrc[1 + k], ysrc[i])
            fd[i][k].wait_recv()
            to_partner(1, xsrc[i], ysrc[1 + k])

    land(0)
    arrive(quarters["near"])
    start(acrosses["near"], wholes["near"])
    hop(ra, 3)
    lax.fori_loop(7, 8, grad_step, 0)
    hop(rb, 1)
    hop(rc, 1)
    land(1)
    land(2)
    start(mo)
    land(3)
    arrive(ft)

    rs = []
    for dx in (2, 1, 3, 0):
        q = lax.rem(x + dx, 4)
        kind = lax.div(q, 2)
        basis = fall[kind].reshape(D, RANK)
        rows = pl.ds(pl.multiple_of(q * 256, 256), 256)
        low_t = jnp.dot(grad_t[rows, :], basis, preferred_element_type=F32)
        part[q] = low_t.T.astype(BF).reshape(4, 64, 256)
        for k, (a, b) in enumerate(XY):
            if a == dx:
                cp = remote(part.at[q, lax.rem(y + b, 4)], rsb.at[k], rs_s.at[k], rs_r.at[k], at(a, b, 0))
                cp.start()
                rs.append(cp)

    arrive(ra[3])
    start(quarters["below"], quarters["above"])
    hop(rb, 2)
    hop(rc, 2)

    keep_f = pltpu.make_async_copy(fall, f_out, s_loc.at[11])
    keep_f.start()

    grams = []
    for kind in range(2):
        basis = fall[kind].reshape(D, RANK)
        g = lax.dot_general(basis, basis, (((0,), (0,)), ((), ())), preferred_element_type=F32)
        hi = g.astype(BF)
        grams.append((hi, (g - hi.astype(F32)).astype(BF)))

    start(wholes["below"], wholes["above"])
    total = part[x, y].astype(F32)
    for cp in rs:
        cp.wait_recv()
    for k in range(15):
        total = total + rsb[k].astype(F32)
    zb[z] = total.astype(BF)
    zs = [remote(zb.at[z], zb.at[z], zb_s.at[k], zb_r.at[k], at(0, 0, d)) for k, d in enumerate(ZD)]
    for cp in zs:
        cp.start()
    hop(rb, 3)
    arrive(quarters["above"])
    start(acrosses["above"])
    hop(rc, 3)
    arrive(quarters["below"])
    for cp in mo:
        cp.wait_recv()
    first = mom[:, 0].reshape(64, 256)
    second = mom[:, 1].reshape(64, 256)
    for cp in zs:
        cp.wait_recv()
    low = zb[0].astype(F32)
    for k in range(1, 8):
        low = low + zb[k].astype(F32)
    first_new = 0.8 * first + 0.2 * low
    second_new = 0.95 * second + 0.05 * low * low
    nb[x, y] = (first_new / jnp.sqrt(second_new)).astype(BF)
    ag = [
        remote(nb.at[x, y], nb.at[x, y], ag_s.at[k], ag_r.at[k], at(a, b, 0))
        for k, (a, b) in enumerate(XY)
    ]
    for cp in ag:
        cp.start()

    start(acrosses["below"])

    part_low = low.reshape(8, 8, 256)
    mine = jnp.zeros((8, 256), F32)
    for k in range(8):
        mine = jnp.where(z == k, part_low[k], mine)
    lowb[x] = mine
    lo = [remote(lowb.at[x], lowb.at[x], lo_s.at[k], lo_r.at[k], at(a, 0, 0)) for k, a in enumerate((2, 1, 3))]
    for cp in lo:
        cp.start()

    for cp in ag:
        cp.wait_recv()
    keep_n = pltpu.make_async_copy(nb, n_out, s_loc.at[12])
    keep_n.start()
    for kind in range(2):
        acc = jnp.zeros((8, 128), F32)
        for q in (2 * kind, 2 * kind + 1):
            normed = nb[q].reshape(RANK, 256)
            t = jnp.dot(grams[kind][0], normed, preferred_element_type=F32)
            t = t + jnp.dot(grams[kind][1], normed, preferred_element_type=F32)
            s = jnp.sum((t * normed.astype(F32)).reshape(32, 8, 256), axis=0)
            acc = acc + s[:, :128] + s[:, 128:]
        sqb[c, kind] = acc
    sq = remote(sqb.at[c], sqb.at[c], sq_s, sq_r, at(0, 0, 0, 1))
    sq.start()
    for cp in lo:
        cp.wait_recv()
    keep_low = pltpu.make_async_copy(lowb, low_out, s_loc.at[13])
    keep_low.start()
    sq.wait_recv()
    keep_sq = pltpu.make_async_copy(sqb, sq_out, s_loc.at[14])
    keep_sq.start()
    arrive(rb[3], rc[3], *wholes.values(), *acrosses.values())
    rings = [cp for h in (*ra, *rb, *rc) for cp in h]
    spread = [cp for d in (quarters, wholes, acrosses) for cps in d.values() for cp in cps]
    relays = [cp for cps in (*fc, *fd) for cp in cps]
    for cp in (*fz, *mo, *by, *rings, *fa, *fb, *relays, *ft, *rs, *spread, *zs, *ag, *lo, sq):
        cp.wait_send()
    for cp in (keep_f, keep_n, keep_low, keep_sq):
        cp.wait()


def gathered(x, ci, cg, im, gm, inf, gf, i1, i2, g1, g2):
    sem = pltpu.SemaphoreType.DMA
    return pl.pallas_call(
        move_kernel,
        name="move",
        out_shape=(
            jax.ShapeDtypeStruct((NZ, NY, 64, W), BF),
            jax.ShapeDtypeStruct((2, NZ, NY, NX, 16, RANK), BF),
            jax.ShapeDtypeStruct((NX, NY, 64, 256), BF),
            jax.ShapeDtypeStruct((NX, 8, 256), F32),
            jax.ShapeDtypeStruct((2, 2, 8, 128), F32),
        ),
        in_specs=[pl.BlockSpec(memory_space=ANY)] * 11,
        out_specs=[pl.BlockSpec(memory_space=ANY)] * 5,
        scratch_shapes=[
            pltpu.VMEM((1024, D), BF),
            pltpu.VMEM((2, 1024, 512), BF),
            pltpu.VMEM((1024, 1024), BF),
            pltpu.VMEM((1024, D), BF),
            pltpu.VMEM((64, RANK), BF),
            pltpu.VMEM((4, 16, RANK), BF),
            pltpu.VMEM((2, NZ, NY, NX, 16, RANK), BF),
            pltpu.VMEM((2, 64, 512), F32),
            pltpu.VMEM((64, W), BF),
            pltpu.VMEM((4, 8, 512), F32),
            pltpu.VMEM((4, 2, 8, 256), F32),
            pltpu.VMEM((NZ, 2, 8, 256), F32),
            pltpu.VMEM((NX, NY, 64, 256), BF),
            pltpu.VMEM((15, 64, 256), BF),
            pltpu.VMEM((NZ, 64, 256), BF),
            pltpu.VMEM((NX, NY, 64, 256), BF),
            pltpu.VMEM((NX, 8, 256), F32),
            pltpu.VMEM((2, 2, 8, 128), F32),
            sem((15,)),
            *[sem((n,)) for n in (7, 7, 7, 7)],
            *[sem((4, 2))] * 6,
            *[sem((3,))] * 6,
            *[sem((4, 3))] * 4,
            *[sem((n,)) for n in (32, 32, 18, 18, 27, 27, 15, 15, 7, 7, 3, 3, 15, 15)],
            sem,
            sem,
        ],
        compiler_params=pltpu.CompilerParams(
            collective_id=0, has_side_effects=True, vmem_limit_bytes=VMEM
        ),
        cost_estimate=pl.CostEstimate(flops=6 * 10**9, bytes_accessed=16 * 2**20, transcendentals=0),
    )(x, ci, cg, im, gm, inf, gf, i1, i2, g1, g2)


def write_kernel(
    f_hbm, n_hbm, m_hbm, sq_hbm, low_ref, im_ref, gm_ref, i1_ref, i2_ref, g1_ref, g2_ref,
    im_out, gm_out, iu_out, gu_out, i1_out, i2_out, g1_out, g2_out, ic_out, gc_out,
    fv, nv, mv, sqv, cv, s_f, s_n, s_m, s_c,
):
    _, y, z, _ = where_am_i()
    order = (HERE, 2, 4, 1, 5, 0, 6, 7)
    row = [lax.rem(z + k + 8 - HERE, 8) for k in range(8)]
    loads = [pltpu.make_async_copy(sq_hbm, sqv, s_n.at[0]), pltpu.make_async_copy(n_hbm, nv, s_n.at[1])]
    for cp in loads:
        cp.start()
    fs = [pltpu.make_async_copy(f_hbm.at[:, row[k]], fv.at[k], s_f.at[k]) for k in range(8)]
    ms = [pltpu.make_async_copy(m_hbm.at[k], mv.at[k], s_m.at[k]) for k in range(8)]
    for k in order:
        fs[k].start()
        ms[k].start()

    for kind, (f_old, s_old, f_new, s_new) in enumerate(
        ((i1_ref, i2_ref, i1_out, i2_out), (g1_ref, g2_ref, g1_out, g2_out))
    ):
        for h in range(2):
            low = low_ref[2 * kind + h]
            cols = slice(256 * h, 256 * h + 256)
            f_new[:, cols] = 0.8 * f_old[:, cols] + 0.2 * low
            s_new[:, cols] = 0.95 * s_old[:, cols] + 0.05 * low * low

    loads[0].wait()
    scale = []
    for kind in range(2):
        square = jnp.sum(sqv[0, kind] + sqv[1, kind], axis=(0, 1), keepdims=True)
        scale.append(lax.rsqrt(square / (D * W) + 0.1))
    loads[1].wait()
    outs = []
    for k in order:
        fs[k].wait()
        if k == HERE:
            for kind, (old, new, upd) in enumerate(((im_ref, im_out, iu_out), (gm_ref, gm_out, gu_out))):
                basis = fv[k, kind, y].reshape(64, RANK)
                for h in range(2):
                    normed = nv[2 * kind + h].reshape(RANK, 256)
                    cols = slice(256 * h, 256 * h + 256)
                    u = jnp.dot(basis, normed, preferred_element_type=F32) * scale[kind]
                    upd[:, cols] = u
                    new[:, cols] = old[:, cols] - 0.05 * u
        ms[k].wait()
        for kind, out in enumerate((ic_out, gc_out)):
            basis = fv[k, kind].reshape(256, RANK)
            for h in range(2):
                normed = nv[2 * kind + h].reshape(RANK, 256)
                full = jnp.dot(basis, normed, preferred_element_type=F32)
                col = kind * 512 + 256 * h
                old = mv[k, :, :, col : col + 256].reshape(256, 256).astype(F32)
                cv[k, kind, :, 256 * h : 256 * h + 256] = (old - 0.05 * (full * scale[kind])).astype(BF)
            rows = pl.ds(pl.multiple_of(row[k] * 256, 256), 256)
            cp = pltpu.make_async_copy(cv.at[k, kind], out.at[rows, :], s_c.at[k, kind])
            cp.start()
            outs.append(cp)
    for cp in outs:
        cp.wait()


def written(f, n, m, sq, low, im, gm, i1, i2, g1, g2):
    sem, whole, kept = pltpu.SemaphoreType.DMA, pl.BlockSpec(memory_space=pltpu.VMEM), pl.BlockSpec(memory_space=ANY)
    return pl.pallas_call(
        write_kernel,
        name="write",
        out_shape=(
            *[jax.ShapeDtypeStruct((64, 512), F32)] * 4,
            *[jax.ShapeDtypeStruct((8, 512), F32)] * 4,
            *[jax.ShapeDtypeStruct((D, 512), BF)] * 2,
        ),
        in_specs=[kept] * 4 + [whole] * 7,
        out_specs=[whole] * 8 + [kept] * 2,
        scratch_shapes=[
            pltpu.VMEM((8, 2, NY, NX, 16, RANK), BF),
            pltpu.VMEM((NX, NY, 64, 256), BF),
            pltpu.VMEM((8, NY, 64, W), BF),
            pltpu.VMEM((2, 2, 8, 128), F32),
            pltpu.VMEM((8, 2, 256, 512), BF),
            sem((8,)),
            sem((2,)),
            sem((8,)),
            sem((8, 2)),
        ],
        compiler_params=pltpu.CompilerParams(vmem_limit_bytes=VMEM),
    )(f, n, m, sq, low, im, gm, i1, i2, g1, g2)


def on_device(x, ci, cg, im, gm, inf, gf, i1, i2, g1, g2):
    m, f, n, low, sq = gathered(x, ci, cg, im, gm, inf, gf, i1, i2, g1, g2)
    out = written(f, n, m, sq, low, im, gm, i1, i2, g1, g2)
    return tuple(out)


def solution(mesh):
    tokens, rows, moments = P(("fs", "rep"), "tp"), P("fs", "tp"), P("fs", "tp")
    return jax.shard_map(
        on_device,
        mesh=mesh,
        in_specs=(
            P(("fs", "rep"), None), tokens, tokens, rows, rows, P("fs", None), P("fs", None),
            moments, moments, moments, moments,
        ),
        out_specs=(rows,) * 4 + (moments,) * 4 + (P(None, "tp"),) * 2,
        check_vma=False,
    )
```

```python
import jax
import jax.numpy as jnp
from jax import lax
from jax.experimental import pallas as pl
from jax.experimental.pallas import tpu as pltpu
from jax.sharding import PartitionSpec as P

D = 2048
W = 1024
RANK = 256
NX, NY, NZ = 4, 4, 8
YZ_COLS, YZ0, YZ1 = pl.ds(0, 512), pl.ds(0, 256), pl.ds(256, 256)
ZY_COLS, ZYX_COLS, Z_COLS = pl.ds(512, 128), pl.ds(640, 384), pl.ds(512, 512)
HERE = 3
NEAR, BELOW, ABOVE = pl.ds(2, 3), pl.ds(0, 2), pl.ds(5, 3)
BF = jnp.bfloat16
F32 = jnp.float32
VMEM = 67_043_328
ANY = pl.ANY

XY = sorted(
    [(a, b) for a in range(4) for b in range(4) if (a, b) != (0, 0)],
    key=lambda o: -(min(o[0], 4 - o[0]) + min(o[1], 4 - o[1])),
)
ZD = sorted(range(1, 8), key=lambda d: -min(d, 8 - d))


def where_am_i():
    fs, x, c = lax.axis_index("fs"), lax.axis_index("rep"), lax.axis_index("tp")
    return x, lax.rem(fs, 4), lax.div(fs, 4), c


GROUPS = ("fz", "mo", "by", "ra", "rb", "rc", "fab", "fcd", "ft", "rs", "quarter", "whole", "across", "zs", "lo", "ag", "sq")
SEM = {name: k for k, name in enumerate(GROUPS)}


def take(region, sem):
    pltpu.make_async_copy(region, region, sem).wait()


def remote(src, dst, ss, rs, dev):
    return pltpu.make_async_remote_copy(
        src_ref=src,
        dst_ref=dst,
        send_sem=ss,
        recv_sem=rs,
        device_id=dev,
        device_id_type=pl.DeviceIdType.MESH,
    )


def move_kernel(
    x_hbm, ci_hbm, cg_hbm, im_hbm, gm_hbm, if_hbm, gf_hbm, i1_hbm, i2_hbm, g1_hbm, g2_hbm,
    m_out, f_out, n_out, low_out, sq_out,
    xv, cot, cot_t, grad_t, fac, fsh, fall, mast, msh, mom_in, mom_own, mom,
    part, rsb, zb, nb, lowb, sqb,
    s_loc, sent, got, ring_got, pair_got, land_got, leg_got,
):
    x, y, z, c = where_am_i()

    def at(dx, dy, dz, dc=0):
        return {
            "fs": lax.rem(z + dz, 8) * 4 + lax.rem(y + dy, 4),
            "rep": lax.rem(x + dx, 4),
            "tp": lax.rem(c + dc, 2),
        }

    def s_of(name):
        return sent.at[SEM[name]]

    def g_of(name):
        return got.at[SEM[name]]

    @pl.when(c == 0)
    def _():
        pltpu.make_async_copy(if_hbm, fac, s_loc.at[0]).start()

    @pl.when(c == 1)
    def _():
        pltpu.make_async_copy(gf_hbm, fac, s_loc.at[0]).start()

    moms = [
        pltpu.make_async_copy(r, mom_in.at[k], s_loc.at[1 + k])
        for k, r in enumerate((i1_hbm, g1_hbm, i2_hbm, g2_hbm))
    ]
    masters = [
        pltpu.make_async_copy(r, mast.at[k], s_loc.at[5 + k]) for k, r in enumerate((im_hbm, gm_hbm))
    ]
    cots = [
        pltpu.make_async_copy(r, cot.at[k], s_loc.at[7 + k]) for k, r in enumerate((ci_hbm, cg_hbm))
    ]
    load_x = pltpu.make_async_copy(x_hbm, xv, s_loc.at[9])
    for cp in (*moms, *masters, *cots, load_x):
        cp.start()

    barrier = pltpu.get_barrier_semaphore()
    peers = [at(a, b, 0) for a, b in XY] + [at(0, 0, d) for d in ZD] + [at(0, 0, 0, 1)]
    for p in peers:
        pl.semaphore_signal(barrier, inc=1, device_id=p, device_id_type=pl.DeviceIdType.MESH)

    pltpu.make_async_copy(if_hbm, fac, s_loc.at[0]).wait()
    new = lax.broadcasted_iota(jnp.int32, (RANK, RANK), 1)
    old = lax.broadcasted_iota(jnp.int32, (RANK, RANK), 0)
    ny, nz, ni = lax.shift_right_logical(new, 6), (lax.shift_right_logical(new, 3) & 7), new & 7
    perm = jnp.where(old == (nz * 4 + ny) * 8 + ni, 1.0, 0.0).astype(BF)
    shard = jnp.dot(fac[...], perm, preferred_element_type=F32).astype(BF)
    fsh[...] = shard.reshape(4, 16, RANK)
    fall[c, z, y, x] = fsh[x]

    for cp in moms:
        cp.wait()
    for q in range(4):
        kind, col = q // 2, (q % 2) * 256
        mom_own[q, 0] = mom_in[kind, :, col : col + 256]
        mom_own[q, 1] = mom_in[2 + kind, :, col : col + 256]
    mom[z] = mom_own[x]

    for cp in masters:
        cp.wait()
    msh[:, :512] = mast[0].astype(BF)
    msh[:, 512:] = mast[1].astype(BF)
    keep_m = pltpu.make_async_copy(msh, m_out.at[HERE, y], s_loc.at[10])
    keep_m.start()

    pl.semaphore_wait(barrier, len(peers))

    fz = [
        remote(fsh.at[x], fall.at[c, z, y, x], s_of("fz"), g_of("fz"), at(0, 0, d))
        for k, d in enumerate(ZD)
    ]
    mo = [remote(mom_own.at[x], mom.at[z], s_of("mo"), g_of("mo"), at(0, 0, d)) for k, d in enumerate(ZD)]
    by = [
        remote(msh.at[:, YZ_COLS], m_out.at[HERE, y, :, YZ_COLS], s_of("by"), g_of("by"), at(0, b, 0))
        for k, b in enumerate((2, 1, 3))
    ]

    def ring(block, n):
        ss, rs = s_of(("ra", "rb", "rc")[n]), ring_got.at[n]
        hops = []
        for h in range(4):
            lower, upper = (pl.ds(0, 32), pl.ds(32, 32)) if h == 3 else (pl.ds(0, 64),) * 2
            up = (block(HERE - h, lower), block(HERE - h - 1 if h < 3 else HERE + 4, lower))
            down = (block(HERE + h, upper), block(HERE + h + 1, upper))
            hops.append(
                (
                    remote(*up, ss, rs.at[h], at(0, 0, 1)),
                    remote(*down, ss, rs.at[h], at(0, 0, 7)),
                )
            )
        return hops

    ra = ring(lambda k, rows: m_out.at[k, y, rows, Z_COLS], 0)
    rb = ring(lambda k, rows: m_out.at[k, :, rows, YZ0], 1)
    rc = ring(lambda k, rows: m_out.at[k, :, rows, YZ1], 2)
    every = pl.ds(0, 64)

    def ring_blocks(n, count):
        if n == 0:
            return m_out.at[pl.ds(0, count), y, :, Z_COLS]
        return m_out.at[pl.ds(0, count), :, :, (YZ0, YZ1)[n - 1]]

    def landed(n, h):
        take(ring_blocks(n, 2 if h < 3 else 1), ring_got.at[n, h])

    def hop(n, h):
        if h:
            landed(n, h - 1)
        for cp in (ra, rb, rc)[n][h]:
            cp.start()

    for cp in (*fz, *by):
        cp.start()
    keep_m.wait()
    hop(0, 0)

    rows16 = pl.ds(pl.multiple_of(x * 16, 16), 16)
    part_of = {"near": NEAR, "below": BELOW, "above": ABOVE}

    def along_y(group, rows, cols, name, rsem):
        block = m_out.at[part_of[group], y, rows, cols]
        return [
            remote(block, block, s_of(name), rsem, at(0, b, 0))
            for b in (2, 1, 3)
        ]

    def along_x(group):
        out = []
        for a in (2, 1, 3):
            for j in range(3):
                block = m_out.at[part_of[group], lax.rem(y + 1 + j, 4), rows16, ZYX_COLS]
                out.append(remote(block, block, s_of("across"), g_of("across"), at(a, 0, 0)))
        return out

    groups = ("near", "below", "above")
    quarters = {g: along_y(g, rows16, ZYX_COLS, "quarter", leg_got.at[k]) for k, g in enumerate(groups)}
    wholes = {g: along_y(g, every, ZY_COLS, "whole", g_of("whole")) for g in groups}
    acrosses = {g: along_x(g) for g in groups}

    def start(*lists):
        for cps in lists:
            for cp in cps:
                cp.start()

    def quarters_arrive(k):
        take(m_out.at[pl.ds(0, (3, 2, 3)[k]), pl.ds(0, 3), pl.ds(0, 16), ZYX_COLS], leg_got.at[k])

    for cp in cots:
        cp.wait()
    for k in range(2):
        cot_t[k * 512 : (k + 1) * 512, :] = cot[k].T
    load_x.wait()

    def grad_step(i, _):
        cols = pl.ds(pl.multiple_of(i * 256, 256), 256)
        grad_t[:, cols] = jnp.dot(cot_t[...], xv[:, cols], preferred_element_type=F32).astype(BF)
        return 0

    lax.fori_loop(0, 2, grad_step, 0)

    take(fall.at[c, pl.ds(0, 7), 0, 0], g_of("fz"))
    def piece(half, xs, ys):
        return fall.at[c, pl.ds(4 * half, 4), ys, xs]

    def send_piece(half, xs, ys, ss, rs, dev):
        block = piece(half, xs, ys)
        return remote(block, block, ss, rs, dev)

    def back(p, d):
        return lax.rem(p + 4 - d, 4)

    near = (1, 3, 2)
    fa = [send_piece(0, x, y, s_of("fab"), pair_got.at[k], at(0, b, 0)) for k, b in enumerate(near)]
    fb = [send_piece(1, x, y, s_of("fab"), pair_got.at[k], at(a, 0, 0)) for k, a in enumerate(near)]
    ysrc = [y] + [back(y, b) for b in near]
    xsrc = [x] + [back(x, a) for a in near]
    fc = [
        [send_piece(0, x, ys, s_of("fcd"), land_got.at[i], at(a, 0, 0)) for a in near]
        for i, ys in enumerate(ysrc)
    ]
    fd = [
        [send_piece(1, xs, y, s_of("fcd"), land_got.at[i], at(0, b, 0)) for b in near]
        for i, xs in enumerate(xsrc)
    ]

    def to_partner(half, xs, ys):
        send_piece(half, xs, ys, s_of("ft"), g_of("ft"), at(0, 0, 0, 1)).start()

    start(fa, fb, fc[0], fd[0])
    to_partner(0, x, y)
    to_partner(1, x, y)

    lax.fori_loop(2, 4, grad_step, 0)
    hop(0, 1)
    start(quarters["near"])
    take(m_out.at[0, pl.ds(0, 3), :, YZ_COLS], g_of("by"))
    hop(1, 0)

    def relay(k):
        take(fall.at[c, :, 0, 0], pair_got.at[k])
        start(fc[1 + k], fd[1 + k])
        to_partner(0, x, ysrc[1 + k])
        to_partner(1, xsrc[1 + k], y)

    relay(0)
    relay(1)
    lax.fori_loop(4, 5, grad_step, 0)
    relay(2)
    hop(0, 2)
    hop(2, 0)
    lax.fori_loop(5, 7, grad_step, 0)

    def land(i):
        take(fall.at[c, :, pl.ds(0, 3), 0], land_got.at[i])
        for k in range(3):
            to_partner(0, xsrc[1 + k], ysrc[i])
            to_partner(1, xsrc[i], ysrc[1 + k])

    land(0)
    quarters_arrive(0)
    start(acrosses["near"], wholes["near"])
    lax.fori_loop(7, 8, grad_step, 0)
    land(1)
    land(2)
    hop(0, 3)
    land(3)
    hop(1, 1)
    hop(2, 1)
    start(mo)
    take(fall.at[1 - c], g_of("ft"))

    for dx in (2, 1, 3, 0):
        q = lax.rem(x + dx, 4)
        kind = lax.div(q, 2)
        basis = fall[kind].reshape(D, RANK)
        rows = pl.ds(pl.multiple_of(q * 256, 256), 256)
        low_t = jnp.dot(grad_t[rows, :], basis, preferred_element_type=F32)
        part[q] = low_t.T.astype(BF).reshape(4, 64, 256)
        for k, (a, b) in enumerate(XY):
            if a == dx:
                remote(part.at[q, lax.rem(y + b, 4)], rsb.at[k], s_of("rs"), g_of("rs"), at(a, b, 0)).start()

    landed(0, 3)
    start(quarters["below"], quarters["above"])
    hop(1, 2)
    hop(2, 2)

    keep_f = pltpu.make_async_copy(fall, f_out, s_loc.at[11])
    keep_f.start()

    grams = []
    for kind in range(2):
        basis = fall[kind].reshape(D, RANK)
        g = lax.dot_general(basis, basis, (((0,), (0,)), ((), ())), preferred_element_type=F32)
        hi = g.astype(BF)
        grams.append((hi, (g - hi.astype(F32)).astype(BF)))

    start(wholes["below"], wholes["above"])
    total = part[x, y].astype(F32)
    take(rsb, g_of("rs"))
    for k in range(15):
        total = total + rsb[k].astype(F32)
    zb[z] = total.astype(BF)
    zs = [remote(zb.at[z], zb.at[z], s_of("zs"), g_of("zs"), at(0, 0, d)) for k, d in enumerate(ZD)]
    for cp in zs:
        cp.start()
    hop(1, 3)
    quarters_arrive(2)
    start(acrosses["above"])
    hop(2, 3)
    quarters_arrive(1)
    take(mom.at[pl.ds(0, 7)], g_of("mo"))
    first = mom[:, 0].reshape(64, 256)
    second = mom[:, 1].reshape(64, 256)
    take(zb.at[pl.ds(0, 7)], g_of("zs"))
    low = zb[0].astype(F32)
    for k in range(1, 8):
        low = low + zb[k].astype(F32)
    first_new = 0.8 * first + 0.2 * low
    second_new = 0.95 * second + 0.05 * low * low
    nb[x, y] = (first_new / jnp.sqrt(second_new)).astype(BF)
    ag = [
        remote(nb.at[x, y], nb.at[x, y], s_of("ag"), g_of("ag"), at(a, b, 0))
        for k, (a, b) in enumerate(XY)
    ]
    for cp in ag:
        cp.start()

    part_low = low.reshape(8, 8, 256)
    mine = jnp.zeros((8, 256), F32)
    for k in range(8):
        mine = jnp.where(z == k, part_low[k], mine)
    lowb[x] = mine
    lo = [remote(lowb.at[x], lowb.at[x], s_of("lo"), g_of("lo"), at(a, 0, 0)) for a in (2, 1, 3)]
    for cp in lo:
        cp.start()
    start(acrosses["below"])

    take(rsb, g_of("ag"))
    keep_n = pltpu.make_async_copy(nb, n_out, s_loc.at[12])
    keep_n.start()
    for kind in range(2):
        acc = jnp.zeros((8, 128), F32)
        for q in (2 * kind, 2 * kind + 1):
            normed = nb[q].reshape(RANK, 256)
            t = jnp.dot(grams[kind][0], normed, preferred_element_type=F32)
            t = t + jnp.dot(grams[kind][1], normed, preferred_element_type=F32)
            s = jnp.sum((t * normed.astype(F32)).reshape(32, 8, 256), axis=0)
            acc = acc + s[:, :128] + s[:, 128:]
        sqb[c, kind] = acc
    sq = remote(sqb.at[c], sqb.at[c], s_of("sq"), g_of("sq"), at(0, 0, 0, 1))
    sq.start()
    take(lowb.at[pl.ds(0, 3)], g_of("lo"))
    keep_low = pltpu.make_async_copy(lowb, low_out, s_loc.at[13])
    keep_low.start()
    take(sqb.at[0], g_of("sq"))
    keep_sq = pltpu.make_async_copy(sqb, sq_out, s_loc.at[14])
    keep_sq.start()
    landed(1, 3)
    landed(2, 3)
    spread = {
        "whole": m_out.at[:, pl.ds(0, 3), :, ZY_COLS],
        "across": m_out.at[:, pl.ds(0, 3), pl.ds(0, 48), ZYX_COLS],
    }
    for name, region in spread.items():
        take(region, g_of(name))
    gone = {
        "fz": fall.at[0, pl.ds(0, 7), 0, 0],
        "mo": mom.at[pl.ds(0, 7)],
        "by": m_out.at[0, pl.ds(0, 3), :, YZ_COLS],
        "ra": ring_blocks(0, 7),
        "rb": ring_blocks(1, 7),
        "rc": ring_blocks(2, 7),
        "fab": fall.at[0, :, pl.ds(0, 3), 0],
        "fcd": fall.at[0, :, :, pl.ds(0, 3)],
        "ft": fall.at[0],
        "rs": rsb,
        "quarter": m_out.at[:, pl.ds(0, 3), pl.ds(0, 16), ZYX_COLS],
        "zs": zb.at[pl.ds(0, 7)],
        "ag": rsb,
        "lo": lowb.at[pl.ds(0, 3)],
        "sq": sqb.at[0],
        **spread,
    }
    for name in GROUPS:
        take(gone[name], s_of(name))
    for cp in (keep_f, keep_n, keep_low, keep_sq):
        cp.wait()


def gathered(x, ci, cg, im, gm, inf, gf, i1, i2, g1, g2):
    sem = pltpu.SemaphoreType.DMA
    return pl.pallas_call(
        move_kernel,
        name="move",
        out_shape=(
            jax.ShapeDtypeStruct((NZ, NY, 64, W), BF),
            jax.ShapeDtypeStruct((2, NZ, NY, NX, 16, RANK), BF),
            jax.ShapeDtypeStruct((NX, NY, 64, 256), BF),
            jax.ShapeDtypeStruct((NX, 8, 256), F32),
            jax.ShapeDtypeStruct((2, 2, 8, 128), F32),
        ),
        in_specs=[pl.BlockSpec(memory_space=ANY)] * 11,
        out_specs=[pl.BlockSpec(memory_space=ANY)] * 5,
        scratch_shapes=[
            pltpu.VMEM((1024, D), BF),
            pltpu.VMEM((2, 1024, 512), BF),
            pltpu.VMEM((1024, 1024), BF),
            pltpu.VMEM((1024, D), BF),
            pltpu.VMEM((64, RANK), BF),
            pltpu.VMEM((4, 16, RANK), BF),
            pltpu.VMEM((2, NZ, NY, NX, 16, RANK), BF),
            pltpu.VMEM((2, 64, 512), F32),
            pltpu.VMEM((64, W), BF),
            pltpu.VMEM((4, 8, 512), F32),
            pltpu.VMEM((4, 2, 8, 256), F32),
            pltpu.VMEM((NZ, 2, 8, 256), F32),
            pltpu.VMEM((NX, NY, 64, 256), BF),
            pltpu.VMEM((15, 64, 256), BF),
            pltpu.VMEM((NZ, 64, 256), BF),
            pltpu.VMEM((NX, NY, 64, 256), BF),
            pltpu.VMEM((NX, 8, 256), F32),
            pltpu.VMEM((2, 2, 8, 128), F32),
            sem((15,)),
            sem((len(GROUPS),)),
            sem((len(GROUPS),)),
            sem((3, 4)),
            sem((3,)),
            sem((4,)),
            sem((3,)),
        ],
        compiler_params=pltpu.CompilerParams(
            collective_id=0, has_side_effects=True, vmem_limit_bytes=VMEM
        ),
        cost_estimate=pl.CostEstimate(flops=6 * 10**9, bytes_accessed=16 * 2**20, transcendentals=0),
    )(x, ci, cg, im, gm, inf, gf, i1, i2, g1, g2)


def write_kernel(
    f_hbm, n_hbm, m_hbm, sq_hbm, low_hbm, im_hbm, gm_hbm, i1_hbm, i2_hbm, g1_hbm, g2_hbm,
    im_out, gm_out, iu_out, gu_out, i1_out, i2_out, g1_out, g2_out, ic_out, gc_out,
    fv, nv, mv, sqv, lowv, old_v, new_v, upd_v, mom_v, mom_new, cv, s_f, s_m, s_in, s_c, s_out,
):
    _, y, z, _ = where_am_i()
    order = (HERE, 2, 4, 1, 5, 0, 6, 7)
    row = [lax.rem(z + k + 8 - HERE, 8) for k in range(8)]
    small = [
        (sq_hbm, sqv), (n_hbm, nv), (im_hbm, old_v.at[0]), (gm_hbm, old_v.at[1]), (low_hbm, lowv),
        *[(r, mom_v.at[k]) for k, r in enumerate((i1_hbm, i2_hbm, g1_hbm, g2_hbm))],
    ]
    small = [pltpu.make_async_copy(src, dst, s_in.at[k]) for k, (src, dst) in enumerate(small)]
    fs = [pltpu.make_async_copy(f_hbm.at[:, row[k]], fv.at[k], s_f.at[k]) for k in range(8)]
    ms = [pltpu.make_async_copy(m_hbm.at[k], mv.at[k], s_m.at[k]) for k in range(8)]
    small[0].start()
    small[1].start()
    fs[HERE].start()
    ms[HERE].start()
    for cp in small[2:]:
        cp.start()
    outs = []

    def put(src, dst, sem):
        cp = pltpu.make_async_copy(src, dst, sem)
        cp.start()
        outs.append(cp)

    small[0].wait()
    for k in order[1:]:
        fs[k].start()
        ms[k].start()
    scale = []
    for kind in range(2):
        square = jnp.sum(sqv[0, kind] + sqv[1, kind], axis=(0, 1), keepdims=True)
        scale.append(lax.rsqrt(square / (D * W) + 0.1))
    small[1].wait()
    for at, k in enumerate(order):
        fs[k].wait()
        ms[k].wait()
        for kind, out in enumerate((ic_out, gc_out)):
            basis = fv[k, kind].reshape(256, RANK)
            for h in range(2):
                normed = nv[2 * kind + h].reshape(RANK, 256)
                full = jnp.dot(basis, normed, preferred_element_type=F32)
                col = kind * 512 + 256 * h
                old = mv[k, :, :, col : col + 256].reshape(256, 256).astype(F32)
                cv[k, kind, :, 256 * h : 256 * h + 256] = (old - 0.05 * (full * scale[kind])).astype(BF)
            rows = pl.ds(pl.multiple_of(row[k] * 256, 256), 256)
            put(cv.at[k, kind], out.at[rows, :], s_c.at[k, kind])
        if at == 0:
            for cp in small[2:]:
                cp.wait()
            for kind, (new_out, upd_out) in enumerate(((im_out, iu_out), (gm_out, gu_out))):
                basis = fv[k, kind, y].reshape(64, RANK)
                for h in range(2):
                    normed = nv[2 * kind + h].reshape(RANK, 256)
                    cols = slice(256 * h, 256 * h + 256)
                    u = jnp.dot(basis, normed, preferred_element_type=F32) * scale[kind]
                    upd_v[kind, :, cols] = u
                    new_v[kind, :, cols] = old_v[kind, :, cols] - 0.05 * u
                put(upd_v.at[kind], upd_out, s_out.at[2 * kind])
                put(new_v.at[kind], new_out, s_out.at[2 * kind + 1])
            for kind, (first_out, second_out) in enumerate(((i1_out, i2_out), (g1_out, g2_out))):
                for h in range(2):
                    low = lowv[2 * kind + h]
                    cols = slice(256 * h, 256 * h + 256)
                    mom_new[2 * kind, :, cols] = 0.8 * mom_v[2 * kind, :, cols] + 0.2 * low
                    mom_new[2 * kind + 1, :, cols] = 0.95 * mom_v[2 * kind + 1, :, cols] + 0.05 * low * low
                put(mom_new.at[2 * kind], first_out, s_out.at[4 + 2 * kind])
                put(mom_new.at[2 * kind + 1], second_out, s_out.at[5 + 2 * kind])
    for cp in outs:
        cp.wait()


def written(f, n, m, sq, low, im, gm, i1, i2, g1, g2):
    sem, kept = pltpu.SemaphoreType.DMA, pl.BlockSpec(memory_space=ANY)
    return pl.pallas_call(
        write_kernel,
        name="write",
        out_shape=(
            *[jax.ShapeDtypeStruct((64, 512), F32)] * 4,
            *[jax.ShapeDtypeStruct((8, 512), F32)] * 4,
            *[jax.ShapeDtypeStruct((D, 512), BF)] * 2,
        ),
        in_specs=[kept] * 11,
        out_specs=[kept] * 10,
        scratch_shapes=[
            pltpu.VMEM((8, 2, NY, NX, 16, RANK), BF),
            pltpu.VMEM((NX, NY, 64, 256), BF),
            pltpu.VMEM((8, NY, 64, W), BF),
            pltpu.VMEM((2, 2, 8, 128), F32),
            pltpu.VMEM((NX, 8, 256), F32),
            *[pltpu.VMEM((2, 64, 512), F32)] * 3,
            *[pltpu.VMEM((4, 8, 512), F32)] * 2,
            pltpu.VMEM((8, 2, 256, 512), BF),
            *[sem((n,)) for n in (8, 8, 9)],
            sem((8, 2)),
            sem((8,)),
        ],
        compiler_params=pltpu.CompilerParams(vmem_limit_bytes=VMEM),
    )(f, n, m, sq, low, im, gm, i1, i2, g1, g2)


def on_device(x, ci, cg, im, gm, inf, gf, i1, i2, g1, g2):
    m, f, n, low, sq = gathered(x, ci, cg, im, gm, inf, gf, i1, i2, g1, g2)
    out = written(f, n, m, sq, low, im, gm, i1, i2, g1, g2)
    return tuple(out)


def solution(mesh):
    tokens, rows, moments = P(("fs", "rep"), "tp"), P("fs", "tp"), P("fs", "tp")
    return jax.shard_map(
        on_device,
        mesh=mesh,
        in_specs=(
            P(("fs", "rep"), None), tokens, tokens, rows, rows, P("fs", None), P("fs", None),
            moments, moments, moments, moments,
        ),
        out_specs=(rows,) * 4 + (moments,) * 4 + (P(None, "tp"),) * 2,
        check_vma=False,
    )
```

```python
import functools

import jax
import jax.numpy as jnp
from jax import lax
from jax.experimental import pallas as pl
from jax.experimental.pallas import tpu as pltpu
from jax.sharding import PartitionSpec as P

D = 2048
W = 1024
RANK = 256
NX, NY, NZ = 4, 4, 8
YZ_COLS, YZ0, YZ1 = pl.ds(0, 384), pl.ds(0, 256), pl.ds(256, 128)
ZY_COLS, ZYX_COLS, Z_COLS = pl.ds(384, 256), pl.ds(640, 384), pl.ds(384, 640)
HERE = 3
NEAR, BELOW, ABOVE = pl.ds(2, 3), pl.ds(0, 2), pl.ds(5, 3)
BF = jnp.bfloat16
F32 = jnp.float32
VMEM = 67_043_328
ANY = pl.ANY

XY = sorted(
    [(a, b) for a in range(4) for b in range(4) if (a, b) != (0, 0)],
    key=lambda o: -(min(o[0], 4 - o[0]) + min(o[1], 4 - o[1])),
)
ZD = sorted(range(1, 8), key=lambda d: -min(d, 8 - d))


def where_am_i():
    fs, x, c = lax.axis_index("fs"), lax.axis_index("rep"), lax.axis_index("tp")
    return x, lax.rem(fs, 4), lax.div(fs, 4), c


GROUPS = ("fz", "mo", "by", "ra", "rb", "rc", "fab", "fcd", "ft", "rs", "quarter", "whole", "across", "zs", "lo", "ag", "sq")
SEM = {name: k for k, name in enumerate(GROUPS)}


def take(region, sem):
    pltpu.make_async_copy(region, region, sem).wait()


def remote(src, dst, ss, rs, dev):
    return pltpu.make_async_remote_copy(
        src_ref=src,
        dst_ref=dst,
        send_sem=ss,
        recv_sem=rs,
        device_id=dev,
        device_id_type=pl.DeviceIdType.MESH,
    )


def move_kernel(
    x_hbm, ci_hbm, cg_hbm, im_hbm, gm_hbm, if_hbm, gf_hbm, i1_hbm, i2_hbm, g1_hbm, g2_hbm,
    m_out, f_out, n_out, low_out, sq_out,
    xv, cot, cot_t, grad_t, fac, fsh, fall, mast, msh, mom_in, mom_own, mom,
    part, rsb, zb, nb, lowb, sqb,
    s_loc, sent, got, ring_got, pair_got, land_got, leg_got,
):
    x, y, z, c = where_am_i()

    def at(dx, dy, dz, dc=0):
        return {
            "fs": lax.rem(z + dz, 8) * 4 + lax.rem(y + dy, 4),
            "rep": lax.rem(x + dx, 4),
            "tp": lax.rem(c + dc, 2),
        }

    def s_of(name):
        return sent.at[SEM[name]]

    def g_of(name):
        return got.at[SEM[name]]

    @pl.when(c == 0)
    def _():
        pltpu.make_async_copy(if_hbm, fac, s_loc.at[0]).start()

    @pl.when(c == 1)
    def _():
        pltpu.make_async_copy(gf_hbm, fac, s_loc.at[0]).start()

    moms = [
        pltpu.make_async_copy(r, mom_in.at[k], s_loc.at[1 + k])
        for k, r in enumerate((i1_hbm, g1_hbm, i2_hbm, g2_hbm))
    ]
    masters = [
        pltpu.make_async_copy(r, mast.at[k], s_loc.at[5 + k]) for k, r in enumerate((im_hbm, gm_hbm))
    ]
    cots = [
        pltpu.make_async_copy(r, cot.at[k], s_loc.at[7 + k]) for k, r in enumerate((ci_hbm, cg_hbm))
    ]
    load_x = pltpu.make_async_copy(x_hbm, xv, s_loc.at[9])
    for cp in (*moms, *masters, *cots, load_x):
        cp.start()

    barrier = pltpu.get_barrier_semaphore()
    peers = [at(a, b, 0) for a, b in XY] + [at(0, 0, d) for d in ZD] + [at(0, 0, 0, 1)]
    for p in peers:
        pl.semaphore_signal(barrier, inc=1, device_id=p, device_id_type=pl.DeviceIdType.MESH)

    pltpu.make_async_copy(if_hbm, fac, s_loc.at[0]).wait()
    new = lax.broadcasted_iota(jnp.int32, (RANK, RANK), 1)
    old = lax.broadcasted_iota(jnp.int32, (RANK, RANK), 0)
    ny, nz, ni = lax.shift_right_logical(new, 6), (lax.shift_right_logical(new, 3) & 7), new & 7
    perm = jnp.where(old == (nz * 4 + ny) * 8 + ni, 1.0, 0.0).astype(BF)
    shard = jnp.dot(fac[...], perm, preferred_element_type=F32).astype(BF)
    fsh[...] = shard.reshape(4, 16, RANK)
    fall[c, z, y, x] = fsh[x]

    for cp in moms:
        cp.wait()
    for q in range(4):
        kind, col = q // 2, (q % 2) * 256
        mom_own[q, 0] = mom_in[kind, :, col : col + 256]
        mom_own[q, 1] = mom_in[2 + kind, :, col : col + 256]
    mom[z] = mom_own[x]

    for cp in masters:
        cp.wait()
    msh[:, :512] = mast[0].astype(BF)
    msh[:, 512:] = mast[1].astype(BF)
    keep_m = pltpu.make_async_copy(msh, m_out.at[HERE, y], s_loc.at[10])
    keep_m.start()

    pl.semaphore_wait(barrier, len(peers))

    fz = [
        remote(fsh.at[x], fall.at[c, z, y, x], s_of("fz"), g_of("fz"), at(0, 0, d))
        for k, d in enumerate(ZD)
    ]
    mo = [remote(mom_own.at[x], mom.at[z], s_of("mo"), g_of("mo"), at(0, 0, d)) for k, d in enumerate(ZD)]
    by = [
        remote(msh.at[:, YZ_COLS], m_out.at[HERE, y, :, YZ_COLS], s_of("by"), g_of("by"), at(0, b, 0))
        for k, b in enumerate((2, 1, 3))
    ]

    def ring(block, n):
        ss, rs = s_of(("ra", "rb", "rc")[n]), ring_got.at[n]
        hops = []
        for h in range(4):
            lower, upper = (pl.ds(0, 32), pl.ds(32, 32)) if h == 3 else (pl.ds(0, 64),) * 2
            up = (block(HERE - h, lower), block(HERE - h - 1 if h < 3 else HERE + 4, lower))
            down = (block(HERE + h, upper), block(HERE + h + 1, upper))
            hops.append(
                (
                    remote(*up, ss, rs.at[h], at(0, 0, 1)),
                    remote(*down, ss, rs.at[h], at(0, 0, 7)),
                )
            )
        return hops

    ra = ring(lambda k, rows: m_out.at[k, y, rows, Z_COLS], 0)
    rb = ring(lambda k, rows: m_out.at[k, :, rows, YZ0], 1)
    rc = ring(lambda k, rows: m_out.at[k, :, rows, YZ1], 2)
    every = pl.ds(0, 64)

    def ring_blocks(n, count):
        if n == 0:
            return m_out.at[pl.ds(0, count), y, :, Z_COLS]
        return m_out.at[pl.ds(0, count), :, :, (YZ0, YZ1)[n - 1]]

    def landed(n, h):
        take(ring_blocks(n, 2 if h < 3 else 1), ring_got.at[n, h])

    def hop(n, h):
        if h:
            landed(n, h - 1)
        for cp in (ra, rb, rc)[n][h]:
            cp.start()

    for cp in (*fz, *by):
        cp.start()
    keep_m.wait()
    hop(0, 0)

    rows16 = pl.ds(pl.multiple_of(x * 16, 16), 16)
    part_of = {"near": NEAR, "below": BELOW, "above": ABOVE}

    def along_y(group, rows, cols, name, rsem):
        block = m_out.at[part_of[group], y, rows, cols]
        return [
            remote(block, block, s_of(name), rsem, at(0, b, 0))
            for b in (2, 1, 3)
        ]

    def along_x(group):
        out = []
        for a in (2, 1, 3):
            for j in range(3):
                block = m_out.at[part_of[group], lax.rem(y + 1 + j, 4), rows16, ZYX_COLS]
                out.append(remote(block, block, s_of("across"), g_of("across"), at(a, 0, 0)))
        return out

    groups = ("near", "below", "above")
    quarters = {g: along_y(g, rows16, ZYX_COLS, "quarter", leg_got.at[k]) for k, g in enumerate(groups)}
    wholes = {g: along_y(g, every, ZY_COLS, "whole", g_of("whole")) for g in groups}
    acrosses = {g: along_x(g) for g in groups}

    def start(*lists):
        for cps in lists:
            for cp in cps:
                cp.start()

    def quarters_arrive(k):
        take(m_out.at[pl.ds(0, (3, 2, 3)[k]), pl.ds(0, 3), pl.ds(0, 16), ZYX_COLS], leg_got.at[k])

    for cp in cots:
        cp.wait()
    for k in range(2):
        cot_t[k * 512 : (k + 1) * 512, :] = cot[k].T
    load_x.wait()

    def grad_step(i, _):
        cols = pl.ds(pl.multiple_of(i * 256, 256), 256)
        grad_t[:, cols] = jnp.dot(cot_t[...], xv[:, cols], preferred_element_type=F32).astype(BF)
        return 0

    lax.fori_loop(0, 2, grad_step, 0)

    take(fall.at[c, pl.ds(0, 7), 0, 0], g_of("fz"))
    def piece(half, xs, ys):
        return fall.at[c, pl.ds(4 * half, 4), ys, xs]

    def send_piece(half, xs, ys, ss, rs, dev):
        block = piece(half, xs, ys)
        return remote(block, block, ss, rs, dev)

    def back(p, d):
        return lax.rem(p + 4 - d, 4)

    near = (1, 3, 2)
    fa = [send_piece(0, x, y, s_of("fab"), pair_got.at[k], at(0, b, 0)) for k, b in enumerate(near)]
    fb = [send_piece(1, x, y, s_of("fab"), pair_got.at[k], at(a, 0, 0)) for k, a in enumerate(near)]
    ysrc = [y] + [back(y, b) for b in near]
    xsrc = [x] + [back(x, a) for a in near]
    fc = [
        [send_piece(0, x, ys, s_of("fcd"), land_got.at[i], at(a, 0, 0)) for a in near]
        for i, ys in enumerate(ysrc)
    ]
    fd = [
        [send_piece(1, xs, y, s_of("fcd"), land_got.at[i], at(0, b, 0)) for b in near]
        for i, xs in enumerate(xsrc)
    ]

    def to_partner(half, xs, ys):
        send_piece(half, xs, ys, s_of("ft"), g_of("ft"), at(0, 0, 0, 1)).start()

    start(fa, fb, fc[0], fd[0])
    to_partner(0, x, y)
    to_partner(1, x, y)

    lax.fori_loop(2, 4, grad_step, 0)
    hop(0, 1)
    take(m_out.at[0, pl.ds(0, 3), :, YZ_COLS], g_of("by"))
    hop(1, 0)

    def relay(k):
        take(fall.at[c, :, 0, 0], pair_got.at[k])
        start(fc[1 + k], fd[1 + k])
        to_partner(0, x, ysrc[1 + k])
        to_partner(1, xsrc[1 + k], y)

    relay(0)
    relay(1)
    start(quarters["near"])
    lax.fori_loop(4, 5, grad_step, 0)
    relay(2)
    hop(0, 2)
    hop(2, 0)
    lax.fori_loop(5, 7, grad_step, 0)

    def land(i):
        take(fall.at[c, :, pl.ds(0, 3), 0], land_got.at[i])
        for k in range(3):
            to_partner(0, xsrc[1 + k], ysrc[i])
            to_partner(1, xsrc[i], ysrc[1 + k])

    land(0)
    lax.fori_loop(7, 8, grad_step, 0)
    land(1)
    hop(0, 3)
    land(2)
    quarters_arrive(0)
    land(3)
    start(acrosses["near"], wholes["near"])
    hop(1, 1)

    for n in range(4):
        if n == 2:
            hop(2, 1)
            start(mo)
            take(fall.at[1 - c], g_of("ft"))
        kind = c if n < 2 else 1 - c
        q = 2 * kind + n % 2
        basis = fall[kind].reshape(D, RANK)
        rows = pl.ds(pl.multiple_of(q * 256, 256), 256)
        low_t = jnp.dot(grad_t[rows, :], basis, preferred_element_type=F32)
        part[q] = low_t.T.astype(BF).reshape(4, 64, 256)
        a = lax.rem(q + 4 - x, 4)

        def send_part(b):
            slot = a * 4 + b - 1
            dev = {"fs": z * 4 + lax.rem(y + b, 4), "rep": q, "tp": c}
            remote(part.at[q, lax.rem(y + b, 4)], rsb.at[slot], s_of("rs"), g_of("rs"), dev).start()

        for b in (2, 1, 3):
            send_part(b)
        pl.when(q != x)(functools.partial(send_part, 0))

    landed(0, 3)
    start(quarters["below"], quarters["above"])
    hop(1, 2)
    hop(2, 2)

    keep_f = pltpu.make_async_copy(fall, f_out, s_loc.at[11])
    keep_f.start()

    grams = []
    for kind in range(2):
        basis = fall[kind].reshape(D, RANK)
        g = lax.dot_general(basis, basis, (((0,), (0,)), ((), ())), preferred_element_type=F32)
        hi = g.astype(BF)
        grams.append((hi, (g - hi.astype(F32)).astype(BF)))

    start(wholes["below"], wholes["above"])
    total = part[x, y].astype(F32)
    take(rsb, g_of("rs"))
    for k in range(15):
        total = total + rsb[k].astype(F32)
    zb[z] = total.astype(BF)
    zs = [remote(zb.at[z], zb.at[z], s_of("zs"), g_of("zs"), at(0, 0, d)) for k, d in enumerate(ZD)]
    for cp in zs:
        cp.start()
    hop(1, 3)
    quarters_arrive(2)
    start(acrosses["above"])
    hop(2, 3)
    quarters_arrive(1)
    take(mom.at[pl.ds(0, 7)], g_of("mo"))
    first = mom[:, 0].reshape(64, 256)
    second = mom[:, 1].reshape(64, 256)
    take(zb.at[pl.ds(0, 7)], g_of("zs"))
    low = zb[0].astype(F32)
    for k in range(1, 8):
        low = low + zb[k].astype(F32)
    first_new = 0.8 * first + 0.2 * low
    second_new = 0.95 * second + 0.05 * low * low
    nb[x, y] = (first_new / jnp.sqrt(second_new)).astype(BF)
    ag = [
        remote(nb.at[x, y], nb.at[x, y], s_of("ag"), g_of("ag"), at(a, b, 0))
        for k, (a, b) in enumerate(XY)
    ]
    for cp in ag:
        cp.start()

    part_low = low.reshape(8, 8, 256)
    mine = jnp.zeros((8, 256), F32)
    for k in range(8):
        mine = jnp.where(z == k, part_low[k], mine)
    lowb[x] = mine
    lo = [remote(lowb.at[x], lowb.at[x], s_of("lo"), g_of("lo"), at(a, 0, 0)) for a in (2, 1, 3)]
    for cp in lo:
        cp.start()
    start(acrosses["below"])

    take(rsb, g_of("ag"))
    keep_n = pltpu.make_async_copy(nb, n_out, s_loc.at[12])
    keep_n.start()
    for kind in range(2):
        acc = jnp.zeros((8, 128), F32)
        for q in (2 * kind, 2 * kind + 1):
            normed = nb[q].reshape(RANK, 256)
            t = jnp.dot(grams[kind][0], normed, preferred_element_type=F32)
            t = t + jnp.dot(grams[kind][1], normed, preferred_element_type=F32)
            s = jnp.sum((t * normed.astype(F32)).reshape(32, 8, 256), axis=0)
            acc = acc + s[:, :128] + s[:, 128:]
        sqb[c, kind] = acc
    sq = remote(sqb.at[c], sqb.at[c], s_of("sq"), g_of("sq"), at(0, 0, 0, 1))
    sq.start()
    take(lowb.at[pl.ds(0, 3)], g_of("lo"))
    keep_low = pltpu.make_async_copy(lowb, low_out, s_loc.at[13])
    keep_low.start()
    take(sqb.at[0], g_of("sq"))
    keep_sq = pltpu.make_async_copy(sqb, sq_out, s_loc.at[14])
    keep_sq.start()
    landed(1, 3)
    landed(2, 3)
    spread = {
        "whole": m_out.at[:, pl.ds(0, 3), :, ZY_COLS],
        "across": m_out.at[:, pl.ds(0, 3), pl.ds(0, 48), ZYX_COLS],
    }
    for name, region in spread.items():
        take(region, g_of(name))
    gone = {
        "fz": fall.at[0, pl.ds(0, 7), 0, 0],
        "mo": mom.at[pl.ds(0, 7)],
        "by": m_out.at[0, pl.ds(0, 3), :, YZ_COLS],
        "ra": ring_blocks(0, 7),
        "rb": ring_blocks(1, 7),
        "rc": ring_blocks(2, 7),
        "fab": fall.at[0, :, pl.ds(0, 3), 0],
        "fcd": fall.at[0, :, :, pl.ds(0, 3)],
        "ft": fall.at[0],
        "rs": rsb,
        "quarter": m_out.at[:, pl.ds(0, 3), pl.ds(0, 16), ZYX_COLS],
        "zs": zb.at[pl.ds(0, 7)],
        "ag": rsb,
        "lo": lowb.at[pl.ds(0, 3)],
        "sq": sqb.at[0],
        **spread,
    }
    for name in GROUPS:
        take(gone[name], s_of(name))
    for cp in (keep_f, keep_n, keep_low, keep_sq):
        cp.wait()


def gathered(x, ci, cg, im, gm, inf, gf, i1, i2, g1, g2):
    sem = pltpu.SemaphoreType.DMA
    return pl.pallas_call(
        move_kernel,
        name="move",
        out_shape=(
            jax.ShapeDtypeStruct((NZ, NY, 64, W), BF),
            jax.ShapeDtypeStruct((2, NZ, NY, NX, 16, RANK), BF),
            jax.ShapeDtypeStruct((NX, NY, 64, 256), BF),
            jax.ShapeDtypeStruct((NX, 8, 256), F32),
            jax.ShapeDtypeStruct((2, 2, 8, 128), F32),
        ),
        in_specs=[pl.BlockSpec(memory_space=ANY)] * 11,
        out_specs=[pl.BlockSpec(memory_space=ANY)] * 5,
        scratch_shapes=[
            pltpu.VMEM((1024, D), BF),
            pltpu.VMEM((2, 1024, 512), BF),
            pltpu.VMEM((1024, 1024), BF),
            pltpu.VMEM((1024, D), BF),
            pltpu.VMEM((64, RANK), BF),
            pltpu.VMEM((4, 16, RANK), BF),
            pltpu.VMEM((2, NZ, NY, NX, 16, RANK), BF),
            pltpu.VMEM((2, 64, 512), F32),
            pltpu.VMEM((64, W), BF),
            pltpu.VMEM((4, 8, 512), F32),
            pltpu.VMEM((4, 2, 8, 256), F32),
            pltpu.VMEM((NZ, 2, 8, 256), F32),
            pltpu.VMEM((NX, NY, 64, 256), BF),
            pltpu.VMEM((15, 64, 256), BF),
            pltpu.VMEM((NZ, 64, 256), BF),
            pltpu.VMEM((NX, NY, 64, 256), BF),
            pltpu.VMEM((NX, 8, 256), F32),
            pltpu.VMEM((2, 2, 8, 128), F32),
            sem((15,)),
            sem((len(GROUPS),)),
            sem((len(GROUPS),)),
            sem((3, 4)),
            sem((3,)),
            sem((4,)),
            sem((3,)),
        ],
        compiler_params=pltpu.CompilerParams(
            collective_id=0, has_side_effects=True, vmem_limit_bytes=VMEM
        ),
        cost_estimate=pl.CostEstimate(flops=6 * 10**9, bytes_accessed=16 * 2**20, transcendentals=0),
    )(x, ci, cg, im, gm, inf, gf, i1, i2, g1, g2)


def write_kernel(
    f_hbm, n_hbm, m_hbm, sq_hbm, low_hbm, im_hbm, gm_hbm, i1_hbm, i2_hbm, g1_hbm, g2_hbm,
    im_out, gm_out, iu_out, gu_out, i1_out, i2_out, g1_out, g2_out, ic_out, gc_out,
    fv, nv, mv, sqv, lowv, old_v, new_v, upd_v, mom_v, mom_new, cv, s_f, s_m, s_in, s_c, s_out,
):
    _, y, z, _ = where_am_i()
    order = (2, 3, 4, 5, 0, 1, 6, 7)
    row = [lax.rem(z + k + 8 - HERE, 8) for k in range(8)]
    small = [
        (sq_hbm, sqv), (n_hbm, nv), (im_hbm, old_v.at[0]), (gm_hbm, old_v.at[1]), (low_hbm, lowv),
        *[(r, mom_v.at[k]) for k, r in enumerate((i1_hbm, i2_hbm, g1_hbm, g2_hbm))],
    ]
    small = [pltpu.make_async_copy(src, dst, s_in.at[k]) for k, (src, dst) in enumerate(small)]
    fs = [pltpu.make_async_copy(f_hbm.at[:, row[k]], fv.at[k], s_f.at[k]) for k in range(8)]
    ms = [pltpu.make_async_copy(m_hbm.at[k], mv.at[k], s_m.at[k]) for k in range(8)]
    small[0].start()
    small[1].start()
    for k in order[:2]:
        fs[k].start()
        ms[k].start()
    for cp in small[2:]:
        cp.start()
    outs = []

    def put(src, dst, sem):
        cp = pltpu.make_async_copy(src, dst, sem)
        cp.start()
        outs.append(cp)

    small[0].wait()
    for k in order[2:]:
        fs[k].start()
        ms[k].start()
    scale = []
    for kind in range(2):
        square = jnp.sum(sqv[0, kind] + sqv[1, kind], axis=(0, 1), keepdims=True)
        scale.append(lax.rsqrt(square / (D * W) + 0.1))
    small[1].wait()
    for at, k in enumerate(order[::2]):
        for i in (k, k + 1):
            fs[i].wait()
            ms[i].wait()
        for kind, out in enumerate((ic_out, gc_out)):
            basis = fv[k : k + 2, kind].reshape(512, RANK)
            for h in range(2):
                normed = nv[2 * kind + h].reshape(RANK, 256)
                full = jnp.dot(basis, normed, preferred_element_type=F32)
                col = kind * 512 + 256 * h
                old = mv[k : k + 2, :, :, col : col + 256].reshape(512, 256).astype(F32)
                new = (old - full * (0.05 * scale[kind])).astype(BF)
                cv[k : k + 2, kind, :, 256 * h : 256 * h + 256] = new.reshape(2, 256, 256)
            for i in (k, k + 1):
                rows = pl.ds(pl.multiple_of(row[i] * 256, 256), 256)
                put(cv.at[i, kind], out.at[rows, :], s_c.at[i, kind])
        if at == 0:
            for cp in small[2:]:
                cp.wait()
            for kind, (new_out, upd_out) in enumerate(((im_out, iu_out), (gm_out, gu_out))):
                basis = fv[HERE, kind, y].reshape(64, RANK)
                for h in range(2):
                    normed = nv[2 * kind + h].reshape(RANK, 256)
                    cols = slice(256 * h, 256 * h + 256)
                    u = jnp.dot(basis, normed, preferred_element_type=F32) * scale[kind]
                    upd_v[kind, :, cols] = u
                    new_v[kind, :, cols] = old_v[kind, :, cols] - 0.05 * u
                put(upd_v.at[kind], upd_out, s_out.at[2 * kind])
                put(new_v.at[kind], new_out, s_out.at[2 * kind + 1])
            for kind, (first_out, second_out) in enumerate(((i1_out, i2_out), (g1_out, g2_out))):
                for h in range(2):
                    low = lowv[2 * kind + h]
                    cols = slice(256 * h, 256 * h + 256)
                    mom_new[2 * kind, :, cols] = 0.8 * mom_v[2 * kind, :, cols] + 0.2 * low
                    mom_new[2 * kind + 1, :, cols] = 0.95 * mom_v[2 * kind + 1, :, cols] + 0.05 * low * low
                put(mom_new.at[2 * kind], first_out, s_out.at[4 + 2 * kind])
                put(mom_new.at[2 * kind + 1], second_out, s_out.at[5 + 2 * kind])
    for cp in outs:
        cp.wait()


def written(f, n, m, sq, low, im, gm, i1, i2, g1, g2):
    sem, kept = pltpu.SemaphoreType.DMA, pl.BlockSpec(memory_space=ANY)
    return pl.pallas_call(
        write_kernel,
        name="write",
        out_shape=(
            *[jax.ShapeDtypeStruct((64, 512), F32)] * 4,
            *[jax.ShapeDtypeStruct((8, 512), F32)] * 4,
            *[jax.ShapeDtypeStruct((D, 512), BF)] * 2,
        ),
        in_specs=[kept] * 11,
        out_specs=[kept] * 10,
        scratch_shapes=[
            pltpu.VMEM((8, 2, NY, NX, 16, RANK), BF),
            pltpu.VMEM((NX, NY, 64, 256), BF),
            pltpu.VMEM((8, NY, 64, W), BF),
            pltpu.VMEM((2, 2, 8, 128), F32),
            pltpu.VMEM((NX, 8, 256), F32),
            *[pltpu.VMEM((2, 64, 512), F32)] * 3,
            *[pltpu.VMEM((4, 8, 512), F32)] * 2,
            pltpu.VMEM((8, 2, 256, 512), BF),
            *[sem((n,)) for n in (8, 8, 9)],
            sem((8, 2)),
            sem((8,)),
        ],
        compiler_params=pltpu.CompilerParams(vmem_limit_bytes=VMEM),
    )(f, n, m, sq, low, im, gm, i1, i2, g1, g2)


def on_device(x, ci, cg, im, gm, inf, gf, i1, i2, g1, g2):
    m, f, n, low, sq = gathered(x, ci, cg, im, gm, inf, gf, i1, i2, g1, g2)
    out = written(f, n, m, sq, low, im, gm, i1, i2, g1, g2)
    return tuple(out)


def solution(mesh):
    tokens, rows, moments = P(("fs", "rep"), "tp"), P("fs", "tp"), P("fs", "tp")
    return jax.shard_map(
        on_device,
        mesh=mesh,
        in_specs=(
            P(("fs", "rep"), None), tokens, tokens, rows, rows, P("fs", None), P("fs", None),
            moments, moments, moments, moments,
        ),
        out_specs=(rows,) * 4 + (moments,) * 4 + (P(None, "tp"),) * 2,
        check_vma=False,
    )
```

```python
import functools

import jax
import jax.numpy as jnp
from jax import lax
from jax.experimental import pallas as pl
from jax.experimental.pallas import tpu as pltpu
from jax.sharding import PartitionSpec as P

D = 2048
W = 1024
RANK = 256
NX, NY, NZ = 4, 4, 8
YZ_COLS, YZ0, YZ1 = pl.ds(0, 512), pl.ds(0, 256), pl.ds(256, 256)
ZY_COLS, ZYX_COLS, Z_COLS = pl.ds(512, 128), pl.ds(640, 384), pl.ds(512, 512)
HERE = 3
NEAR, BELOW, ABOVE = pl.ds(2, 3), pl.ds(0, 2), pl.ds(5, 3)
BF = jnp.bfloat16
F32 = jnp.float32
VMEM = 67_043_328
KEPT = (6 * 1024 + 512 + 32 + 16) * 1024
ANY = pl.ANY

XY = sorted(
    [(a, b) for a in range(4) for b in range(4) if (a, b) != (0, 0)],
    key=lambda o: -(min(o[0], 4 - o[0]) + min(o[1], 4 - o[1])),
)
ZD = sorted(range(1, 8), key=lambda d: -min(d, 8 - d))


def where_am_i():
    fs, x, c = lax.axis_index("fs"), lax.axis_index("rep"), lax.axis_index("tp")
    return x, lax.rem(fs, 4), lax.div(fs, 4), c


GROUPS = ("fz", "mo", "by", "ra", "rb", "rc", "fab", "fcd", "ft", "rs", "quarter", "whole", "across", "zs", "lo", "nab", "ncd", "sq")
SEM = {name: k for k, name in enumerate(GROUPS)}


def take(region, sem):
    pltpu.make_async_copy(region, region, sem).wait()


def remote(src, dst, ss, rs, dev):
    return pltpu.make_async_remote_copy(
        src_ref=src,
        dst_ref=dst,
        send_sem=ss,
        recv_sem=rs,
        device_id=dev,
        device_id_type=pl.DeviceIdType.MESH,
    )


def move_kernel(
    x_hbm, ci_hbm, cg_hbm, im_hbm, gm_hbm, if_hbm, gf_hbm, i1_hbm, i2_hbm, g1_hbm, g2_hbm,
    m_out, fall, nb, lowb, sqb,
    xv, cot, cot_t, grad_t, fac, fsh, mast, msh, mom_in, mom_own, mom,
    part, rsb, zb,
    s_loc, sent, got, ring_got, pair_got, land_got, leg_got, npair_got,
):
    x, y, z, c = where_am_i()

    def at(dx, dy, dz, dc=0):
        return {
            "fs": lax.rem(z + dz, 8) * 4 + lax.rem(y + dy, 4),
            "rep": lax.rem(x + dx, 4),
            "tp": lax.rem(c + dc, 2),
        }

    def s_of(name):
        return sent.at[SEM[name]]

    def g_of(name):
        return got.at[SEM[name]]

    @pl.when(c == 0)
    def _():
        pltpu.make_async_copy(if_hbm, fac, s_loc.at[0]).start()

    @pl.when(c == 1)
    def _():
        pltpu.make_async_copy(gf_hbm, fac, s_loc.at[0]).start()

    moms = [
        pltpu.make_async_copy(r, mom_in.at[k], s_loc.at[1 + k])
        for k, r in enumerate((i1_hbm, g1_hbm, i2_hbm, g2_hbm))
    ]
    masters = [
        pltpu.make_async_copy(r, mast.at[k], s_loc.at[5 + k]) for k, r in enumerate((im_hbm, gm_hbm))
    ]
    cots = [
        pltpu.make_async_copy(r, cot.at[k], s_loc.at[7 + k]) for k, r in enumerate((ci_hbm, cg_hbm))
    ]
    load_x = pltpu.make_async_copy(x_hbm, xv, s_loc.at[9])
    for cp in (*moms, *masters, *cots, load_x):
        cp.start()

    barrier = pltpu.get_barrier_semaphore()
    peers = [at(a, b, 0) for a, b in XY] + [at(0, 0, d) for d in ZD] + [at(0, 0, 0, 1)]
    for p in peers:
        pl.semaphore_signal(barrier, inc=1, device_id=p, device_id_type=pl.DeviceIdType.MESH)

    pltpu.make_async_copy(if_hbm, fac, s_loc.at[0]).wait()
    new = lax.broadcasted_iota(jnp.int32, (RANK, RANK), 1)
    old = lax.broadcasted_iota(jnp.int32, (RANK, RANK), 0)
    ny, nz, ni = lax.shift_right_logical(new, 6), (lax.shift_right_logical(new, 3) & 7), new & 7
    perm = jnp.where(old == (nz * 4 + ny) * 8 + ni, 1.0, 0.0).astype(BF)
    shard = jnp.dot(fac[...], perm, preferred_element_type=F32).astype(BF)
    fsh[...] = shard.reshape(4, 16, RANK)
    fall[c, z, y, x] = fsh[x]

    for cp in moms:
        cp.wait()
    for q in range(4):
        kind, col = q // 2, (q % 2) * 256
        mom_own[q, 0] = mom_in[kind, :, col : col + 256]
        mom_own[q, 1] = mom_in[2 + kind, :, col : col + 256]
    mom[z] = mom_own[x]

    for cp in masters:
        cp.wait()
    msh[:, :512] = mast[0].astype(BF)
    msh[:, 512:] = mast[1].astype(BF)
    m_out[HERE, y] = msh[...]

    pl.semaphore_wait(barrier, len(peers))

    fz = [
        remote(fsh.at[x], fall.at[c, z, y, x], s_of("fz"), g_of("fz"), at(0, 0, d))
        for k, d in enumerate(ZD)
    ]
    mo = [remote(mom_own.at[x], mom.at[z], s_of("mo"), g_of("mo"), at(0, 0, d)) for k, d in enumerate(ZD)]
    by = [
        remote(msh.at[:, YZ_COLS], m_out.at[HERE, y, :, YZ_COLS], s_of("by"), g_of("by"), at(0, b, 0))
        for k, b in enumerate((2, 1, 3))
    ]

    def ring(block, n):
        ss, rs = s_of(("ra", "rb", "rc")[n]), ring_got.at[n]
        hops = []
        for h in range(4):
            lower, upper = (pl.ds(0, 32), pl.ds(32, 32)) if h == 3 else (pl.ds(0, 64),) * 2
            up = (block(HERE - h, lower), block(HERE - h - 1 if h < 3 else HERE + 4, lower))
            down = (block(HERE + h, upper), block(HERE + h + 1, upper))
            hops.append(
                (
                    remote(*up, ss, rs.at[h], at(0, 0, 1)),
                    remote(*down, ss, rs.at[h], at(0, 0, 7)),
                )
            )
        return hops

    ra = ring(lambda k, rows: m_out.at[k, y, rows, Z_COLS], 0)
    rb = ring(lambda k, rows: m_out.at[k, :, rows, YZ0], 1)
    rc = ring(lambda k, rows: m_out.at[k, :, rows, YZ1], 2)
    every = pl.ds(0, 64)

    def ring_blocks(n, count):
        if n == 0:
            return m_out.at[pl.ds(0, count), y, :, Z_COLS]
        return m_out.at[pl.ds(0, count), :, :, (YZ0, YZ1)[n - 1]]

    def landed(n, h):
        take(ring_blocks(n, 2 if h < 3 else 1), ring_got.at[n, h])

    def hop(n, h):
        if h:
            landed(n, h - 1)
        for cp in (ra, rb, rc)[n][h]:
            cp.start()

    for cp in (*fz, *by):
        cp.start()
    hop(0, 0)

    rows16 = pl.ds(pl.multiple_of(x * 16, 16), 16)
    part_of = {"near": NEAR, "below": BELOW, "above": ABOVE}

    def along_y(group, rows, cols, name, rsem):
        block = m_out.at[part_of[group], y, rows, cols]
        return [
            remote(block, block, s_of(name), rsem, at(0, b, 0))
            for b in (2, 1, 3)
        ]

    def along_x(group):
        out = []
        for a in (2, 1, 3):
            for j in range(3):
                block = m_out.at[part_of[group], lax.rem(y + 1 + j, 4), rows16, ZYX_COLS]
                out.append(remote(block, block, s_of("across"), g_of("across"), at(a, 0, 0)))
        return out

    groups = ("near", "below", "above")
    quarters = {g: along_y(g, rows16, ZYX_COLS, "quarter", leg_got.at[k]) for k, g in enumerate(groups)}
    wholes = {g: along_y(g, every, ZY_COLS, "whole", g_of("whole")) for g in groups}
    acrosses = {g: along_x(g) for g in groups}

    def start(*lists):
        for cps in lists:
            for cp in cps:
                cp.start()

    def quarters_arrive(k):
        take(m_out.at[pl.ds(0, (3, 2, 3)[k]), pl.ds(0, 3), pl.ds(0, 16), ZYX_COLS], leg_got.at[k])

    for cp in cots:
        cp.wait()
    for k in range(2):
        cot_t[k * 512 : (k + 1) * 512, :] = cot[k].T
    load_x.wait()

    def grad_step(i, _):
        cols = pl.ds(pl.multiple_of(i * 256, 256), 256)
        grad_t[:, cols] = jnp.dot(cot_t[...], xv[:, cols], preferred_element_type=F32).astype(BF)
        return 0

    lax.fori_loop(0, 2, grad_step, 0)

    take(fall.at[c, pl.ds(0, 7), 0, 0], g_of("fz"))
    def piece(half, xs, ys):
        return fall.at[c, pl.ds(4 * half, 4), ys, xs]

    def send_piece(half, xs, ys, ss, rs, dev):
        block = piece(half, xs, ys)
        return remote(block, block, ss, rs, dev)

    def back(p, d):
        return lax.rem(p + 4 - d, 4)

    near = (1, 3, 2)
    fa = [send_piece(0, x, y, s_of("fab"), pair_got.at[k], at(0, b, 0)) for k, b in enumerate(near)]
    fb = [send_piece(1, x, y, s_of("fab"), pair_got.at[k], at(a, 0, 0)) for k, a in enumerate(near)]
    ysrc = [y] + [back(y, b) for b in near]
    xsrc = [x] + [back(x, a) for a in near]
    fc = [
        [send_piece(0, x, ys, s_of("fcd"), land_got.at[i], at(a, 0, 0)) for a in near]
        for i, ys in enumerate(ysrc)
    ]
    fd = [
        [send_piece(1, xs, y, s_of("fcd"), land_got.at[i], at(0, b, 0)) for b in near]
        for i, xs in enumerate(xsrc)
    ]

    def to_partner(half, xs, ys):
        send_piece(half, xs, ys, s_of("ft"), g_of("ft"), at(0, 0, 0, 1)).start()

    start(fa, fb, fc[0], fd[0])
    to_partner(0, x, y)
    to_partner(1, x, y)

    lax.fori_loop(2, 4, grad_step, 0)
    hop(0, 1)
    take(m_out.at[0, pl.ds(0, 3), :, YZ_COLS], g_of("by"))
    hop(1, 0)

    def relay(k):
        take(fall.at[c, :, 0, 0], pair_got.at[k])
        start(fc[1 + k], fd[1 + k])
        to_partner(0, x, ysrc[1 + k])
        to_partner(1, xsrc[1 + k], y)

    relay(0)
    relay(1)
    start(quarters["near"])
    lax.fori_loop(4, 5, grad_step, 0)
    relay(2)
    hop(0, 2)
    hop(2, 0)
    lax.fori_loop(5, 7, grad_step, 0)

    def land(i):
        take(fall.at[c, :, pl.ds(0, 3), 0], land_got.at[i])
        for k in range(3):
            to_partner(0, xsrc[1 + k], ysrc[i])
            to_partner(1, xsrc[i], ysrc[1 + k])

    land(0)
    lax.fori_loop(7, 8, grad_step, 0)
    land(1)
    hop(0, 3)
    land(2)
    quarters_arrive(0)
    land(3)
    start(acrosses["near"], wholes["near"])
    hop(1, 1)

    for n in range(4):
        if n == 2:
            start(mo)
            take(fall.at[1 - c], g_of("ft"))
        kind = c if n < 2 else 1 - c
        q = 2 * kind + n % 2
        basis = fall[kind].reshape(D, RANK)
        rows = pl.ds(pl.multiple_of(q * 256, 256), 256)
        low_t = jnp.dot(grad_t[rows, :], basis, preferred_element_type=F32)
        part[q] = low_t.T.astype(BF).reshape(4, 64, 256)
        a = lax.rem(q + 4 - x, 4)

        def send_part(b):
            slot = a * 4 + b - 1
            dev = {"fs": z * 4 + lax.rem(y + b, 4), "rep": q, "tp": c}
            remote(part.at[q, lax.rem(y + b, 4)], rsb.at[slot], s_of("rs"), g_of("rs"), dev).start()

        for b in (2, 1, 3):
            send_part(b)
        pl.when(q != x)(functools.partial(send_part, 0))

    landed(0, 3)
    start(quarters["below"], quarters["above"])
    hop(2, 1)
    hop(1, 2)

    grams = []
    for kind in range(2):
        basis = fall[kind].reshape(D, RANK)
        g = lax.dot_general(basis, basis, (((0,), (0,)), ((), ())), preferred_element_type=F32)
        hi = g.astype(BF)
        grams.append((hi, (g - hi.astype(F32)).astype(BF)))

    start(wholes["below"], wholes["above"])
    total = part[x, y].astype(F32)
    take(rsb, g_of("rs"))
    for k in range(15):
        total = total + rsb[k].astype(F32)
    zb[z] = total.astype(BF)
    zs = [remote(zb.at[z], zb.at[z], s_of("zs"), g_of("zs"), at(0, 0, d)) for k, d in enumerate(ZD)]
    for cp in zs:
        cp.start()
    quarters_arrive(2)
    start(acrosses["above"])
    quarters_arrive(1)
    take(mom.at[pl.ds(0, 7)], g_of("mo"))
    first = mom[:, 0].reshape(64, 256)
    second = mom[:, 1].reshape(64, 256)
    take(zb.at[pl.ds(0, 7)], g_of("zs"))
    hop(2, 2)
    hop(1, 3)
    low = zb[0].astype(F32)
    for k in range(1, 8):
        low = low + zb[k].astype(F32)
    first_new = 0.8 * first + 0.2 * low
    second_new = 0.95 * second + 0.05 * low * low
    nb[x, y] = (first_new / jnp.sqrt(second_new)).astype(BF)
    halves = (pl.ds(0, 32), pl.ds(32, 32))

    def normed_piece(half, xs, ys, name, rsem, dev):
        block = nb.at[xs, ys, halves[half]]
        return remote(block, block, s_of(name), rsem, dev)

    na = [normed_piece(0, x, y, "nab", npair_got.at[k], at(0, b, 0)) for k, b in enumerate(near)]
    nbb = [normed_piece(1, x, y, "nab", npair_got.at[k], at(a, 0, 0)) for k, a in enumerate(near)]
    nc = [[normed_piece(0, x, ys, "ncd", g_of("ncd"), at(a, 0, 0)) for a in near] for ys in ysrc]
    nd = [[normed_piece(1, xs, y, "ncd", g_of("ncd"), at(0, b, 0)) for b in near] for xs in xsrc]
    start(na, nbb, nc[0], nd[0])

    part_low = low.reshape(8, 8, 256)
    mine = jnp.zeros((8, 256), F32)
    for k in range(8):
        mine = jnp.where(z == k, part_low[k], mine)
    lowb[x] = mine
    lo = [remote(lowb.at[x], lowb.at[x], s_of("lo"), g_of("lo"), at(a, 0, 0)) for a in (2, 1, 3)]
    for cp in lo:
        cp.start()

    for k in range(3):
        take(nb.at[0, 0], npair_got.at[k])
        start(nc[1 + k], nd[1 + k])
    start(acrosses["below"])
    hop(2, 3)
    take(nb.at[pl.ds(0, 3)], g_of("ncd"))
    for kind in range(2):
        acc = jnp.zeros((8, 128), F32)
        for q in (2 * kind, 2 * kind + 1):
            normed = nb[q].reshape(RANK, 256)
            t = jnp.dot(grams[kind][0], normed, preferred_element_type=F32)
            t = t + jnp.dot(grams[kind][1], normed, preferred_element_type=F32)
            s = jnp.sum((t * normed.astype(F32)).reshape(32, 8, 256), axis=0)
            acc = acc + s[:, :128] + s[:, 128:]
        sqb[c, kind] = acc
    sq = remote(sqb.at[c], sqb.at[c], s_of("sq"), g_of("sq"), at(0, 0, 0, 1))
    sq.start()
    take(lowb.at[pl.ds(0, 3)], g_of("lo"))
    take(sqb.at[0], g_of("sq"))
    landed(1, 3)
    landed(2, 3)
    spread = {
        "whole": m_out.at[:, pl.ds(0, 3), :, ZY_COLS],
        "across": m_out.at[:, pl.ds(0, 3), pl.ds(0, 48), ZYX_COLS],
    }
    for name, region in spread.items():
        take(region, g_of(name))
    gone = {
        "fz": fall.at[0, pl.ds(0, 7), 0, 0],
        "mo": mom.at[pl.ds(0, 7)],
        "by": m_out.at[0, pl.ds(0, 3), :, YZ_COLS],
        "ra": ring_blocks(0, 7),
        "rb": ring_blocks(1, 7),
        "rc": ring_blocks(2, 7),
        "fab": fall.at[0, :, pl.ds(0, 3), 0],
        "fcd": fall.at[0, :, :, pl.ds(0, 3)],
        "ft": fall.at[0],
        "rs": rsb,
        "quarter": m_out.at[:, pl.ds(0, 3), pl.ds(0, 16), ZYX_COLS],
        "zs": zb.at[pl.ds(0, 7)],
        "nab": nb.at[0, pl.ds(0, 3)],
        "ncd": nb.at[pl.ds(0, 3)],
        "lo": lowb.at[pl.ds(0, 3)],
        "sq": sqb.at[0],
        **spread,
    }
    for name in GROUPS:
        take(gone[name], s_of(name))


def gathered(x, ci, cg, im, gm, inf, gf, i1, i2, g1, g2):
    sem = pltpu.SemaphoreType.DMA
    return pl.pallas_call(
        move_kernel,
        name="move",
        out_shape=(
            pltpu.VMEM((NZ, NY, 64, W), BF),
            pltpu.VMEM((2, NZ, NY, NX, 16, RANK), BF),
            pltpu.VMEM((NX, NY, 64, 256), BF),
            pltpu.VMEM((NX, 8, 256), F32),
            pltpu.VMEM((2, 2, 8, 128), F32),
        ),
        in_specs=[pl.BlockSpec(memory_space=ANY)] * 11,
        out_specs=[pl.BlockSpec(memory_space=pltpu.VMEM)] * 5,
        scratch_shapes=[
            pltpu.VMEM((1024, D), BF),
            pltpu.VMEM((2, 1024, 512), BF),
            pltpu.VMEM((1024, 1024), BF),
            pltpu.VMEM((1024, D), BF),
            pltpu.VMEM((64, RANK), BF),
            pltpu.VMEM((4, 16, RANK), BF),
            pltpu.VMEM((2, 64, 512), F32),
            pltpu.VMEM((64, W), BF),
            pltpu.VMEM((4, 8, 512), F32),
            pltpu.VMEM((4, 2, 8, 256), F32),
            pltpu.VMEM((NZ, 2, 8, 256), F32),
            pltpu.VMEM((NX, NY, 64, 256), BF),
            pltpu.VMEM((15, 64, 256), BF),
            pltpu.VMEM((NZ, 64, 256), BF),
            sem((10,)),
            sem((len(GROUPS),)),
            sem((len(GROUPS),)),
            sem((3, 4)),
            sem((3,)),
            sem((4,)),
            sem((3,)),
            sem((3,)),
        ],
        compiler_params=pltpu.CompilerParams(
            collective_id=0, has_side_effects=True, vmem_limit_bytes=VMEM - KEPT
        ),
        cost_estimate=pl.CostEstimate(flops=6 * 10**9, bytes_accessed=16 * 2**20, transcendentals=0),
    )(x, ci, cg, im, gm, inf, gf, i1, i2, g1, g2)


def write_kernel(
    fv, nv, mv, sqv, lowv, im_hbm, gm_hbm, i1_hbm, i2_hbm, g1_hbm, g2_hbm,
    im_out, gm_out, iu_out, gu_out, i1_out, i2_out, g1_out, g2_out, ic_out, gc_out,
    old_v, new_v, upd_v, mom_v, mom_new, cv, s_in, s_c, s_out,
):
    _, y, z, _ = where_am_i()
    order = (2, 3, 4, 5, 0, 1, 6, 7)
    row = [lax.rem(z + k + 8 - HERE, 8) for k in range(8)]
    small = [
        (im_hbm, old_v.at[0]), (gm_hbm, old_v.at[1]),
        *[(r, mom_v.at[k]) for k, r in enumerate((i1_hbm, i2_hbm, g1_hbm, g2_hbm))],
    ]
    small = [pltpu.make_async_copy(src, dst, s_in.at[k]) for k, (src, dst) in enumerate(small)]
    for cp in small:
        cp.start()
    outs = []

    def put(src, dst, sem):
        cp = pltpu.make_async_copy(src, dst, sem)
        cp.start()
        outs.append(cp)

    scale = []
    for kind in range(2):
        square = jnp.sum(sqv[0, kind] + sqv[1, kind], axis=(0, 1), keepdims=True)
        scale.append(lax.rsqrt(square / (D * W) + 0.1))
    for at, k in enumerate(order[::2]):
        for kind, out in enumerate((ic_out, gc_out)):
            basis = jnp.concatenate([fv[kind, row[i]].reshape(256, RANK) for i in (k, k + 1)], axis=0)
            for h in range(2):
                normed = nv[2 * kind + h].reshape(RANK, 256)
                full = jnp.dot(basis, normed, preferred_element_type=F32)
                col = kind * 512 + 256 * h
                old = mv[k : k + 2, :, :, col : col + 256].reshape(512, 256).astype(F32)
                new = (old - full * (0.05 * scale[kind])).astype(BF)
                cv[k : k + 2, kind, :, 256 * h : 256 * h + 256] = new.reshape(2, 256, 256)
            for i in (k, k + 1):
                rows = pl.ds(pl.multiple_of(row[i] * 256, 256), 256)
                put(cv.at[i, kind], out.at[rows, :], s_c.at[i, kind])
        if at == 0:
            for cp in small:
                cp.wait()
            for kind, (new_out, upd_out) in enumerate(((im_out, iu_out), (gm_out, gu_out))):
                basis = fv[kind, z, y].reshape(64, RANK)
                for h in range(2):
                    normed = nv[2 * kind + h].reshape(RANK, 256)
                    cols = slice(256 * h, 256 * h + 256)
                    u = jnp.dot(basis, normed, preferred_element_type=F32) * scale[kind]
                    upd_v[kind, :, cols] = u
                    new_v[kind, :, cols] = old_v[kind, :, cols] - 0.05 * u
                put(upd_v.at[kind], upd_out, s_out.at[2 * kind])
                put(new_v.at[kind], new_out, s_out.at[2 * kind + 1])
            for kind, (first_out, second_out) in enumerate(((i1_out, i2_out), (g1_out, g2_out))):
                for h in range(2):
                    low = lowv[2 * kind + h]
                    cols = slice(256 * h, 256 * h + 256)
                    mom_new[2 * kind, :, cols] = 0.8 * mom_v[2 * kind, :, cols] + 0.2 * low
                    mom_new[2 * kind + 1, :, cols] = 0.95 * mom_v[2 * kind + 1, :, cols] + 0.05 * low * low
                put(mom_new.at[2 * kind], first_out, s_out.at[4 + 2 * kind])
                put(mom_new.at[2 * kind + 1], second_out, s_out.at[5 + 2 * kind])
    for cp in outs:
        cp.wait()


def written(f, n, m, sq, low, im, gm, i1, i2, g1, g2):
    sem, kept = pltpu.SemaphoreType.DMA, pl.BlockSpec(memory_space=ANY)
    held = pl.BlockSpec(memory_space=pltpu.VMEM)
    return pl.pallas_call(
        write_kernel,
        name="write",
        out_shape=(
            *[jax.ShapeDtypeStruct((64, 512), F32)] * 4,
            *[jax.ShapeDtypeStruct((8, 512), F32)] * 4,
            *[jax.ShapeDtypeStruct((D, 512), BF)] * 2,
        ),
        in_specs=[held] * 5 + [kept] * 6,
        out_specs=[kept] * 10,
        scratch_shapes=[
            *[pltpu.VMEM((2, 64, 512), F32)] * 3,
            *[pltpu.VMEM((4, 8, 512), F32)] * 2,
            pltpu.VMEM((8, 2, 256, 512), BF),
            sem((6,)),
            sem((8, 2)),
            sem((8,)),
        ],
        compiler_params=pltpu.CompilerParams(vmem_limit_bytes=VMEM - KEPT),
    )(f, n, m, sq, low, im, gm, i1, i2, g1, g2)


def on_device(x, ci, cg, im, gm, inf, gf, i1, i2, g1, g2):
    m, f, n, low, sq = gathered(x, ci, cg, im, gm, inf, gf, i1, i2, g1, g2)
    f, n, m, sq, low = (pltpu.with_memory_space_constraint(a, pltpu.VMEM) for a in (f, n, m, sq, low))
    out = written(f, n, m, sq, low, im, gm, i1, i2, g1, g2)
    return tuple(out)


def solution(mesh):
    tokens, rows, moments = P(("fs", "rep"), "tp"), P("fs", "tp"), P("fs", "tp")
    return jax.shard_map(
        on_device,
        mesh=mesh,
        in_specs=(
            P(("fs", "rep"), None), tokens, tokens, rows, rows, P("fs", None), P("fs", None),
            moments, moments, moments, moments,
        ),
        out_specs=(rows,) * 4 + (moments,) * 4 + (P(None, "tp"),) * 2,
        check_vma=False,
    )
```

```python
import functools

import jax
import jax.numpy as jnp
from jax import lax
from jax.experimental import pallas as pl
from jax.experimental.pallas import tpu as pltpu
from jax.sharding import PartitionSpec as P

D = 2048
W = 1024
RANK = 256
NX, NY, NZ = 4, 4, 8
YZ_COLS, YZ0, YZ1 = pl.ds(0, 512), pl.ds(0, 256), pl.ds(256, 256)
ZY_COLS, ZYX_COLS, Z_COLS = pl.ds(512, 128), pl.ds(640, 384), pl.ds(512, 512)
HERE = 3
NEAR, BELOW, ABOVE = pl.ds(2, 3), pl.ds(0, 2), pl.ds(5, 3)
BF = jnp.bfloat16
F32 = jnp.float32
VMEM = 67_043_328
KEPT = (6 * 1024 + 512 + 32 + 16) * 1024
ANY = pl.ANY

XY = sorted(
    [(a, b) for a in range(4) for b in range(4) if (a, b) != (0, 0)],
    key=lambda o: -(min(o[0], 4 - o[0]) + min(o[1], 4 - o[1])),
)
ZD = sorted(range(1, 8), key=lambda d: -min(d, 8 - d))


def where_am_i():
    fs, x, c = lax.axis_index("fs"), lax.axis_index("rep"), lax.axis_index("tp")
    return x, lax.rem(fs, 4), lax.div(fs, 4), c


GROUPS = ("fz", "mo", "by", "ra", "rb", "rc", "fab", "fcd", "ft", "rs", "quarter", "whole", "across", "zs", "lo", "nab", "ncd", "sq")
SEM = {name: k for k, name in enumerate(GROUPS)}


def take(region, sem):
    pltpu.make_async_copy(region, region, sem).wait()


def remote(src, dst, ss, rs, dev):
    return pltpu.make_async_remote_copy(
        src_ref=src,
        dst_ref=dst,
        send_sem=ss,
        recv_sem=rs,
        device_id=dev,
        device_id_type=pl.DeviceIdType.MESH,
    )


def move_kernel(
    x_hbm, ci_hbm, cg_hbm, im_hbm, gm_hbm, if_hbm, gf_hbm, i1_hbm, i2_hbm, g1_hbm, g2_hbm,
    m_out, fall, nb, lowb, sqb,
    xv, cot, cot_t, grad_t, fac, fsh, mast, msh, mom_in, mom_own, mom,
    part, rsb, zb,
    s_loc, sent, got, ring_got, pair_got, land_got, leg_got, npair_got,
):
    x, y, z, c = where_am_i()

    def at(dx, dy, dz, dc=0):
        return {
            "fs": lax.rem(z + dz, 8) * 4 + lax.rem(y + dy, 4),
            "rep": lax.rem(x + dx, 4),
            "tp": lax.rem(c + dc, 2),
        }

    def s_of(name):
        return sent.at[SEM[name]]

    def g_of(name):
        return got.at[SEM[name]]

    @pl.when(c == 0)
    def _():
        pltpu.make_async_copy(if_hbm, fac, s_loc.at[0]).start()

    @pl.when(c == 1)
    def _():
        pltpu.make_async_copy(gf_hbm, fac, s_loc.at[0]).start()

    moms = [
        pltpu.make_async_copy(r, mom_in.at[k], s_loc.at[1 + k])
        for k, r in enumerate((i1_hbm, g1_hbm, i2_hbm, g2_hbm))
    ]
    masters = [
        pltpu.make_async_copy(r, mast.at[k], s_loc.at[5 + k]) for k, r in enumerate((im_hbm, gm_hbm))
    ]
    cots = [
        pltpu.make_async_copy(r, cot.at[k], s_loc.at[7 + k]) for k, r in enumerate((ci_hbm, cg_hbm))
    ]
    load_x = pltpu.make_async_copy(x_hbm, xv, s_loc.at[9])
    for cp in (*moms, *masters, *cots, load_x):
        cp.start()

    barrier = pltpu.get_barrier_semaphore()
    peers = [at(a, b, 0) for a, b in XY] + [at(0, 0, d) for d in ZD] + [at(0, 0, 0, 1)]
    for p in peers:
        pl.semaphore_signal(barrier, inc=1, device_id=p, device_id_type=pl.DeviceIdType.MESH)

    pltpu.make_async_copy(if_hbm, fac, s_loc.at[0]).wait()
    new = lax.broadcasted_iota(jnp.int32, (RANK, RANK), 1)
    old = lax.broadcasted_iota(jnp.int32, (RANK, RANK), 0)
    ny, nz, ni = lax.shift_right_logical(new, 6), (lax.shift_right_logical(new, 3) & 7), new & 7
    perm = jnp.where(old == (nz * 4 + ny) * 8 + ni, 1.0, 0.0).astype(BF)
    shard = jnp.dot(fac[...], perm, preferred_element_type=F32).astype(BF)
    fsh[...] = shard.reshape(4, 16, RANK)
    fall[c, z, y, x] = fsh[x]

    for cp in moms:
        cp.wait()
    for q in range(4):
        kind, col = q // 2, (q % 2) * 256
        mom_own[q, 0] = mom_in[kind, :, col : col + 256]
        mom_own[q, 1] = mom_in[2 + kind, :, col : col + 256]
    mom[z] = mom_own[x]

    for cp in masters:
        cp.wait()
    msh[:, :512] = mast[0].astype(BF)
    msh[:, 512:] = mast[1].astype(BF)
    m_out[HERE, y] = msh[...]

    pl.semaphore_wait(barrier, len(peers))

    fz = [
        remote(fsh.at[x], fall.at[c, z, y, x], s_of("fz"), g_of("fz"), at(0, 0, d))
        for k, d in enumerate(ZD)
    ]
    mo = [remote(mom_own.at[x], mom.at[z], s_of("mo"), g_of("mo"), at(0, 0, d)) for k, d in enumerate(ZD)]
    by = [
        remote(msh.at[:, YZ_COLS], m_out.at[HERE, y, :, YZ_COLS], s_of("by"), g_of("by"), at(0, b, 0))
        for k, b in enumerate((2, 1, 3))
    ]

    def ring(block, n):
        ss, rs = s_of(("ra", "rb", "rc")[n]), ring_got.at[n]
        hops = []
        for h in range(4):
            lower, upper = (pl.ds(0, 32), pl.ds(32, 32)) if h == 3 else (pl.ds(0, 64),) * 2
            up = (block(HERE - h, lower), block(HERE - h - 1 if h < 3 else HERE + 4, lower))
            down = (block(HERE + h, upper), block(HERE + h + 1, upper))
            hops.append(
                (
                    remote(*up, ss, rs.at[h], at(0, 0, 1)),
                    remote(*down, ss, rs.at[h], at(0, 0, 7)),
                )
            )
        return hops

    ra = ring(lambda k, rows: m_out.at[k, y, rows, Z_COLS], 0)
    rb = ring(lambda k, rows: m_out.at[k, :, rows, YZ0], 1)
    rc = ring(lambda k, rows: m_out.at[k, :, rows, YZ1], 2)
    every = pl.ds(0, 64)

    def ring_blocks(n, count):
        if n == 0:
            return m_out.at[pl.ds(0, count), y, :, Z_COLS]
        return m_out.at[pl.ds(0, count), :, :, (YZ0, YZ1)[n - 1]]

    def landed(n, h):
        take(ring_blocks(n, 2 if h < 3 else 1), ring_got.at[n, h])

    def hop(n, h):
        if h:
            landed(n, h - 1)
        for cp in (ra, rb, rc)[n][h]:
            cp.start()

    for cp in (*fz, *by):
        cp.start()
    hop(0, 0)

    rows16 = pl.ds(pl.multiple_of(x * 16, 16), 16)
    part_of = {"near": NEAR, "below": BELOW, "above": ABOVE}

    def along_y(group, rows, cols, name, rsem):
        block = m_out.at[part_of[group], y, rows, cols]
        return [
            remote(block, block, s_of(name), rsem, at(0, b, 0))
            for b in (2, 1, 3)
        ]

    def along_x(group):
        out = []
        for a in (2, 1, 3):
            for j in range(3):
                block = m_out.at[part_of[group], lax.rem(y + 1 + j, 4), rows16, ZYX_COLS]
                out.append(remote(block, block, s_of("across"), g_of("across"), at(a, 0, 0)))
        return out

    groups = ("near", "below", "above")
    quarters = {g: along_y(g, rows16, ZYX_COLS, "quarter", leg_got.at[k]) for k, g in enumerate(groups)}
    wholes = {g: along_y(g, every, ZY_COLS, "whole", g_of("whole")) for g in groups}
    acrosses = {g: along_x(g) for g in groups}

    def start(*lists):
        for cps in lists:
            for cp in cps:
                cp.start()

    def quarters_arrive(k):
        take(m_out.at[pl.ds(0, (3, 2, 3)[k]), pl.ds(0, 3), pl.ds(0, 16), ZYX_COLS], leg_got.at[k])

    for cp in cots:
        cp.wait()
    for k in range(2):
        cot_t[k * 512 : (k + 1) * 512, :] = cot[k].T
    load_x.wait()

    def grad_step(i, _):
        cols = pl.ds(pl.multiple_of(i * 256, 256), 256)
        grad_t[:, cols] = jnp.dot(cot_t[...], xv[:, cols], preferred_element_type=F32).astype(BF)
        return 0

    lax.fori_loop(0, 2, grad_step, 0)

    take(fall.at[c, pl.ds(0, 7), 0, 0], g_of("fz"))
    def piece(half, xs, ys):
        return fall.at[c, pl.ds(4 * half, 4), ys, xs]

    def send_piece(half, xs, ys, ss, rs, dev):
        block = piece(half, xs, ys)
        return remote(block, block, ss, rs, dev)

    def back(p, d):
        return lax.rem(p + 4 - d, 4)

    near = (1, 3, 2)
    fa = [send_piece(0, x, y, s_of("fab"), pair_got.at[k], at(0, b, 0)) for k, b in enumerate(near)]
    fb = [send_piece(1, x, y, s_of("fab"), pair_got.at[k], at(a, 0, 0)) for k, a in enumerate(near)]
    ysrc = [y] + [back(y, b) for b in near]
    xsrc = [x] + [back(x, a) for a in near]
    fc = [
        [send_piece(0, x, ys, s_of("fcd"), land_got.at[i], at(a, 0, 0)) for a in near]
        for i, ys in enumerate(ysrc)
    ]
    fd = [
        [send_piece(1, xs, y, s_of("fcd"), land_got.at[i], at(0, b, 0)) for b in near]
        for i, xs in enumerate(xsrc)
    ]

    def to_partner(half, xs, ys):
        send_piece(half, xs, ys, s_of("ft"), g_of("ft"), at(0, 0, 0, 1)).start()

    start(fa, fb, fc[0], fd[0])
    to_partner(0, x, y)
    to_partner(1, x, y)

    lax.fori_loop(2, 4, grad_step, 0)
    hop(0, 1)
    take(m_out.at[0, pl.ds(0, 3), :, YZ_COLS], g_of("by"))
    hop(1, 0)

    def relay(k):
        take(fall.at[c, :, 0, 0], pair_got.at[k])
        start(fc[1 + k], fd[1 + k])
        to_partner(0, x, ysrc[1 + k])
        to_partner(1, xsrc[1 + k], y)

    relay(0)
    relay(1)
    start(quarters["near"])
    lax.fori_loop(4, 5, grad_step, 0)
    relay(2)
    hop(0, 2)
    hop(2, 0)
    lax.fori_loop(5, 7, grad_step, 0)

    def land(i):
        take(fall.at[c, :, pl.ds(0, 3), 0], land_got.at[i])
        for k in range(3):
            to_partner(0, xsrc[1 + k], ysrc[i])
            to_partner(1, xsrc[i], ysrc[1 + k])

    land(0)
    lax.fori_loop(7, 8, grad_step, 0)
    land(1)
    hop(0, 3)
    land(2)
    quarters_arrive(0)
    land(3)
    start(acrosses["near"], wholes["near"])
    hop(1, 1)

    for n in range(4):
        if n == 2:
            start(mo)
            take(fall.at[1 - c], g_of("ft"))
        kind = c if n < 2 else 1 - c
        q = 2 * kind + n % 2
        basis = fall[kind].reshape(D, RANK)
        rows = pl.ds(pl.multiple_of(q * 256, 256), 256)
        low_t = jnp.dot(grad_t[rows, :], basis, preferred_element_type=F32)
        part[q] = low_t.T.astype(BF).reshape(4, 64, 256)
        a = lax.rem(q + 4 - x, 4)

        def send_part(b):
            slot = a * 4 + b - 1
            dev = {"fs": z * 4 + lax.rem(y + b, 4), "rep": q, "tp": c}
            remote(part.at[q, lax.rem(y + b, 4)], rsb.at[slot], s_of("rs"), g_of("rs"), dev).start()

        for b in (2, 1, 3):
            send_part(b)
        pl.when(q != x)(functools.partial(send_part, 0))

    landed(0, 3)
    start(quarters["below"], quarters["above"])
    hop(2, 1)
    hop(1, 2)

    grams = []
    for kind in range(2):
        basis = fall[kind].reshape(D, RANK)
        g = lax.dot_general(basis, basis, (((0,), (0,)), ((), ())), preferred_element_type=F32)
        hi = g.astype(BF)
        grams.append((hi, (g - hi.astype(F32)).astype(BF)))

    start(wholes["below"], wholes["above"])
    total = part[x, y].astype(F32)
    take(rsb, g_of("rs"))
    for k in range(15):
        total = total + rsb[k].astype(F32)
    zb[z] = total.astype(BF)
    zs = [remote(zb.at[z], zb.at[z], s_of("zs"), g_of("zs"), at(0, 0, d)) for k, d in enumerate(ZD)]
    for cp in zs:
        cp.start()
    quarters_arrive(2)
    start(acrosses["above"])
    quarters_arrive(1)
    take(mom.at[pl.ds(0, 7)], g_of("mo"))
    first = mom[:, 0].reshape(64, 256)
    second = mom[:, 1].reshape(64, 256)
    take(zb.at[pl.ds(0, 7)], g_of("zs"))
    hop(2, 2)
    hop(1, 3)
    low = zb[0].astype(F32)
    for k in range(1, 8):
        low = low + zb[k].astype(F32)
    first_new = 0.8 * first + 0.2 * low
    second_new = 0.95 * second + 0.05 * low * low
    nb[x, y] = (first_new / jnp.sqrt(second_new)).astype(BF)
    halves = (pl.ds(0, 32), pl.ds(32, 32))

    def normed_piece(half, xs, ys, name, rsem, dev):
        block = nb.at[xs, ys, halves[half]]
        return remote(block, block, s_of(name), rsem, dev)

    na = [normed_piece(0, x, y, "nab", npair_got.at[k], at(0, b, 0)) for k, b in enumerate(near)]
    nbb = [normed_piece(1, x, y, "nab", npair_got.at[k], at(a, 0, 0)) for k, a in enumerate(near)]
    nc = [[normed_piece(0, x, ys, "ncd", g_of("ncd"), at(a, 0, 0)) for a in near] for ys in ysrc]
    nd = [[normed_piece(1, xs, y, "ncd", g_of("ncd"), at(0, b, 0)) for b in near] for xs in xsrc]
    start(na, nbb, nc[0], nd[0])

    part_low = low.reshape(8, 8, 256)
    mine = jnp.zeros((8, 256), F32)
    for k in range(8):
        mine = jnp.where(z == k, part_low[k], mine)
    lowb[x] = mine
    lo = [remote(lowb.at[x], lowb.at[x], s_of("lo"), g_of("lo"), at(a, 0, 0)) for a in (2, 1, 3)]
    for cp in lo:
        cp.start()

    for k in range(3):
        take(nb.at[0, 0], npair_got.at[k])
        start(nc[1 + k], nd[1 + k])
    start(acrosses["below"])
    hop(2, 3)
    take(nb.at[pl.ds(0, 3)], g_of("ncd"))
    for kind in range(2):
        acc = jnp.zeros((8, 128), F32)
        for q in (2 * kind, 2 * kind + 1):
            normed = nb[q].reshape(RANK, 256)
            t = jnp.dot(grams[kind][0], normed, preferred_element_type=F32)
            t = t + jnp.dot(grams[kind][1], normed, preferred_element_type=F32)
            s = jnp.sum((t * normed.astype(F32)).reshape(32, 8, 256), axis=0)
            acc = acc + s[:, :128] + s[:, 128:]
        sqb[c, kind] = acc
    sq = remote(sqb.at[c], sqb.at[c], s_of("sq"), g_of("sq"), at(0, 0, 0, 1))
    sq.start()
    take(lowb.at[pl.ds(0, 3)], g_of("lo"))
    take(sqb.at[0], g_of("sq"))
    landed(1, 3)
    landed(2, 3)
    spread = {
        "whole": m_out.at[:, pl.ds(0, 3), :, ZY_COLS],
        "across": m_out.at[:, pl.ds(0, 3), pl.ds(0, 48), ZYX_COLS],
    }
    for name, region in spread.items():
        take(region, g_of(name))
    gone = {
        "fz": fall.at[0, pl.ds(0, 7), 0, 0],
        "mo": mom.at[pl.ds(0, 7)],
        "by": m_out.at[0, pl.ds(0, 3), :, YZ_COLS],
        "ra": ring_blocks(0, 7),
        "rb": ring_blocks(1, 7),
        "rc": ring_blocks(2, 7),
        "fab": fall.at[0, :, pl.ds(0, 3), 0],
        "fcd": fall.at[0, :, :, pl.ds(0, 3)],
        "ft": fall.at[0],
        "rs": rsb,
        "quarter": m_out.at[:, pl.ds(0, 3), pl.ds(0, 16), ZYX_COLS],
        "zs": zb.at[pl.ds(0, 7)],
        "nab": nb.at[0, pl.ds(0, 3)],
        "ncd": nb.at[pl.ds(0, 3)],
        "lo": lowb.at[pl.ds(0, 3)],
        "sq": sqb.at[0],
        **spread,
    }
    for name in GROUPS:
        take(gone[name], s_of(name))


def gathered(x, ci, cg, im, gm, inf, gf, i1, i2, g1, g2):
    sem = pltpu.SemaphoreType.DMA
    return pl.pallas_call(
        move_kernel,
        name="move",
        out_shape=(
            pltpu.VMEM((NZ, NY, 64, W), BF),
            pltpu.VMEM((2, NZ, NY, NX, 16, RANK), BF),
            pltpu.VMEM((NX, NY, 64, 256), BF),
            pltpu.VMEM((NX, 8, 256), F32),
            pltpu.VMEM((2, 2, 8, 128), F32),
        ),
        in_specs=[pl.BlockSpec(memory_space=ANY)] * 11,
        out_specs=[pl.BlockSpec(memory_space=pltpu.VMEM)] * 5,
        scratch_shapes=[
            pltpu.VMEM((1024, D), BF),
            pltpu.VMEM((2, 1024, 512), BF),
            pltpu.VMEM((1024, 1024), BF),
            pltpu.VMEM((1024, D), BF),
            pltpu.VMEM((64, RANK), BF),
            pltpu.VMEM((4, 16, RANK), BF),
            pltpu.VMEM((2, 64, 512), F32),
            pltpu.VMEM((64, W), BF),
            pltpu.VMEM((4, 8, 512), F32),
            pltpu.VMEM((4, 2, 8, 256), F32),
            pltpu.VMEM((NZ, 2, 8, 256), F32),
            pltpu.VMEM((NX, NY, 64, 256), BF),
            pltpu.VMEM((15, 64, 256), BF),
            pltpu.VMEM((NZ, 64, 256), BF),
            sem((10,)),
            sem((len(GROUPS),)),
            sem((len(GROUPS),)),
            sem((3, 4)),
            sem((3,)),
            sem((4,)),
            sem((3,)),
            sem((3,)),
        ],
        compiler_params=pltpu.CompilerParams(
            collective_id=0, has_side_effects=True, vmem_limit_bytes=VMEM - KEPT
        ),
        cost_estimate=pl.CostEstimate(flops=6 * 10**9, bytes_accessed=16 * 2**20, transcendentals=0),
    )(x, ci, cg, im, gm, inf, gf, i1, i2, g1, g2)


def write_kernel(
    fv, nv, mv, sqv, lowv, im_hbm, gm_hbm, i1_hbm, i2_hbm, g1_hbm, g2_hbm,
    im_out, gm_out, iu_out, gu_out, i1_out, i2_out, g1_out, g2_out, ic_out, gc_out,
    old_v, new_v, upd_v, mom_v, mom_new, cv, s_in, s_c, s_out,
):
    _, y, z, _ = where_am_i()
    small = [
        (im_hbm, old_v.at[0]), (gm_hbm, old_v.at[1]),
        *[(r, mom_v.at[k]) for k, r in enumerate((i1_hbm, i2_hbm, g1_hbm, g2_hbm))],
    ]
    small = [pltpu.make_async_copy(src, dst, s_in.at[k]) for k, (src, dst) in enumerate(small)]
    for cp in small:
        cp.start()
    outs = []

    def put(src, dst, sem):
        cp = pltpu.make_async_copy(src, dst, sem)
        cp.start()
        outs.append(cp)

    scale = []
    for kind in range(2):
        square = jnp.sum(sqv[0, kind] + sqv[1, kind], axis=(0, 1), keepdims=True)
        scale.append(lax.rsqrt(square / (D * W) + 0.1))

    def rows_out(b, kind):
        out = (ic_out, gc_out)[kind]
        rows = pl.ds(pl.multiple_of(256 * b, 256), 256)
        return pltpu.make_async_copy(cv.at[b, kind], out.at[rows, :], s_c.at[b, kind])

    def blocks(p, _):
        k = 2 * p
        for kind in range(2):
            basis = fv[kind, pl.ds(k, 2)].reshape(512, RANK)
            for h in range(2):
                normed = nv[2 * kind + h].reshape(RANK, 256)
                full = jnp.dot(basis, normed, preferred_element_type=F32)
                col = kind * 512 + 256 * h
                for i in range(2):
                    old = mv[lax.rem(k + i + 8 - z + HERE, 8), :, :, col : col + 256].reshape(256, 256)
                    new = old.astype(F32) - full[256 * i : 256 * (i + 1)] * (0.05 * scale[kind])
                    cv[k + i, kind, :, 256 * h : 256 * h + 256] = new.astype(BF)
            for i in range(2):
                rows_out(k + i, kind).start()
        return 0

    lax.fori_loop(0, 2, blocks, 0)
    for cp in small:
        cp.wait()
    for kind, (new_out, upd_out) in enumerate(((im_out, iu_out), (gm_out, gu_out))):
        basis = fv[kind, z, y].reshape(64, RANK)
        for h in range(2):
            normed = nv[2 * kind + h].reshape(RANK, 256)
            cols = slice(256 * h, 256 * h + 256)
            u = jnp.dot(basis, normed, preferred_element_type=F32) * scale[kind]
            upd_v[kind, :, cols] = u
            new_v[kind, :, cols] = old_v[kind, :, cols] - 0.05 * u
        put(upd_v.at[kind], upd_out, s_out.at[2 * kind])
        put(new_v.at[kind], new_out, s_out.at[2 * kind + 1])
    for kind, (first_out, second_out) in enumerate(((i1_out, i2_out), (g1_out, g2_out))):
        for h in range(2):
            low = lowv[2 * kind + h]
            cols = slice(256 * h, 256 * h + 256)
            mom_new[2 * kind, :, cols] = 0.8 * mom_v[2 * kind, :, cols] + 0.2 * low
            mom_new[2 * kind + 1, :, cols] = 0.95 * mom_v[2 * kind + 1, :, cols] + 0.05 * low * low
        put(mom_new.at[2 * kind], first_out, s_out.at[4 + 2 * kind])
        put(mom_new.at[2 * kind + 1], second_out, s_out.at[5 + 2 * kind])
    lax.fori_loop(2, 4, blocks, 0)
    for cp in outs:
        cp.wait()
    for b in range(8):
        for kind in range(2):
            rows_out(b, kind).wait()


def written(f, n, m, sq, low, im, gm, i1, i2, g1, g2):
    sem, kept = pltpu.SemaphoreType.DMA, pl.BlockSpec(memory_space=ANY)
    held = pl.BlockSpec(memory_space=pltpu.VMEM)
    return pl.pallas_call(
        write_kernel,
        name="write",
        out_shape=(
            *[jax.ShapeDtypeStruct((64, 512), F32)] * 4,
            *[jax.ShapeDtypeStruct((8, 512), F32)] * 4,
            *[jax.ShapeDtypeStruct((D, 512), BF)] * 2,
        ),
        in_specs=[held] * 5 + [kept] * 6,
        out_specs=[kept] * 10,
        scratch_shapes=[
            *[pltpu.VMEM((2, 64, 512), F32)] * 3,
            *[pltpu.VMEM((4, 8, 512), F32)] * 2,
            pltpu.VMEM((8, 2, 256, 512), BF),
            sem((6,)),
            sem((8, 2)),
            sem((8,)),
        ],
        compiler_params=pltpu.CompilerParams(vmem_limit_bytes=VMEM - KEPT),
    )(f, n, m, sq, low, im, gm, i1, i2, g1, g2)


def on_device(x, ci, cg, im, gm, inf, gf, i1, i2, g1, g2):
    m, f, n, low, sq = gathered(x, ci, cg, im, gm, inf, gf, i1, i2, g1, g2)
    f, n, m, sq, low = (pltpu.with_memory_space_constraint(a, pltpu.VMEM) for a in (f, n, m, sq, low))
    out = written(f, n, m, sq, low, im, gm, i1, i2, g1, g2)
    return tuple(out)


def solution(mesh):
    tokens, rows, moments = P(("fs", "rep"), "tp"), P("fs", "tp"), P("fs", "tp")
    return jax.shard_map(
        on_device,
        mesh=mesh,
        in_specs=(
            P(("fs", "rep"), None), tokens, tokens, rows, rows, P("fs", None), P("fs", None),
            moments, moments, moments, moments,
        ),
        out_specs=(rows,) * 4 + (moments,) * 4 + (P(None, "tp"),) * 2,
        check_vma=False,
    )
```

```python
import functools

import jax
import jax.numpy as jnp
from jax import lax
from jax.experimental import pallas as pl
from jax.experimental.pallas import tpu as pltpu
from jax.sharding import PartitionSpec as P

D = 2048
W = 1024
RANK = 256
NX, NY, NZ = 4, 4, 8
YZ_COLS, YZ0, YZ1 = pl.ds(0, 512), pl.ds(0, 256), pl.ds(256, 256)
ZY_COLS, ZYX_COLS, Z_COLS = pl.ds(512, 128), pl.ds(640, 384), pl.ds(512, 512)
HERE = 3
NEAR, BELOW, ABOVE = pl.ds(2, 3), pl.ds(0, 2), pl.ds(5, 3)
BF = jnp.bfloat16
F32 = jnp.float32
VMEM = 67_043_328
KEPT = (6 * 1024 + 512 + 32 + 16) * 1024
ANY = pl.ANY

XY = sorted(
    [(a, b) for a in range(4) for b in range(4) if (a, b) != (0, 0)],
    key=lambda o: -(min(o[0], 4 - o[0]) + min(o[1], 4 - o[1])),
)
ZD = sorted(range(1, 8), key=lambda d: -min(d, 8 - d))


def where_am_i():
    fs, x, c = lax.axis_index("fs"), lax.axis_index("rep"), lax.axis_index("tp")
    return x, lax.rem(fs, 4), lax.div(fs, 4), c


GROUPS = ("fz", "mo", "by", "ra", "rb", "rc", "fab", "fcd", "ft", "rs", "quarter", "whole", "across", "zs", "lo", "nab", "ncd", "sq")
SEM = {name: k for k, name in enumerate(GROUPS)}
GOT = {name: k for k, name in enumerate(("fz", "mo", "by", "ft", "rs", "whole", "across", "zs", "lo", "ncd", "sq"))}


def take(region, sem):
    pltpu.make_async_copy(region, region, sem).wait()


def remote(src, dst, ss, rs, dev):
    return pltpu.make_async_remote_copy(
        src_ref=src,
        dst_ref=dst,
        send_sem=ss,
        recv_sem=rs,
        device_id=dev,
        device_id_type=pl.DeviceIdType.MESH,
    )


def move_kernel(
    x_hbm, ci_hbm, cg_hbm, im_hbm, gm_hbm, if_hbm, gf_hbm, i1_hbm, i2_hbm, g1_hbm, g2_hbm,
    m_out, fall, nb, lowb, sqb,
    xv, cot, cot_t, grad_t, fac, fsh, mast, msh, mom_in, mom_own, mom,
    part, rsb, zb,
    s_loc, sent, got, ring_got, pair_got, land_got, leg_got, npair_got,
):
    x, y, z, c = where_am_i()

    def at(dx, dy, dz, dc=0):
        return {
            "fs": lax.rem(z + dz, 8) * 4 + lax.rem(y + dy, 4),
            "rep": lax.rem(x + dx, 4),
            "tp": lax.rem(c + dc, 2),
        }

    def s_of(name):
        return sent.at[SEM[name]]

    def g_of(name):
        return got.at[GOT[name]]

    @pl.when(c == 0)
    def _():
        pltpu.make_async_copy(if_hbm, fac, s_loc.at[0]).start()

    @pl.when(c == 1)
    def _():
        pltpu.make_async_copy(gf_hbm, fac, s_loc.at[0]).start()

    moms = [
        pltpu.make_async_copy(r, mom_in.at[k], s_loc.at[1 + k])
        for k, r in enumerate((i1_hbm, g1_hbm, i2_hbm, g2_hbm))
    ]
    masters = [
        pltpu.make_async_copy(r, mast.at[k], s_loc.at[5 + k]) for k, r in enumerate((im_hbm, gm_hbm))
    ]
    cots = [
        pltpu.make_async_copy(r, cot.at[k], s_loc.at[7 + k]) for k, r in enumerate((ci_hbm, cg_hbm))
    ]
    load_x = pltpu.make_async_copy(x_hbm, xv, s_loc.at[9])
    for cp in (*moms, *masters, *cots, load_x):
        cp.start()

    barrier = pltpu.get_barrier_semaphore()
    peers = [at(a, b, 0) for a, b in XY] + [at(0, 0, d) for d in ZD] + [at(0, 0, 0, 1)]
    for p in peers:
        pl.semaphore_signal(barrier, inc=1, device_id=p, device_id_type=pl.DeviceIdType.MESH)

    pltpu.make_async_copy(if_hbm, fac, s_loc.at[0]).wait()
    new = lax.broadcasted_iota(jnp.int32, (RANK, RANK), 1)
    old = lax.broadcasted_iota(jnp.int32, (RANK, RANK), 0)
    ny, nz, ni = lax.shift_right_logical(new, 6), (lax.shift_right_logical(new, 3) & 7), new & 7
    perm = jnp.where(old == (nz * 4 + ny) * 8 + ni, 1.0, 0.0).astype(BF)
    shard = jnp.dot(fac[...], perm, preferred_element_type=F32).astype(BF)
    fsh[...] = shard.reshape(4, 16, RANK)
    fall[c, z, y, x] = fsh[x]

    for cp in moms:
        cp.wait()
    for q in range(4):
        kind, col = q // 2, (q % 2) * 256
        mom_own[q, 0] = mom_in[kind, :, col : col + 256]
        mom_own[q, 1] = mom_in[2 + kind, :, col : col + 256]
    mom[z] = mom_own[x]

    for cp in masters:
        cp.wait()
    msh[:, :512] = mast[0].astype(BF)
    msh[:, 512:] = mast[1].astype(BF)
    m_out[HERE, y] = msh[...]

    pl.semaphore_wait(barrier, len(peers))

    fz = [
        remote(fsh.at[x], fall.at[c, z, y, x], s_of("fz"), g_of("fz"), at(0, 0, d))
        for k, d in enumerate(ZD)
    ]
    mo = [remote(mom_own.at[x], mom.at[z], s_of("mo"), g_of("mo"), at(0, 0, d)) for k, d in enumerate(ZD)]
    by = [
        remote(msh.at[:, YZ_COLS], m_out.at[HERE, y, :, YZ_COLS], s_of("by"), g_of("by"), at(0, b, 0))
        for k, b in enumerate((2, 1, 3))
    ]

    def ring(block, n):
        ss, rs = s_of(("ra", "rb", "rc")[n]), ring_got.at[n]
        hops = []
        for h in range(4):
            lower, upper = (pl.ds(0, 32), pl.ds(32, 32)) if h == 3 else (pl.ds(0, 64),) * 2
            up = (block(HERE - h, lower), block(HERE - h - 1 if h < 3 else HERE + 4, lower))
            down = (block(HERE + h, upper), block(HERE + h + 1, upper))
            hops.append(
                (
                    remote(*up, ss, rs.at[h], at(0, 0, 1)),
                    remote(*down, ss, rs.at[h], at(0, 0, 7)),
                )
            )
        return hops

    ra = ring(lambda k, rows: m_out.at[k, y, rows, Z_COLS], 0)
    rb = ring(lambda k, rows: m_out.at[k, :, rows, YZ0], 1)
    rc = ring(lambda k, rows: m_out.at[k, :, rows, YZ1], 2)
    every = pl.ds(0, 64)

    def ring_blocks(n, count):
        if n == 0:
            return m_out.at[pl.ds(0, count), y, :, Z_COLS]
        return m_out.at[pl.ds(0, count), :, :, (YZ0, YZ1)[n - 1]]

    def landed(n, h):
        take(ring_blocks(n, 2 if h < 3 else 1), ring_got.at[n, h])

    def hop(n, h):
        if h:
            landed(n, h - 1)
        for cp in (ra, rb, rc)[n][h]:
            cp.start()

    for cp in (*fz, *by):
        cp.start()
    hop(0, 0)

    rows16 = pl.ds(pl.multiple_of(x * 16, 16), 16)
    part_of = {"near": NEAR, "below": BELOW, "above": ABOVE}

    def along_y(group, rows, cols, name, rsem):
        block = m_out.at[part_of[group], y, rows, cols]
        return [
            remote(block, block, s_of(name), rsem, at(0, b, 0))
            for b in (2, 1, 3)
        ]

    def along_x(group):
        out = []
        for a in (2, 1, 3):
            for j in range(3):
                block = m_out.at[part_of[group], lax.rem(y + 1 + j, 4), rows16, ZYX_COLS]
                out.append(remote(block, block, s_of("across"), g_of("across"), at(a, 0, 0)))
        return out

    groups = ("near", "below", "above")
    quarters = {g: along_y(g, rows16, ZYX_COLS, "quarter", leg_got.at[k]) for k, g in enumerate(groups)}
    wholes = {g: along_y(g, every, ZY_COLS, "whole", g_of("whole")) for g in groups}
    acrosses = {g: along_x(g) for g in groups}

    def start(*lists):
        for cps in lists:
            for cp in cps:
                cp.start()

    def quarters_arrive(k):
        take(m_out.at[pl.ds(0, (3, 2, 3)[k]), pl.ds(0, 3), pl.ds(0, 16), ZYX_COLS], leg_got.at[k])

    for cp in cots:
        cp.wait()
    for k in range(2):
        cot_t[k * 512 : (k + 1) * 512, :] = cot[k].T
    load_x.wait()

    def grad_step(i, _):
        cols = pl.ds(pl.multiple_of(i * 256, 256), 256)
        grad_t[:, cols] = jnp.dot(cot_t[...], xv[:, cols], preferred_element_type=F32).astype(BF)
        return 0

    lax.fori_loop(0, 2, grad_step, 0)

    take(fall.at[c, pl.ds(0, 7), 0, 0], g_of("fz"))
    def piece(half, xs, ys):
        return fall.at[c, pl.ds(4 * half, 4), ys, xs]

    def send_piece(half, xs, ys, ss, rs, dev):
        block = piece(half, xs, ys)
        return remote(block, block, ss, rs, dev)

    def back(p, d):
        return lax.rem(p + 4 - d, 4)

    near = (1, 3, 2)
    fa = [send_piece(0, x, y, s_of("fab"), pair_got.at[k], at(0, b, 0)) for k, b in enumerate(near)]
    fb = [send_piece(1, x, y, s_of("fab"), pair_got.at[k], at(a, 0, 0)) for k, a in enumerate(near)]
    ysrc = [y] + [back(y, b) for b in near]
    xsrc = [x] + [back(x, a) for a in near]
    fc = [
        [send_piece(0, x, ys, s_of("fcd"), land_got.at[i], at(a, 0, 0)) for a in near]
        for i, ys in enumerate(ysrc)
    ]
    fd = [
        [send_piece(1, xs, y, s_of("fcd"), land_got.at[i], at(0, b, 0)) for b in near]
        for i, xs in enumerate(xsrc)
    ]

    def to_partner(half, xs, ys):
        send_piece(half, xs, ys, s_of("ft"), g_of("ft"), at(0, 0, 0, 1)).start()

    start(fa, fb, fc[0], fd[0])
    to_partner(0, x, y)
    to_partner(1, x, y)

    lax.fori_loop(2, 4, grad_step, 0)
    hop(0, 1)
    take(m_out.at[0, pl.ds(0, 3), :, YZ_COLS], g_of("by"))
    hop(1, 0)

    def relay(k):
        take(fall.at[c, :, 0, 0], pair_got.at[k])
        start(fc[1 + k], fd[1 + k])
        to_partner(0, x, ysrc[1 + k])
        to_partner(1, xsrc[1 + k], y)

    relay(0)
    relay(1)
    start(quarters["near"])
    lax.fori_loop(4, 5, grad_step, 0)
    relay(2)
    hop(0, 2)
    hop(2, 0)
    lax.fori_loop(5, 7, grad_step, 0)

    def land(i):
        take(fall.at[c, :, pl.ds(0, 3), 0], land_got.at[i])
        for k in range(3):
            to_partner(0, xsrc[1 + k], ysrc[i])
            to_partner(1, xsrc[i], ysrc[1 + k])

    land(0)
    lax.fori_loop(7, 8, grad_step, 0)
    land(1)
    hop(0, 3)
    land(2)
    quarters_arrive(0)
    land(3)
    start(acrosses["near"], wholes["near"])
    hop(1, 1)

    def send_part(q, a, b):
        dev = {"fs": z * 4 + lax.rem(y + b, 4), "rep": q, "tp": c}
        slot = rsb.at[a * 4 + b - 1]
        remote(part.at[q, lax.rem(y + b, 4)], slot, s_of("rs"), g_of("rs"), dev).start()

    for kind in (c, 1 - c):
        if kind is not c:
            start(mo)
            take(fall.at[1 - c], g_of("ft"))
        rows = pl.ds(pl.multiple_of(kind * 512, 512), 512)
        low_t = jnp.dot(grad_t[rows, :], fall[kind].reshape(D, RANK), preferred_element_type=F32)
        for h in range(2):
            q = 2 * kind + h
            part[q] = low_t[256 * h : 256 * (h + 1)].astype(BF).T.reshape(4, 64, 256)
            a = lax.rem(q + 4 - x, 4)
            for b in (2, 1, 3):
                send_part(q, a, b)
            pl.when(q != x)(functools.partial(send_part, q, a, 0))

    landed(0, 3)
    start(quarters["below"], quarters["above"])
    hop(2, 1)
    hop(1, 2)

    grams = []
    for kind in range(2):
        basis = fall[kind].reshape(D, RANK)
        g = lax.dot_general(basis, basis, (((0,), (0,)), ((), ())), preferred_element_type=F32)
        hi = g.astype(BF)
        grams.append((hi, (g - hi.astype(F32)).astype(BF)))

    start(wholes["below"], wholes["above"])
    total = part[x, y].astype(F32)
    take(rsb, g_of("rs"))
    for k in range(15):
        total = total + rsb[k].astype(F32)
    zb[z] = total.astype(BF)
    zs = [remote(zb.at[z], zb.at[z], s_of("zs"), g_of("zs"), at(0, 0, d)) for k, d in enumerate(ZD)]
    for cp in zs:
        cp.start()
    quarters_arrive(2)
    start(acrosses["above"])
    quarters_arrive(1)
    take(mom.at[pl.ds(0, 7)], g_of("mo"))
    first = mom[:, 0].reshape(64, 256)
    second = mom[:, 1].reshape(64, 256)
    take(zb.at[pl.ds(0, 7)], g_of("zs"))
    hop(2, 2)
    hop(1, 3)
    low = zb[0].astype(F32)
    for k in range(1, 8):
        low = low + zb[k].astype(F32)
    first_new = 0.8 * first + 0.2 * low
    second_new = 0.95 * second + 0.05 * low * low
    nb[x, y] = (first_new / jnp.sqrt(second_new)).astype(BF)
    halves = (pl.ds(0, 32), pl.ds(32, 32))

    def normed_piece(half, xs, ys, name, rsem, dev):
        block = nb.at[xs, ys, halves[half]]
        return remote(block, block, s_of(name), rsem, dev)

    na = [normed_piece(0, x, y, "nab", npair_got.at[k], at(0, b, 0)) for k, b in enumerate(near)]
    nbb = [normed_piece(1, x, y, "nab", npair_got.at[k], at(a, 0, 0)) for k, a in enumerate(near)]
    nc = [[normed_piece(0, x, ys, "ncd", g_of("ncd"), at(a, 0, 0)) for a in near] for ys in ysrc]
    nd = [[normed_piece(1, xs, y, "ncd", g_of("ncd"), at(0, b, 0)) for b in near] for xs in xsrc]
    start(na, nbb, nc[0], nd[0])

    part_low = low.reshape(8, 8, 256)
    mine = jnp.zeros((8, 256), F32)
    for k in range(8):
        mine = jnp.where(z == k, part_low[k], mine)
    lowb[x] = mine
    lo = [remote(lowb.at[x], lowb.at[x], s_of("lo"), g_of("lo"), at(a, 0, 0)) for a in (2, 1, 3)]
    for cp in lo:
        cp.start()

    for k in range(3):
        take(nb.at[0, 0], npair_got.at[k])
        start(nc[1 + k], nd[1 + k])
    start(acrosses["below"])
    hop(2, 3)
    take(nb.at[pl.ds(0, 3)], g_of("ncd"))
    for kind in range(2):
        acc = jnp.zeros((8, 128), F32)
        for q in (2 * kind, 2 * kind + 1):
            normed = nb[q].reshape(RANK, 256)
            t = jnp.dot(grams[kind][0], normed, preferred_element_type=F32)
            t = t + jnp.dot(grams[kind][1], normed, preferred_element_type=F32)
            s = jnp.sum((t * normed.astype(F32)).reshape(32, 8, 256), axis=0)
            acc = acc + s[:, :128] + s[:, 128:]
        sqb[c, kind] = acc
    sq = remote(sqb.at[c], sqb.at[c], s_of("sq"), g_of("sq"), at(0, 0, 0, 1))
    sq.start()
    take(lowb.at[pl.ds(0, 3)], g_of("lo"))
    take(sqb.at[0], g_of("sq"))
    landed(1, 3)
    landed(2, 3)
    spread = {
        "whole": m_out.at[:, pl.ds(0, 3), :, ZY_COLS],
        "across": m_out.at[:, pl.ds(0, 3), pl.ds(0, 48), ZYX_COLS],
    }
    for name, region in spread.items():
        take(region, g_of(name))
    gone = {
        "fz": fall.at[0, pl.ds(0, 7), 0, 0],
        "mo": mom.at[pl.ds(0, 7)],
        "by": m_out.at[0, pl.ds(0, 3), :, YZ_COLS],
        "ra": ring_blocks(0, 7),
        "rb": ring_blocks(1, 7),
        "rc": ring_blocks(2, 7),
        "fab": fall.at[0, :, pl.ds(0, 3), 0],
        "fcd": fall.at[0, :, :, pl.ds(0, 3)],
        "ft": fall.at[0],
        "rs": rsb,
        "quarter": m_out.at[:, pl.ds(0, 3), pl.ds(0, 16), ZYX_COLS],
        "zs": zb.at[pl.ds(0, 7)],
        "nab": nb.at[0, pl.ds(0, 3)],
        "ncd": nb.at[pl.ds(0, 3)],
        "lo": lowb.at[pl.ds(0, 3)],
        "sq": sqb.at[0],
        **spread,
    }
    for name in GROUPS:
        take(gone[name], s_of(name))


def gathered(x, ci, cg, im, gm, inf, gf, i1, i2, g1, g2):
    sem = pltpu.SemaphoreType.DMA
    return pl.pallas_call(
        move_kernel,
        name="move",
        out_shape=(
            pltpu.VMEM((NZ, NY, 64, W), BF),
            pltpu.VMEM((2, NZ, NY, NX, 16, RANK), BF),
            pltpu.VMEM((NX, NY, 64, 256), BF),
            pltpu.VMEM((NX, 8, 256), F32),
            pltpu.VMEM((2, 2, 8, 128), F32),
        ),
        in_specs=[pl.BlockSpec(memory_space=ANY)] * 11,
        out_specs=[pl.BlockSpec(memory_space=pltpu.VMEM)] * 5,
        scratch_shapes=[
            pltpu.VMEM((1024, D), BF),
            pltpu.VMEM((2, 1024, 512), BF),
            pltpu.VMEM((1024, 1024), BF),
            pltpu.VMEM((1024, D), BF),
            pltpu.VMEM((64, RANK), BF),
            pltpu.VMEM((4, 16, RANK), BF),
            pltpu.VMEM((2, 64, 512), F32),
            pltpu.VMEM((64, W), BF),
            pltpu.VMEM((4, 8, 512), F32),
            pltpu.VMEM((4, 2, 8, 256), F32),
            pltpu.VMEM((NZ, 2, 8, 256), F32),
            pltpu.VMEM((NX, NY, 64, 256), BF),
            pltpu.VMEM((15, 64, 256), BF),
            pltpu.VMEM((NZ, 64, 256), BF),
            sem((10,)),
            sem((len(GROUPS),)),
            sem((len(GOT),)),
            sem((3, 4)),
            sem((3,)),
            sem((4,)),
            sem((3,)),
            sem((3,)),
        ],
        compiler_params=pltpu.CompilerParams(
            collective_id=0, has_side_effects=True, vmem_limit_bytes=VMEM - KEPT
        ),
        cost_estimate=pl.CostEstimate(flops=6 * 10**9, bytes_accessed=16 * 2**20, transcendentals=0),
    )(x, ci, cg, im, gm, inf, gf, i1, i2, g1, g2)


def write_kernel(
    fv, nv, mv, sqv, lowv, im_hbm, gm_hbm, i1_hbm, i2_hbm, g1_hbm, g2_hbm,
    im_out, gm_out, iu_out, gu_out, i1_out, i2_out, g1_out, g2_out, ic_out, gc_out,
    old_v, new_v, upd_v, mom_v, mom_new, cv, s_in, s_c, s_out,
):
    _, y, z, _ = where_am_i()
    small = [
        (im_hbm, old_v.at[0]), (gm_hbm, old_v.at[1]),
        *[(r, mom_v.at[k]) for k, r in enumerate((i1_hbm, i2_hbm, g1_hbm, g2_hbm))],
    ]
    small = [pltpu.make_async_copy(src, dst, s_in.at[k]) for k, (src, dst) in enumerate(small)]
    for cp in small:
        cp.start()
    outs = []

    def put(src, dst, sem):
        cp = pltpu.make_async_copy(src, dst, sem)
        cp.start()
        outs.append(cp)

    scale = []
    for kind in range(2):
        square = jnp.sum(sqv[0, kind] + sqv[1, kind], axis=(0, 1), keepdims=True)
        scale.append(lax.rsqrt(square / (D * W) + 0.1))

    def rows_out(b, kind):
        out = (ic_out, gc_out)[kind]
        rows = pl.ds(pl.multiple_of(256 * b, 256), 256)
        return pltpu.make_async_copy(cv.at[b, kind], out.at[rows, :], s_c.at[b, kind])

    def blocks(p, _):
        k = 2 * p
        for kind in range(2):
            basis = fv[kind, pl.ds(k, 2)].reshape(512, RANK)
            for h in range(2):
                normed = nv[2 * kind + h].reshape(RANK, 256)
                full = jnp.dot(basis, normed, preferred_element_type=F32)
                col = kind * 512 + 256 * h
                for i in range(2):
                    old = mv[lax.rem(k + i + 8 - z + HERE, 8), :, :, col : col + 256].reshape(256, 256)
                    new = old.astype(F32) - full[256 * i : 256 * (i + 1)] * (0.05 * scale[kind])
                    cv[k + i, kind, :, 256 * h : 256 * h + 256] = new.astype(BF)
            for i in range(2):
                rows_out(k + i, kind).start()
        return 0

    lax.fori_loop(0, 2, blocks, 0)
    for cp in small:
        cp.wait()
    for kind, (new_out, upd_out) in enumerate(((im_out, iu_out), (gm_out, gu_out))):
        basis = fv[kind, z, y].reshape(64, RANK)
        for h in range(2):
            normed = nv[2 * kind + h].reshape(RANK, 256)
            cols = slice(256 * h, 256 * h + 256)
            u = jnp.dot(basis, normed, preferred_element_type=F32) * scale[kind]
            upd_v[kind, :, cols] = u
            new_v[kind, :, cols] = old_v[kind, :, cols] - 0.05 * u
        put(upd_v.at[kind], upd_out, s_out.at[2 * kind])
        put(new_v.at[kind], new_out, s_out.at[2 * kind + 1])
    for kind, (first_out, second_out) in enumerate(((i1_out, i2_out), (g1_out, g2_out))):
        for h in range(2):
            low = lowv[2 * kind + h]
            cols = slice(256 * h, 256 * h + 256)
            mom_new[2 * kind, :, cols] = 0.8 * mom_v[2 * kind, :, cols] + 0.2 * low
            mom_new[2 * kind + 1, :, cols] = 0.95 * mom_v[2 * kind + 1, :, cols] + 0.05 * low * low
        put(mom_new.at[2 * kind], first_out, s_out.at[4 + 2 * kind])
        put(mom_new.at[2 * kind + 1], second_out, s_out.at[5 + 2 * kind])
    lax.fori_loop(2, 4, blocks, 0)
    for cp in outs:
        cp.wait()
    for b in range(8):
        for kind in range(2):
            rows_out(b, kind).wait()


def written(f, n, m, sq, low, im, gm, i1, i2, g1, g2):
    sem, kept = pltpu.SemaphoreType.DMA, pl.BlockSpec(memory_space=ANY)
    held = pl.BlockSpec(memory_space=pltpu.VMEM)
    return pl.pallas_call(
        write_kernel,
        name="write",
        out_shape=(
            *[jax.ShapeDtypeStruct((64, 512), F32)] * 4,
            *[jax.ShapeDtypeStruct((8, 512), F32)] * 4,
            *[jax.ShapeDtypeStruct((D, 512), BF)] * 2,
        ),
        in_specs=[held] * 5 + [kept] * 6,
        out_specs=[kept] * 10,
        scratch_shapes=[
            *[pltpu.VMEM((2, 64, 512), F32)] * 3,
            *[pltpu.VMEM((4, 8, 512), F32)] * 2,
            pltpu.VMEM((8, 2, 256, 512), BF),
            sem((6,)),
            sem((8, 2)),
            sem((8,)),
        ],
        compiler_params=pltpu.CompilerParams(vmem_limit_bytes=VMEM - KEPT),
    )(f, n, m, sq, low, im, gm, i1, i2, g1, g2)


def on_device(x, ci, cg, im, gm, inf, gf, i1, i2, g1, g2):
    m, f, n, low, sq = gathered(x, ci, cg, im, gm, inf, gf, i1, i2, g1, g2)
    f, n, m, sq, low = (pltpu.with_memory_space_constraint(a, pltpu.VMEM) for a in (f, n, m, sq, low))
    out = written(f, n, m, sq, low, im, gm, i1, i2, g1, g2)
    return tuple(out)


def solution(mesh):
    tokens, rows, moments = P(("fs", "rep"), "tp"), P("fs", "tp"), P("fs", "tp")
    return jax.shard_map(
        on_device,
        mesh=mesh,
        in_specs=(
            P(("fs", "rep"), None), tokens, tokens, rows, rows, P("fs", None), P("fs", None),
            moments, moments, moments, moments,
        ),
        out_specs=(rows,) * 4 + (moments,) * 4 + (P(None, "tp"),) * 2,
        check_vma=False,
    )
```

```python
import functools

import jax
import jax.numpy as jnp
from jax import lax
from jax.experimental import pallas as pl
from jax.experimental.pallas import tpu as pltpu
from jax.sharding import PartitionSpec as P

D = 2048
W = 1024
RANK = 256
NX, NY, NZ = 4, 4, 8
YZ_COLS, YZ0, YZ1 = pl.ds(0, 512), pl.ds(0, 256), pl.ds(256, 256)
ZY_COLS, ZYX_COLS, Z_COLS = pl.ds(512, 128), pl.ds(640, 384), pl.ds(512, 512)
HERE = 3
NEAR, BELOW, ABOVE = pl.ds(2, 3), pl.ds(0, 2), pl.ds(5, 3)
BF = jnp.bfloat16
F32 = jnp.float32
VMEM = 67_043_328
KEPT = (6 * 1024 + 512 + 32 + 16) * 1024
ANY = pl.ANY

XY = sorted(
    [(a, b) for a in range(4) for b in range(4) if (a, b) != (0, 0)],
    key=lambda o: -(min(o[0], 4 - o[0]) + min(o[1], 4 - o[1])),
)
ZD = sorted(range(1, 8), key=lambda d: -min(d, 8 - d))


def where_am_i():
    fs, x, c = lax.axis_index("fs"), lax.axis_index("rep"), lax.axis_index("tp")
    return x, lax.rem(fs, 4), lax.div(fs, 4), c


GROUPS = ("fz", "mo", "by", "ra", "rb", "rc", "fab", "fcd", "ft", "rs", "quarter", "whole", "across", "zs", "lo", "nab", "ncd", "sq")
SEM = {name: k for k, name in enumerate(GROUPS)}
GOT = {name: k for k, name in enumerate(("fz", "mo", "by", "ft", "rs", "whole", "across", "zs", "lo", "ncd", "sq"))}


def take(region, sem):
    pltpu.make_async_copy(region, region, sem).wait()


def remote(src, dst, ss, rs, dev):
    return pltpu.make_async_remote_copy(
        src_ref=src,
        dst_ref=dst,
        send_sem=ss,
        recv_sem=rs,
        device_id=dev,
        device_id_type=pl.DeviceIdType.MESH,
    )


def move_kernel(
    x_hbm, ci_hbm, cg_hbm, im_hbm, gm_hbm, if_hbm, gf_hbm, i1_hbm, i2_hbm, g1_hbm, g2_hbm,
    m_out, fall, nb, lowb, sqb,
    xv, cot, cot_t, grad_t, fac, fsh, mast, msh, mom_in, mom_own, mom,
    part, rsb, zb,
    s_loc, sent, got, ring_got, pair_got, land_got, leg_got, npair_got,
):
    x, y, z, c = where_am_i()

    def at(dx, dy, dz, dc=0):
        return {
            "fs": lax.rem(z + dz, 8) * 4 + lax.rem(y + dy, 4),
            "rep": lax.rem(x + dx, 4),
            "tp": lax.rem(c + dc, 2),
        }

    def s_of(name):
        return sent.at[SEM[name]]

    def g_of(name):
        return got.at[GOT[name]]

    @pl.when(c == 0)
    def _():
        pltpu.make_async_copy(if_hbm, fac, s_loc.at[0]).start()

    @pl.when(c == 1)
    def _():
        pltpu.make_async_copy(gf_hbm, fac, s_loc.at[0]).start()

    moms = [
        pltpu.make_async_copy(r, mom_in.at[k], s_loc.at[1 + k])
        for k, r in enumerate((i1_hbm, g1_hbm, i2_hbm, g2_hbm))
    ]
    masters = [
        pltpu.make_async_copy(r, mast.at[k], s_loc.at[5 + k]) for k, r in enumerate((im_hbm, gm_hbm))
    ]
    cots = [
        pltpu.make_async_copy(r, cot.at[k], s_loc.at[7 + k]) for k, r in enumerate((ci_hbm, cg_hbm))
    ]
    load_x = pltpu.make_async_copy(x_hbm, xv, s_loc.at[9])
    for cp in (*moms, *masters, *cots, load_x):
        cp.start()

    barrier = pltpu.get_barrier_semaphore()
    peers = [at(a, b, 0) for a, b in XY] + [at(0, 0, d) for d in ZD] + [at(0, 0, 0, 1)]
    for p in peers:
        pl.semaphore_signal(barrier, inc=1, device_id=p, device_id_type=pl.DeviceIdType.MESH)

    pltpu.make_async_copy(if_hbm, fac, s_loc.at[0]).wait()
    new = lax.broadcasted_iota(jnp.int32, (RANK, RANK), 1)
    old = lax.broadcasted_iota(jnp.int32, (RANK, RANK), 0)
    ny, nz, ni = lax.shift_right_logical(new, 6), (lax.shift_right_logical(new, 3) & 7), new & 7
    perm = jnp.where(old == (nz * 4 + ny) * 8 + ni, 1.0, 0.0).astype(BF)
    shard = jnp.dot(fac[...], perm, preferred_element_type=F32).astype(BF)
    fsh[...] = shard.reshape(4, 16, RANK)
    fall[c, z, y, x] = fsh[x]

    for cp in moms:
        cp.wait()
    for q in range(4):
        kind, col = q // 2, (q % 2) * 256
        mom_own[q, 0] = mom_in[kind, :, col : col + 256]
        mom_own[q, 1] = mom_in[2 + kind, :, col : col + 256]
    mom[z] = mom_own[x]

    for cp in masters:
        cp.wait()
    msh[:, :512] = mast[0].astype(BF)
    msh[:, 512:] = mast[1].astype(BF)
    m_out[HERE, y] = msh[...]

    pl.semaphore_wait(barrier, len(peers))

    fz = [
        remote(fsh.at[x], fall.at[c, z, y, x], s_of("fz"), g_of("fz"), at(0, 0, d))
        for k, d in enumerate(ZD)
    ]
    mo = [remote(mom_own.at[x], mom.at[z], s_of("mo"), g_of("mo"), at(0, 0, d)) for k, d in enumerate(ZD)]
    by = [
        remote(msh.at[:, YZ_COLS], m_out.at[HERE, y, :, YZ_COLS], s_of("by"), g_of("by"), at(0, b, 0))
        for k, b in enumerate((2, 1, 3))
    ]

    def ring(block, n):
        ss, rs = s_of(("ra", "rb", "rc")[n]), ring_got.at[n]
        hops = []
        for h in range(4):
            lower, upper = (pl.ds(0, 32), pl.ds(32, 32)) if h == 3 else (pl.ds(0, 64),) * 2
            up = (block(HERE - h, lower), block(HERE - h - 1 if h < 3 else HERE + 4, lower))
            down = (block(HERE + h, upper), block(HERE + h + 1, upper))
            hops.append(
                (
                    remote(*up, ss, rs.at[h], at(0, 0, 1)),
                    remote(*down, ss, rs.at[h], at(0, 0, 7)),
                )
            )
        return hops

    ra = ring(lambda k, rows: m_out.at[k, y, rows, Z_COLS], 0)
    rb = ring(lambda k, rows: m_out.at[k, :, rows, YZ0], 1)
    rc = ring(lambda k, rows: m_out.at[k, :, rows, YZ1], 2)
    every = pl.ds(0, 64)

    def ring_blocks(n, count):
        if n == 0:
            return m_out.at[pl.ds(0, count), y, :, Z_COLS]
        return m_out.at[pl.ds(0, count), :, :, (YZ0, YZ1)[n - 1]]

    def landed(n, h):
        take(ring_blocks(n, 2 if h < 3 else 1), ring_got.at[n, h])

    def hop(n, h):
        if h:
            landed(n, h - 1)
        for cp in (ra, rb, rc)[n][h]:
            cp.start()

    for cp in (*fz, *by):
        cp.start()
    hop(0, 0)
    for cp in mo:
        cp.start()

    rows16 = pl.ds(pl.multiple_of(x * 16, 16), 16)
    part_of = {"near": NEAR, "below": BELOW, "above": ABOVE}

    def along_y(group, rows, cols, name, rsem):
        block = m_out.at[part_of[group], y, rows, cols]
        return [
            remote(block, block, s_of(name), rsem, at(0, b, 0))
            for b in (2, 1, 3)
        ]

    def along_x(group):
        out = []
        for a in (2, 1, 3):
            for j in range(3):
                block = m_out.at[part_of[group], lax.rem(y + 1 + j, 4), rows16, ZYX_COLS]
                out.append(remote(block, block, s_of("across"), g_of("across"), at(a, 0, 0)))
        return out

    groups = ("near", "below", "above")
    quarters = {g: along_y(g, rows16, ZYX_COLS, "quarter", leg_got.at[k]) for k, g in enumerate(groups)}
    wholes = {g: along_y(g, every, ZY_COLS, "whole", g_of("whole")) for g in groups}
    acrosses = {g: along_x(g) for g in groups}

    def start(*lists):
        for cps in lists:
            for cp in cps:
                cp.start()

    def quarters_arrive(k):
        take(m_out.at[pl.ds(0, (3, 2, 3)[k]), pl.ds(0, 3), pl.ds(0, 16), ZYX_COLS], leg_got.at[k])

    for cp in cots:
        cp.wait()
    for k in range(2):
        cot_t[k * 512 : (k + 1) * 512, :] = cot[k].T
    load_x.wait()

    def grad_step(i, _):
        cols = pl.ds(pl.multiple_of(i * 256, 256), 256)
        grad_t[:, cols] = jnp.dot(cot_t[...], xv[:, cols], preferred_element_type=F32).astype(BF)
        return 0

    lax.fori_loop(0, 2, grad_step, 0)

    take(fall.at[c, pl.ds(0, 7), 0, 0], g_of("fz"))
    def piece(half, xs, ys):
        return fall.at[c, pl.ds(4 * half, 4), ys, xs]

    def send_piece(half, xs, ys, ss, rs, dev):
        block = piece(half, xs, ys)
        return remote(block, block, ss, rs, dev)

    def back(p, d):
        return lax.rem(p + 4 - d, 4)

    near = (1, 3, 2)
    fa = [send_piece(0, x, y, s_of("fab"), pair_got.at[k], at(0, b, 0)) for k, b in enumerate(near)]
    fb = [send_piece(1, x, y, s_of("fab"), pair_got.at[k], at(a, 0, 0)) for k, a in enumerate(near)]
    ysrc = [y] + [back(y, b) for b in near]
    xsrc = [x] + [back(x, a) for a in near]
    fc = [
        [send_piece(0, x, ys, s_of("fcd"), land_got.at[i], at(a, 0, 0)) for a in near]
        for i, ys in enumerate(ysrc)
    ]
    fd = [
        [send_piece(1, xs, y, s_of("fcd"), land_got.at[i], at(0, b, 0)) for b in near]
        for i, xs in enumerate(xsrc)
    ]

    def to_partner(half, xs, ys):
        send_piece(half, xs, ys, s_of("ft"), g_of("ft"), at(0, 0, 0, 1)).start()

    start(fa, fb, fc[0], fd[0])
    to_partner(0, x, y)
    to_partner(1, x, y)

    lax.fori_loop(2, 4, grad_step, 0)
    hop(0, 1)
    take(m_out.at[0, pl.ds(0, 3), :, YZ_COLS], g_of("by"))
    hop(1, 0)

    def relay(k):
        take(fall.at[c, :, 0, 0], pair_got.at[k])
        start(fc[1 + k], fd[1 + k])
        to_partner(0, x, ysrc[1 + k])
        to_partner(1, xsrc[1 + k], y)

    relay(0)
    relay(1)
    start(quarters["near"])
    lax.fori_loop(4, 5, grad_step, 0)
    relay(2)
    hop(0, 2)
    hop(2, 0)
    lax.fori_loop(5, 7, grad_step, 0)

    def land(i):
        take(fall.at[c, :, pl.ds(0, 3), 0], land_got.at[i])
        for k in range(3):
            to_partner(0, xsrc[1 + k], ysrc[i])
            to_partner(1, xsrc[i], ysrc[1 + k])

    land(0)
    lax.fori_loop(7, 8, grad_step, 0)
    land(1)
    hop(0, 3)
    land(2)
    quarters_arrive(0)
    land(3)
    start(acrosses["near"], wholes["near"])
    hop(1, 1)

    def send_part(q, a, b):
        dev = {"fs": z * 4 + lax.rem(y + b, 4), "rep": q, "tp": c}
        slot = rsb.at[a * 4 + b - 1]
        remote(part.at[q, lax.rem(y + b, 4)], slot, s_of("rs"), g_of("rs"), dev).start()

    for kind in (c, 1 - c):
        if kind is not c:
            take(fall.at[1 - c], g_of("ft"))
        rows = pl.ds(pl.multiple_of(kind * 512, 512), 512)
        low_t = jnp.dot(grad_t[rows, :], fall[kind].reshape(D, RANK), preferred_element_type=F32)
        for h in range(2):
            q = 2 * kind + h
            part[q] = low_t[256 * h : 256 * (h + 1)].astype(BF).T.reshape(4, 64, 256)
            a = lax.rem(q + 4 - x, 4)
            for b in (2, 1, 3):
                send_part(q, a, b)
            pl.when(q != x)(functools.partial(send_part, q, a, 0))

    landed(0, 3)
    start(quarters["below"], quarters["above"])
    hop(2, 1)
    hop(1, 2)

    grams = []
    for kind in range(2):
        basis = fall[kind].reshape(D, RANK)
        g = lax.dot_general(basis, basis, (((0,), (0,)), ((), ())), preferred_element_type=F32)
        hi = g.astype(BF)
        grams.append((hi, (g - hi.astype(F32)).astype(BF)))

    start(wholes["below"], wholes["above"])
    total = part[x, y].astype(F32)
    take(rsb, g_of("rs"))
    for k in range(15):
        total = total + rsb[k].astype(F32)
    zb[z] = total.astype(BF)
    zs = [remote(zb.at[z], zb.at[z], s_of("zs"), g_of("zs"), at(0, 0, d)) for k, d in enumerate(ZD)]
    for cp in zs:
        cp.start()
    quarters_arrive(2)
    start(acrosses["above"])
    quarters_arrive(1)
    take(mom.at[pl.ds(0, 7)], g_of("mo"))
    first = mom[:, 0].reshape(64, 256)
    second = mom[:, 1].reshape(64, 256)
    take(zb.at[pl.ds(0, 7)], g_of("zs"))
    hop(2, 2)
    hop(1, 3)
    low = zb[0].astype(F32)
    for k in range(1, 8):
        low = low + zb[k].astype(F32)
    first_new = 0.8 * first + 0.2 * low
    second_new = 0.95 * second + 0.05 * low * low
    nb[x, y] = (first_new / jnp.sqrt(second_new)).astype(BF)
    halves = (pl.ds(0, 32), pl.ds(32, 32))

    def normed_piece(half, xs, ys, name, rsem, dev):
        block = nb.at[xs, ys, halves[half]]
        return remote(block, block, s_of(name), rsem, dev)

    na = [normed_piece(0, x, y, "nab", npair_got.at[k], at(0, b, 0)) for k, b in enumerate(near)]
    nbb = [normed_piece(1, x, y, "nab", npair_got.at[k], at(a, 0, 0)) for k, a in enumerate(near)]
    nc = [[normed_piece(0, x, ys, "ncd", g_of("ncd"), at(a, 0, 0)) for a in near] for ys in ysrc]
    nd = [[normed_piece(1, xs, y, "ncd", g_of("ncd"), at(0, b, 0)) for b in near] for xs in xsrc]
    start(na, nbb, nc[0], nd[0])

    part_low = low.reshape(8, 8, 256)
    mine = jnp.zeros((8, 256), F32)
    for k in range(8):
        mine = jnp.where(z == k, part_low[k], mine)
    lowb[x] = mine
    lo = [remote(lowb.at[x], lowb.at[x], s_of("lo"), g_of("lo"), at(a, 0, 0)) for a in (2, 1, 3)]
    for cp in lo:
        cp.start()

    for k in range(3):
        take(nb.at[0, 0], npair_got.at[k])
        start(nc[1 + k], nd[1 + k])
    start(acrosses["below"])
    hop(2, 3)
    take(nb.at[pl.ds(0, 3)], g_of("ncd"))
    for kind in range(2):
        acc = jnp.zeros((8, 128), F32)
        for q in (2 * kind, 2 * kind + 1):
            normed = nb[q].reshape(RANK, 256)
            t = jnp.dot(grams[kind][0], normed, preferred_element_type=F32)
            t = t + jnp.dot(grams[kind][1], normed, preferred_element_type=F32)
            s = jnp.sum((t * normed.astype(F32)).reshape(32, 8, 256), axis=0)
            acc = acc + s[:, :128] + s[:, 128:]
        sqb[c, kind] = acc
    sq = remote(sqb.at[c], sqb.at[c], s_of("sq"), g_of("sq"), at(0, 0, 0, 1))
    sq.start()
    take(lowb.at[pl.ds(0, 3)], g_of("lo"))
    take(sqb.at[0], g_of("sq"))
    landed(1, 3)
    landed(2, 3)
    spread = {
        "whole": m_out.at[:, pl.ds(0, 3), :, ZY_COLS],
        "across": m_out.at[:, pl.ds(0, 3), pl.ds(0, 48), ZYX_COLS],
    }
    for name, region in spread.items():
        take(region, g_of(name))
    gone = {
        "fz": fall.at[0, pl.ds(0, 7), 0, 0],
        "mo": mom.at[pl.ds(0, 7)],
        "by": m_out.at[0, pl.ds(0, 3), :, YZ_COLS],
        "ra": ring_blocks(0, 7),
        "rb": ring_blocks(1, 7),
        "rc": ring_blocks(2, 7),
        "fab": fall.at[0, :, pl.ds(0, 3), 0],
        "fcd": fall.at[0, :, :, pl.ds(0, 3)],
        "ft": fall.at[0],
        "rs": rsb,
        "quarter": m_out.at[:, pl.ds(0, 3), pl.ds(0, 16), ZYX_COLS],
        "zs": zb.at[pl.ds(0, 7)],
        "nab": nb.at[0, pl.ds(0, 3)],
        "ncd": nb.at[pl.ds(0, 3)],
        "lo": lowb.at[pl.ds(0, 3)],
        "sq": sqb.at[0],
        **spread,
    }
    for name in GROUPS:
        take(gone[name], s_of(name))


def gathered(x, ci, cg, im, gm, inf, gf, i1, i2, g1, g2):
    sem = pltpu.SemaphoreType.DMA
    return pl.pallas_call(
        move_kernel,
        name="move",
        out_shape=(
            pltpu.VMEM((NZ, NY, 64, W), BF),
            pltpu.VMEM((2, NZ, NY, NX, 16, RANK), BF),
            pltpu.VMEM((NX, NY, 64, 256), BF),
            pltpu.VMEM((NX, 8, 256), F32),
            pltpu.VMEM((2, 2, 8, 128), F32),
        ),
        in_specs=[pl.BlockSpec(memory_space=ANY)] * 11,
        out_specs=[pl.BlockSpec(memory_space=pltpu.VMEM)] * 5,
        scratch_shapes=[
            pltpu.VMEM((1024, D), BF),
            pltpu.VMEM((2, 1024, 512), BF),
            pltpu.VMEM((1024, 1024), BF),
            pltpu.VMEM((1024, D), BF),
            pltpu.VMEM((64, RANK), BF),
            pltpu.VMEM((4, 16, RANK), BF),
            pltpu.VMEM((2, 64, 512), F32),
            pltpu.VMEM((64, W), BF),
            pltpu.VMEM((4, 8, 512), F32),
            pltpu.VMEM((4, 2, 8, 256), F32),
            pltpu.VMEM((NZ, 2, 8, 256), F32),
            pltpu.VMEM((NX, NY, 64, 256), BF),
            pltpu.VMEM((15, 64, 256), BF),
            pltpu.VMEM((NZ, 64, 256), BF),
            sem((10,)),
            sem((len(GROUPS),)),
            sem((len(GOT),)),
            sem((3, 4)),
            sem((3,)),
            sem((4,)),
            sem((3,)),
            sem((3,)),
        ],
        compiler_params=pltpu.CompilerParams(
            collective_id=0, has_side_effects=True, vmem_limit_bytes=VMEM - KEPT
        ),
        cost_estimate=pl.CostEstimate(flops=6 * 10**9, bytes_accessed=16 * 2**20, transcendentals=0),
    )(x, ci, cg, im, gm, inf, gf, i1, i2, g1, g2)


def write_kernel(
    fv, nv, mv, sqv, lowv, im_hbm, gm_hbm, i1_hbm, i2_hbm, g1_hbm, g2_hbm,
    im_out, gm_out, iu_out, gu_out, i1_out, i2_out, g1_out, g2_out, ic_out, gc_out,
    old_v, new_v, upd_v, mom_v, mom_new, cv, s_in, s_c, s_out,
):
    _, y, z, _ = where_am_i()
    small = [
        (im_hbm, old_v.at[0]), (gm_hbm, old_v.at[1]),
        *[(r, mom_v.at[k]) for k, r in enumerate((i1_hbm, i2_hbm, g1_hbm, g2_hbm))],
    ]
    small = [pltpu.make_async_copy(src, dst, s_in.at[k]) for k, (src, dst) in enumerate(small)]
    for cp in small:
        cp.start()
    outs = []

    def put(src, dst, sem):
        cp = pltpu.make_async_copy(src, dst, sem)
        cp.start()
        outs.append(cp)

    scale = []
    for kind in range(2):
        square = jnp.sum(sqv[0, kind] + sqv[1, kind], axis=(0, 1), keepdims=True)
        scale.append(lax.rsqrt(square / (D * W) + 0.1))

    def rows_out(b, kind):
        out = (ic_out, gc_out)[kind]
        rows = pl.ds(pl.multiple_of(256 * b, 256), 256)
        return pltpu.make_async_copy(cv.at[b, kind], out.at[rows, :], s_c.at[b, kind])

    def blocks(p, _):
        k = 2 * p
        for kind in range(2):
            basis = fv[kind, pl.ds(k, 2)].reshape(512, RANK)
            for h in range(2):
                normed = nv[2 * kind + h].reshape(RANK, 256)
                full = jnp.dot(basis, normed, preferred_element_type=F32)
                col = kind * 512 + 256 * h
                for i in range(2):
                    old = mv[lax.rem(k + i + 8 - z + HERE, 8), :, :, col : col + 256].reshape(256, 256)
                    new = old.astype(F32) - full[256 * i : 256 * (i + 1)] * (0.05 * scale[kind])
                    cv[k + i, kind, :, 256 * h : 256 * h + 256] = new.astype(BF)
            for i in range(2):
                rows_out(k + i, kind).start()
        return 0

    lax.fori_loop(0, 2, blocks, 0)
    for cp in small:
        cp.wait()
    for kind, (new_out, upd_out) in enumerate(((im_out, iu_out), (gm_out, gu_out))):
        basis = fv[kind, z, y].reshape(64, RANK)
        for h in range(2):
            normed = nv[2 * kind + h].reshape(RANK, 256)
            cols = slice(256 * h, 256 * h + 256)
            u = jnp.dot(basis, normed, preferred_element_type=F32) * scale[kind]
            upd_v[kind, :, cols] = u
            new_v[kind, :, cols] = old_v[kind, :, cols] - 0.05 * u
        put(upd_v.at[kind], upd_out, s_out.at[2 * kind])
        put(new_v.at[kind], new_out, s_out.at[2 * kind + 1])
    for kind, (first_out, second_out) in enumerate(((i1_out, i2_out), (g1_out, g2_out))):
        for h in range(2):
            low = lowv[2 * kind + h]
            cols = slice(256 * h, 256 * h + 256)
            mom_new[2 * kind, :, cols] = 0.8 * mom_v[2 * kind, :, cols] + 0.2 * low
            mom_new[2 * kind + 1, :, cols] = 0.95 * mom_v[2 * kind + 1, :, cols] + 0.05 * low * low
        put(mom_new.at[2 * kind], first_out, s_out.at[4 + 2 * kind])
        put(mom_new.at[2 * kind + 1], second_out, s_out.at[5 + 2 * kind])
    lax.fori_loop(2, 4, blocks, 0)
    for cp in outs:
        cp.wait()
    for b in range(8):
        for kind in range(2):
            rows_out(b, kind).wait()


def written(f, n, m, sq, low, im, gm, i1, i2, g1, g2):
    sem, kept = pltpu.SemaphoreType.DMA, pl.BlockSpec(memory_space=ANY)
    held = pl.BlockSpec(memory_space=pltpu.VMEM)
    return pl.pallas_call(
        write_kernel,
        name="write",
        out_shape=(
            *[jax.ShapeDtypeStruct((64, 512), F32)] * 4,
            *[jax.ShapeDtypeStruct((8, 512), F32)] * 4,
            *[jax.ShapeDtypeStruct((D, 512), BF)] * 2,
        ),
        in_specs=[held] * 5 + [kept] * 6,
        out_specs=[kept] * 10,
        scratch_shapes=[
            *[pltpu.VMEM((2, 64, 512), F32)] * 3,
            *[pltpu.VMEM((4, 8, 512), F32)] * 2,
            pltpu.VMEM((8, 2, 256, 512), BF),
            sem((6,)),
            sem((8, 2)),
            sem((8,)),
        ],
        compiler_params=pltpu.CompilerParams(vmem_limit_bytes=VMEM - KEPT),
    )(f, n, m, sq, low, im, gm, i1, i2, g1, g2)


def on_device(x, ci, cg, im, gm, inf, gf, i1, i2, g1, g2):
    m, f, n, low, sq = gathered(x, ci, cg, im, gm, inf, gf, i1, i2, g1, g2)
    f, n, m, sq, low = (pltpu.with_memory_space_constraint(a, pltpu.VMEM) for a in (f, n, m, sq, low))
    out = written(f, n, m, sq, low, im, gm, i1, i2, g1, g2)
    return tuple(out)


def solution(mesh):
    tokens, rows, moments = P(("fs", "rep"), "tp"), P("fs", "tp"), P("fs", "tp")
    return jax.shard_map(
        on_device,
        mesh=mesh,
        in_specs=(
            P(("fs", "rep"), None), tokens, tokens, rows, rows, P("fs", None), P("fs", None),
            moments, moments, moments, moments,
        ),
        out_specs=(rows,) * 4 + (moments,) * 4 + (P(None, "tp"),) * 2,
        check_vma=False,
    )
```
